32 devices in a mesh: grp: 2 (over y), fs: 4 (over z), tp: 4 (over x, core).
Axes of the slice: x: 2, y: 2, z: 4, core: 2. Of those that a mesh axis runs over, the one named last changes fastest.
Arguments:
- residual_in: bfloat16 [4096, 2048], P(('grp', 'fs', 'tp')), parts along dimension 0, may hold values from -6 to 6
- hidden_first: bfloat16 [4096, 5632], P(('grp', 'fs', 'tp')), parts along dimension 0, may hold values from -6 to 6
- down_weight: bfloat16 [5632, 2048], P('tp', 'fs'), may hold values from -0.078125 to 0.078125
- mixer_out: bfloat16 [4096, 2048], P(('grp', 'fs', 'tp')), parts along dimension 0, may hold values from -6 to 6
- norm_gain: float32 [2, 2048], replicated, may hold values from 0.1 to 1.9
- norm_shift: float32 [2, 2048], replicated, may hold values from -1.5 to 1.5
- gate_weight: bfloat16 [2048, 5632], P('fs', 'tp'), may hold values from -0.125 to 0.125
- up_weight: bfloat16 [2048, 5632], P('fs', 'tp'), may hold values from -0.125 to 0.125
Outputs:
- mixed_state: bfloat16 [4096, 2048], P(('grp', 'fs', 'tp')), parts along dimension 0
- hidden_second: bfloat16 [4096, 5632], P(('grp', 'fs'), 'tp'), parts along dimension 0
The draws below stay inside these ranges and needn't reach their ends.
There are 2 independent parts, one for each index of `grp`. The reference program is written for one: setup_inputs(seed, part) draws one part's arguments, and reference() takes and returns one part's arrays. A program takes and returns all parts, laid end to end along the dimension named above; an argument that names none is the same for every part. Nothing has to cross between parts.
All inputs are finite; a program needn't handle non-finite values.
Results may differ from the reference program's by a relative error of at most 0.012.
Values may be sent and summed in bfloat16 or wider, within the bound.
A program may use at most 64 MiB of HBM per device.

```python
import jax
import jax.numpy as jnp
from jax import lax

D = 2048
FF = 5632
TOKENS = 2048
N_TP = 4


def block_scale(stream_key, dims, split, low, largest):
    loudness, own = 1.0, jax.random.fold_in(stream_key, 6)
    for position, shards_of in split:
        steps = jnp.exp(jax.random.uniform(jax.random.fold_in(own, position), (shards_of,), jnp.float32, low / len(split), largest / len(split)))
        loudness = loudness * jnp.repeat(steps, dims[position] // shards_of).reshape([-1 if axis == position else 1 for axis in range(len(dims))])
    return loudness


def normal_values(stream_key, dims, scale, bound, pieces=(), held_as=jnp.bfloat16):
    entries = scale * jax.random.normal(stream_key, dims, jnp.float32)
    if pieces:
        entries = entries * block_scale(stream_key, dims, pieces, -0.22, 0.18)
    return jnp.clip(entries, -bound, bound).astype(held_as)


def setup_inputs(seed: int = 0, part: int = 0) -> dict:
    key_of = jax.random.split(jax.random.key(seed), 9)
    part_keys = jax.random.split(jax.random.fold_in(key_of[8], part), 9)
    residual_in = normal_values(part_keys[0], (TOKENS, D), 1.0, 6.0, ((0, 16),))
    hidden_first = normal_values(part_keys[1], (TOKENS, FF), 1.0, 6.0, ((0, 16),))
    down_weight = normal_values(key_of[2], (FF, D), FF ** -0.5, 0.078125, ((0, 4), (1, 4)))
    mixer_out = normal_values(part_keys[3], (TOKENS, D), 1.0, 6.0, ((0, 16),))
    norm_gain = jnp.clip(1.0 + 0.18 * jax.random.normal(key_of[4], (2, D), jnp.float32), 0.1, 1.9)
    norm_shift = normal_values(key_of[5], (2, D), 0.3, 1.5, (), jnp.float32)
    gate_weight = normal_values(key_of[6], (D, FF), D ** -0.5, 0.125, ((0, 4), (1, 4)))
    up_weight = normal_values(key_of[7], (D, FF), D ** -0.5, 0.125, ((0, 4), (1, 4)))
    return dict(residual_in=residual_in, hidden_first=hidden_first, down_weight=down_weight, mixer_out=mixer_out, norm_gain=norm_gain, norm_shift=norm_shift, gate_weight=gate_weight, up_weight=up_weight)


def layer_norm(values, gain, shift):
    center = values - lax.optimization_barrier(jnp.mean(values, axis=-1, keepdims=True))
    variance = lax.optimization_barrier(jnp.mean(center * center, axis=-1, keepdims=True))
    return center * lax.rsqrt(variance + 1e-05) * gain + shift

def reference(residual_in, hidden_first, down_weight, mixer_out, norm_gain, norm_shift, gate_weight, up_weight):
    width = FF // N_TP

    def add_block(total, index):
        start = (index * width).astype(jnp.int32)
        rows = lax.dynamic_slice_in_dim(hidden_first, start, width, 1)
        cols = lax.dynamic_slice_in_dim(down_weight, start, width, 0)
        term = jnp.dot(rows, cols, preferred_element_type=jnp.float32).astype(jnp.bfloat16)
        term = lax.optimization_barrier(term)
        return (total + term.astype(jnp.float32), None)
    empty = jnp.zeros((hidden_first.shape[0], down_weight.shape[1]), jnp.float32)
    branch, _ = lax.scan(add_block, empty, jnp.arange(N_TP, dtype=jnp.int32))
    first = layer_norm(jnp.sqrt(2.0) * residual_in.astype(jnp.float32) + 0.5 * branch, norm_gain[0], norm_shift[0])
    mixed_state = layer_norm(jnp.sqrt(2.0) * first + mixer_out.astype(jnp.float32), norm_gain[1], norm_shift[1]).astype(jnp.bfloat16)
    gate = jnp.dot(mixed_state, gate_weight, preferred_element_type=jnp.float32)
    up = jnp.dot(mixed_state, up_weight, preferred_element_type=jnp.float32)
    hidden_second = (jax.nn.silu(gate) * up).astype(jnp.bfloat16)
    return (mixed_state, hidden_second)
```

```python
import functools

import jax
import jax.numpy as jnp
from jax import lax
from jax.experimental import pallas as pl
from jax.experimental.pallas import tpu as pltpu
from jax.sharding import PartitionSpec as P

MESH = pl.DeviceIdType.MESH


def layer_norm(values, gain, shift):
    center = values - jnp.mean(values, axis=-1, keepdims=True)
    variance = jnp.mean(center * center, axis=-1, keepdims=True)
    return center * lax.rsqrt(variance + 1e-05) * gain + shift


def kernel(
    sizes,
    res_ref,
    hid_ref,
    down_ref,
    mix_ref,
    gain_ref,
    shift_ref,
    gate_ref,
    up_ref,
    mixed_ref,
    out_ref,
    down_all,
    host_all,
    each_all,
    spread,
    part,
    red,
    mixed_all,
    host_acc,
    each_acc,
    back,
    load_sem,
    d_send,
    d_recv,
    h_send,
    h_recv,
    e_send,
    e_recv,
    a_send,
    a_recv,
    r_send,
    r_recv,
    m_send,
    m_recv,
    g_send,
    g_recv,
    b_send,
    b_recv,
):
    n_grp, n_fs, n_tp, sub = sizes
    shared = host_all.shape[3]
    g, f, t = lax.axis_index("grp"), lax.axis_index("fs"), lax.axis_index("tp")
    rows = res_ref.shape[0]
    width = gate_ref.shape[1]
    depth = gate_ref.shape[0]
    chunks = n_grp * sub

    def hid_block(peer):
        if len(hid_ref.shape) == 3:
            return hid_ref.at[peer]
        return hid_ref.at[:, pl.ds(pl.multiple_of(peer * width, width), width)]

    def own_rows(peer):
        return pl.ds(pl.multiple_of(peer * rows, rows), rows)

    load_down = pltpu.make_async_copy(down_ref, down_all.at[f], load_sem.at[0])
    loads = []
    for mat, ref in enumerate((gate_ref, up_ref)):
        loads.append(
            pltpu.make_async_copy(
                ref.at[:, pl.ds(0, shared)], host_all.at[f, mat], load_sem.at[1 + mat]
            )
        )
        loads.append(
            pltpu.make_async_copy(
                ref.at[:, pl.ds(shared, width - shared)], each_all.at[f, mat], load_sem.at[4 + mat]
            )
        )
    load_hid = pltpu.make_async_copy(hid_block(t), spread.at[own_rows(t)], load_sem.at[3])
    load_down.start()
    load_hid.start()
    for load in loads:
        load.start()

    lower = 2 * (f // 2)
    half = n_fs // 2
    host = lower + jnp.where(lower + 1 < half, 1, 0)
    is_host = f == host
    other = 2 * lower + 1 - f
    low_host = 1 if half > 1 else 0
    high_host = 2 * ((n_fs - 1) // 2)

    barrier = pltpu.get_barrier_semaphore()

    def greet(device):
        pl.semaphore_signal(barrier, inc=1, device_id=device, device_id_type=MESH)

    for d in range(1, n_grp):
        greet({"grp": lax.rem(g + d, n_grp)})
    for d in range(1, n_tp):
        greet({"tp": lax.rem(t + d, n_tp)})

    @pl.when(f > 0)
    def _():
        greet({"fs": f - 1})

    @pl.when(f < n_fs - 1)
    def _():
        greet({"fs": f + 1})

    inner = jnp.minimum(f, 1) + jnp.minimum(n_fs - 1 - f, 1)
    pl.semaphore_wait(barrier, n_grp - 1 + n_tp - 1 + inner)

    def block_copy(all_refs, send, recv):
        def copy(src, chunk, way, device):
            blocks = all_refs(src)
            size = blocks.shape[0] // chunks
            block = blocks.at[pl.ds(pl.multiple_of(chunk * size, size), size)]
            return pltpu.make_async_remote_copy(
                src_ref=block,
                dst_ref=block,
                send_sem=send(src).at[way, chunk],
                recv_sem=recv(src).at[chunk],
                device_id=device,
                device_id_type=MESH,
            )

        return copy

    def weight(refs, send, recv, mat):
        return block_copy(
            lambda src: refs.at[src, mat],
            lambda src: send.at[2 * src + mat],
            lambda src: recv.at[2 * src + mat],
        )

    def start(copy):
        copy.start()

    def wait_send(copy):
        copy.wait_send()

    class Gather:
        def __init__(self, copies, low, high, whole, needs):
            self.copies, self.low, self.high = copies, low, high
            self.whole, self.needs = whole, needs

        def whole_up(self, plane):
            return (2 * plane < n_fs) & self.whole

        def whole_down(self, plane):
            return (2 * plane >= n_fs) & self.whole

        def reached(self, plane):
            return (plane >= self.low) & (plane <= self.high)

        def along(self, copy, src, chunk, act, mine):
            up = (src <= f) & self.reached(f + 1)
            down = (src >= f) & self.reached(f - 1)
            if not mine:
                up = up & self.whole_up(f + 1)
                down = down & self.whole_down(f - 1)

            @pl.when(up)
            def _():
                act(copy(src, chunk, 0, {"fs": f + 1}))

            @pl.when(down)
            def _():
                act(copy(src, chunk, 1, {"fs": f - 1}))

        def all_along(self, src, act):
            for j in range(sub):
                for copy in self.copies:
                    self.along(copy, src, g * sub + j, act, True)
            if self.whole:
                for d in range(1, n_grp):
                    for j in range(sub):
                        for copy in self.copies:
                            chunk = lax.rem(g + d, n_grp) * sub + j
                            self.along(copy, src, chunk, act, False)

        def across(self, copy, src, chunk, act):
            for d in range(1, n_grp):
                act(copy(src, chunk, 1 + d, {"grp": lax.rem(g + d, n_grp)}))

        def whole_in(self, src):
            return ((src < f) & self.whole_up(f)) | ((src > f) & self.whole_down(f))

        def comes(self, src):
            return (src >= 0) & (src < n_fs) & (src != f) & self.reached(f)

        def swaps(self, src):
            return self.comes(src) & self.needs & jnp.logical_not(self.whole_in(src))

        def take(self, src):
            @pl.when(self.comes(src))
            def _():
                for j in range(sub):
                    for copy in self.copies:
                        chunk = g * sub + j
                        copy(src, chunk, 0, {"fs": other}).wait_recv()
                        self.along(copy, src, chunk, start, True)

                        @pl.when(self.swaps(src))
                        def _():
                            self.across(copy, src, chunk, start)

            if self.whole:

                @pl.when(self.comes(src) & self.whole_in(src))
                def _():
                    for d in range(1, n_grp):
                        for j in range(sub):
                            for copy in self.copies:
                                chunk = lax.rem(g + d, n_grp) * sub + j
                                copy(src, chunk, 0, {"fs": other}).wait_recv()
                                self.along(copy, src, chunk, start, False)

        def take_across(self, src):
            @pl.when(self.swaps(src))
            def _():
                for d in range(1, n_grp):
                    for j in range(sub):
                        for copy in self.copies:
                            chunk = lax.rem(g + d, n_grp) * sub + j
                            copy(src, chunk, 0, {"fs": other}).wait_recv()

        def drain(self, src):
            @pl.when((src == f) | self.comes(src))
            def _():
                if self.whole:
                    @pl.when((src == f) | self.whole_in(src))
                    def _():
                        for d in range(1, n_grp):
                            for j in range(sub):
                                for copy in self.copies:
                                    chunk = lax.rem(g + d, n_grp) * sub + j
                                    self.along(copy, src, chunk, wait_send, False)
                for j in range(sub):
                    for copy in self.copies:
                        self.along(copy, src, g * sub + j, wait_send, True)

            @pl.when(self.swaps(src))
            def _():
                for j in range(sub):
                    for copy in self.copies:
                        self.across(copy, src, g * sub + j, wait_send)

    def source(k):
        return f + (1 - 2 * lax.rem(k, 2)) * ((k + 1) // 2)

    def valid(src):
        return (src >= 0) & (src < n_fs)

    d_copy = block_copy(
        lambda src: down_all.at[src], lambda src: d_send.at[src], lambda src: d_recv.at[src]
    )
    down = Gather([d_copy], 0, n_fs - 1, False, True)
    hosted = Gather(
        [weight(host_all, h_send, h_recv, mat) for mat in range(2)],
        low_host,
        high_host,
        True,
        is_host,
    )
    each = Gather(
        [weight(each_all, e_send, e_recv, mat) for mat in range(2)], 0, n_fs - 1, True, True
    )

    def a_copy(d):
        peer = lax.rem(t + d, n_tp)
        return pltpu.make_async_remote_copy(
            src_ref=hid_block(peer),
            dst_ref=spread.at[own_rows(t)],
            send_sem=a_send.at[d],
            recv_sem=a_recv.at[d],
            device_id={"tp": peer},
            device_id_type=MESH,
        )

    def r_copy(src, d):
        peer = lax.rem(t + d, n_tp)
        return pltpu.make_async_remote_copy(
            src_ref=part.at[src, own_rows(peer)],
            dst_ref=red.at[d, src],
            send_sem=r_send.at[d, src],
            recv_sem=r_recv.at[d, src],
            device_id={"tp": peer},
            device_id_type=MESH,
        )

    core = lax.rem(t, 2)
    sibling = t + 1 - 2 * core

    def m_copy(owner, whose, hop):
        peer = sibling if hop == 0 else lax.rem(t + 2 * hop, n_tp)
        place = mixed_all.at[whose, own_rows(owner)]
        return pltpu.make_async_remote_copy(
            src_ref=place,
            dst_ref=place,
            send_sem=m_send.at[whose, owner, hop],
            recv_sem=m_recv.at[whose, owner],
            device_id={"tp": peer},
            device_id_type=MESH,
        )

    chips = n_tp // 2

    def m_out(whose):
        for hop in list(range(1, chips)) + [0]:
            m_copy(t, whose, hop).start()

    def m_relay(whose):
        for hop in range(1, chips):
            owner = lax.rem(t + 2 * hop, n_tp)
            m_copy(owner, whose, 0).wait_recv()
            m_copy(owner, whose, 0).start()

    def m_rest(whose):
        for hop in range(chips):
            m_copy(lax.rem(sibling + 2 * hop, n_tp), whose, 0).wait_recv()

    def m_drain(whose):
        for hop in range(chips):
            m_copy(t, whose, hop).wait_send()
        for hop in range(1, chips):
            m_copy(lax.rem(t + 2 * hop, n_tp), whose, 0).wait_send()

    def g_copy():
        return pltpu.make_async_remote_copy(
            src_ref=mixed_all.at[0, own_rows(t)],
            dst_ref=mixed_all.at[1, own_rows(t)],
            send_sem=g_send.at[0],
            recv_sem=g_recv.at[0],
            device_id={"fs": other},
            device_id_type=MESH,
        )

    tiles = 2
    tile = n_tp * rows // tiles

    def tile_rows(i):
        return pl.ds(pl.multiple_of(i * tile, tile), tile)

    def b_copy(i):
        return pltpu.make_async_remote_copy(
            src_ref=back.at[tile_rows(i)],
            dst_ref=out_ref.at[tile_rows(i), pl.ds(0, shared)],
            send_sem=b_send.at[i],
            recv_sem=b_recv.at[i],
            device_id={"fs": other},
            device_id_type=MESH,
        )

    load_down.wait()
    down.all_along(f, start)
    for d in range(1, n_tp):
        a_copy(d).start()
    for load in loads:
        load.wait()
    load_hid.wait()

    @pl.when(jnp.logical_not(is_host))
    def _():
        hosted.all_along(f, start)

    def first_half(k, carry):
        src = source(k)

        down.take(src)

        @pl.when((k == 2 * n_fs - 2) & is_host)
        def _():
            hosted.all_along(f, start)

        @pl.when(k == 2)
        def _():
            for d in range(1, n_tp):
                a_copy(d).wait_recv()

        done = source(k - 2)

        @pl.when((k >= 2) & valid(done))
        def _():
            down.take_across(done)
            part[done] = jnp.dot(
                spread[...], down_all[done], preferred_element_type=jnp.float32
            ).astype(jnp.bfloat16)
            for d in range(1, n_tp):
                r_copy(done, d).start()

        return carry

    lax.fori_loop(1, 2 * n_fs + 1, first_half, 0)

    for src in range(n_fs):
        for d in range(1, n_tp):
            r_copy(src, d).wait_recv()
    pieces = []
    for src in range(n_fs):
        total = part[src, own_rows(t)].astype(jnp.float32)
        for d in range(1, n_tp):
            total = total + red[d, src].astype(jnp.float32)
        pieces.append(total)
    branch = jnp.concatenate(pieces, axis=1)
    first = layer_norm(
        jnp.sqrt(2.0) * res_ref[...].astype(jnp.float32) + 0.5 * branch,
        gain_ref[0:1],
        shift_ref[0:1],
    )
    mixed = layer_norm(
        jnp.sqrt(2.0) * first + mix_ref[...].astype(jnp.float32), gain_ref[1:2], shift_ref[1:2]
    ).astype(jnp.bfloat16)
    mixed_all[0, own_rows(t)] = mixed
    mixed_ref[...] = mixed

    @pl.when(jnp.logical_not(is_host))
    def _():
        g_copy().start()

    m_out(0)

    @pl.when(jnp.logical_not(is_host))
    def _():
        each.all_along(f, start)

    def take_hosted(k, carry):
        hosted.take(source(k))
        return carry

    lax.fori_loop(1, 2 * n_fs - 1, take_hosted, 0)

    @pl.when(is_host)
    def _():
        each.all_along(f, start)

    m_relay(0)

    @pl.when(is_host)
    def _():
        g_copy().wait_recv()
        m_out(1)

    def take_each(k, carry):
        each.take(source(k))
        return carry

    lax.fori_loop(1, 3, take_each, 0)
    m_rest(0)

    def products(whose, span, gather, refs, total):
        total[...] = jnp.zeros_like(total)

        def add(k, carry):
            src = source(k)

            @pl.when(valid(src))
            def _():
                if gather is not None:
                    gather.take_across(src)
                here = pl.ds(pl.multiple_of(src * depth, depth), depth)
                for mat in range(2):
                    total[mat] += jnp.dot(
                        mixed_all[whose, span, here],
                        refs[src, mat],
                        preferred_element_type=jnp.float32,
                    )

            return carry

        lax.fori_loop(0, 2 * n_fs - 1, add, 0)
        gate = total[0]
        return (gate / (1.0 + jnp.exp(-gate)) * total[1]).astype(jnp.bfloat16)

    everything = pl.ds(0, n_tp * rows)

    @pl.when(is_host)
    def _():
        m_relay(1)
        out_ref[:, pl.ds(0, shared)] = products(0, everything, hosted, host_all, host_acc)

    lax.fori_loop(3, 2 * n_fs - 1, take_each, 0)

    @pl.when(is_host)
    def _():
        m_rest(1)

        def serve(i, carry):
            back[tile_rows(i)] = products(
                1, tile_rows(i), None, host_all, host_acc.at[:, pl.ds(0, tile)]
            )
            b_copy(i).start()
            return carry

        lax.fori_loop(0, tiles, serve, 0)

    out_ref[:, pl.ds(shared, width - shared)] = products(0, everything, each, each_all, each_acc)

    @pl.when(is_host)
    def _():
        for i in range(tiles):
            b_copy(i).wait_send()
        m_drain(1)

    @pl.when(jnp.logical_not(is_host))
    def _():
        g_copy().wait_send()
        for i in range(tiles):
            b_copy(i).wait_recv()

    m_drain(0)
    for d in range(1, n_tp):
        a_copy(d).wait_send()
        for src in range(n_fs):
            r_copy(src, d).wait_send()

    def drain(src, carry):
        for gather in (down, hosted, each):
            gather.drain(src)
        return carry

    lax.fori_loop(0, n_fs, drain, 0)


def paired_kernel(
    sizes,
    res_ref,
    hid_ref,
    down_ref,
    mix_ref,
    gain_ref,
    shift_ref,
    gate_ref,
    up_ref,
    mixed_ref,
    out_ref,
    down_all,
    cols_all,
    spread,
    part,
    red,
    mixed_all,
    back,
    load_sem,
    c_load,
    d_send,
    d_recv,
    c_send,
    c_recv,
    a_send,
    a_recv,
    r_send,
    r_recv,
    m_send,
    m_recv,
    g_send,
    g_recv,
    b_send,
    b_recv,
):
    n_grp, n_fs, n_tp, sub, own, moved, pieces = sizes
    g, f, t = lax.axis_index("grp"), lax.axis_index("fs"), lax.axis_index("tp")
    rows = res_ref.shape[0]
    width = gate_ref.shape[1]
    depth = gate_ref.shape[0]
    n_col = cols_all.shape[0]
    lanes = width // n_col

    lower = 2 * (f // 2)
    mate = 2 * lower + 1 - f
    inner = (f > 0) & (f < n_fs - 1)
    outer = jnp.logical_not(inner)
    facing = n_fs - 1 - jnp.where(inner, f, mate)
    beyond = n_fs - 1 - jnp.where(inner, mate, f)

    def hid_block(peer):
        return hid_ref.at[:, pl.ds(pl.multiple_of(peer * width, width), width)]

    def own_rows(peer):
        return pl.ds(pl.multiple_of(peer * rows, rows), rows)

    load_down = pltpu.make_async_copy(down_ref, down_all.at[f], load_sem.at[0])
    load_hid = pltpu.make_async_copy(hid_block(t), spread.at[own_rows(t)], load_sem.at[1])

    def load_col(c, mat):
        return pltpu.make_async_copy(
            (gate_ref, up_ref)[mat].at[:, pl.ds(pl.multiple_of(c * lanes, lanes), lanes)],
            cols_all.at[c, f, :, pl.ds(mat * lanes, lanes)],
            c_load.at[c, mat],
        )

    load_down.start()
    load_hid.start()

    def each_col(low, high, act):
        def body(c, carry):
            act(c)
            return carry

        lax.fori_loop(low, high, body, 0)

    def load_cols(c):
        for mat in range(2):
            load_col(c, mat).start()

    def loaded_cols(c):
        for mat in range(2):
            load_col(c, mat).wait()

    each_col(0, n_col, load_cols)

    barrier = pltpu.get_barrier_semaphore()

    def greet(device):
        pl.semaphore_signal(barrier, inc=1, device_id=device, device_id_type=MESH)

    for d in range(1, n_grp):
        greet({"grp": lax.rem(g + d, n_grp)})
    for d in range(1, n_tp):
        greet({"tp": lax.rem(t + d, n_tp)})
    greet({"fs": mate})

    @pl.when(inner)
    def _():
        greet({"fs": facing})

    pl.semaphore_wait(barrier, n_grp - 1 + n_tp - 1 + 1 + inner.astype(jnp.int32))

    MAIN, OUT, ACROSS = 0, 1, 2

    def device_of(way):
        if way == MAIN:
            return {"fs": jnp.where(inner, facing, mate)}
        if way == OUT:
            return {"fs": mate}
        return {"grp": lax.rem(g + way - ACROSS + 1, n_grp)}

    def d_copy(src, share, j, way):
        size = down_all.shape[1] // (n_grp * sub)
        place = share * sub + j
        block = down_all.at[src, pl.ds(pl.multiple_of(place * size, size), size)]
        return pltpu.make_async_remote_copy(
            src_ref=block,
            dst_ref=block,
            send_sem=d_send.at[way, src, place],
            recv_sem=d_recv.at[src, place],
            device_id=device_of(way),
            device_id_type=MESH,
        )

    def c_copy(c, src, share, way):
        size = depth // n_grp
        block = cols_all.at[c, src, pl.ds(pl.multiple_of(share * size, size), size)]
        return pltpu.make_async_remote_copy(
            src_ref=block,
            dst_ref=block,
            send_sem=c_send.at[way, src, c, share],
            recv_sem=c_recv.at[src, c, share],
            device_id=device_of(way),
            device_id_type=MESH,
        )

    across = [ACROSS + d - 1 for d in range(1, n_grp)]
    others = [lax.rem(g + d, n_grp) for d in range(1, n_grp)]

    def d_send_on(src, share, j, ways):
        for way in ways:
            d_copy(src, share, j, way).start()

    def c_send_on(c, src, share, ways):
        for way in ways:
            c_copy(c, src, share, way).start()

    def d_pass(src, j, ways):
        d_copy(src, g, j, MAIN).wait_recv()
        d_send_on(src, g, j, ways)

    def c_pass(c, src, ways):
        c_copy(c, src, g, MAIN).wait_recv()
        c_send_on(c, src, g, ways)

    def d_rest(src):
        for share in others:
            for j in range(sub):
                d_copy(src, share, j, MAIN).wait_recv()

    def c_rest(c, src):
        for share in others:
            c_copy(c, src, share, MAIN).wait_recv()

    def a_copy(d):
        peer = lax.rem(t + d, n_tp)
        return pltpu.make_async_remote_copy(
            src_ref=hid_block(peer),
            dst_ref=spread.at[own_rows(t)],
            send_sem=a_send.at[d],
            recv_sem=a_recv.at[d],
            device_id={"tp": peer},
            device_id_type=MESH,
        )

    def r_copy(src, d):
        peer = lax.rem(t + d, n_tp)
        return pltpu.make_async_remote_copy(
            src_ref=part.at[src, own_rows(peer)],
            dst_ref=red.at[d, src],
            send_sem=r_send.at[d, src],
            recv_sem=r_recv.at[d, src],
            device_id={"tp": peer},
            device_id_type=MESH,
        )

    core = lax.rem(t, 2)
    sibling = t + 1 - 2 * core
    chips = n_tp // 2
    piece = rows // pieces

    def piece_rows(owner, q):
        return pl.ds(pl.multiple_of(owner * rows + q * piece, piece), piece)

    def m_copy(owner, whose, hop, q):
        peer = sibling if hop == 0 else lax.rem(t + 2 * hop, n_tp)
        place = mixed_all.at[whose, piece_rows(owner, q)]
        return pltpu.make_async_remote_copy(
            src_ref=place,
            dst_ref=place,
            send_sem=m_send.at[whose, owner, hop, q],
            recv_sem=m_recv.at[whose, owner, q],
            device_id={"tp": peer},
            device_id_type=MESH,
        )

    def m_out(whose, q):
        for hop in list(range(1, chips)) + [0]:
            m_copy(t, whose, hop, q).start()

    def m_relay(whose, q):
        for hop in range(1, chips):
            owner = lax.rem(t + 2 * hop, n_tp)
            m_copy(owner, whose, 0, q).wait_recv()
            m_copy(owner, whose, 0, q).start()

    def m_rest(whose, q):
        for hop in range(chips):
            m_copy(lax.rem(sibling + 2 * hop, n_tp), whose, 0, q).wait_recv()

    def m_drain(whose, q):
        for hop in range(chips):
            m_copy(t, whose, hop, q).wait_send()
        for hop in range(1, chips):
            m_copy(lax.rem(t + 2 * hop, n_tp), whose, 0, q).wait_send()

    def g_copy(q):
        return pltpu.make_async_remote_copy(
            src_ref=mixed_all.at[0, piece_rows(t, q)],
            dst_ref=mixed_all.at[1, piece_rows(t, q)],
            send_sem=g_send.at[q],
            recv_sem=g_recv.at[q],
            device_id={"fs": mate},
            device_id_type=MESH,
        )

    def col_lanes(c):
        return pl.ds(pl.multiple_of(c * lanes, lanes), lanes)

    def b_copy(c):
        return pltpu.make_async_remote_copy(
            src_ref=back.at[c - own],
            dst_ref=out_ref.at[:, col_lanes(c)],
            send_sem=b_send.at[c - own],
            recv_sem=b_recv.at[c - own],
            device_id={"fs": mate},
            device_id_type=MESH,
        )

    def first_product(src):
        part[src] = jnp.dot(
            spread[...], down_all[src], preferred_element_type=jnp.float32
        ).astype(jnp.bfloat16)
        for d in range(1, n_tp):
            r_copy(src, d).start()

    def take_hidden():
        load_hid.wait()
        for d in range(1, n_tp):
            a_copy(d).wait_recv()

    def norms():
        for src in range(n_fs):
            for d in range(1, n_tp):
                r_copy(src, d).wait_recv()
        columns = []
        for src in range(n_fs):
            total = part[src, own_rows(t)].astype(jnp.float32)
            for d in range(1, n_tp):
                total = total + red[d, src].astype(jnp.float32)
            columns.append(total)
        branch = jnp.concatenate(columns, axis=1)
        first = layer_norm(
            jnp.sqrt(2.0) * res_ref[...].astype(jnp.float32) + 0.5 * branch,
            gain_ref[0:1],
            shift_ref[0:1],
        )
        mixed = layer_norm(
            jnp.sqrt(2.0) * first + mix_ref[...].astype(jnp.float32),
            gain_ref[1:2],
            shift_ref[1:2],
        ).astype(jnp.bfloat16)
        mixed_all[0, own_rows(t)] = mixed
        mixed_ref[...] = mixed

    def second_product(whose, c):
        weight = cols_all[c].reshape(n_fs * depth, 2 * lanes)
        total = jnp.dot(mixed_all[whose], weight, preferred_element_type=jnp.float32)
        gate = total[:, :lanes]
        return (gate / (1.0 + jnp.exp(-gate)) * total[:, lanes:]).astype(jnp.bfloat16)

    load_down.wait()

    @pl.when(inner)
    def _():
        for j in range(sub):
            d_send_on(f, g, j, (MAIN, OUT))

    @pl.when(outer)
    def _():
        for share in [g] + others:
            for j in range(sub):
                d_send_on(f, share, j, (MAIN,))

    for d in range(1, n_tp):
        a_copy(d).start()
    each_col(0, n_col, loaded_cols)

    @pl.when(outer)
    def _():
        each_col(0, n_col, lambda c: c_send_on(c, f, g, (MAIN,)))

    ahead = min(4, n_col)
    early = min(2, n_col)

    @pl.when(inner)
    def _():
        for j in range(sub):
            d_pass(mate, j, (MAIN,))
            d_pass(facing, j, [OUT] + across)
        for c in range(ahead):
            c_send_on(c, f, g, (MAIN,))

    @pl.when(outer)
    def _():
        for j in range(sub):
            d_pass(mate, j, across)

    take_hidden()

    def step(k, carry):
        @pl.when((k == 1) & inner)
        def _():
            for j in range(sub):
                d_pass(beyond, j, [OUT] + across)
            each_col(0, own, lambda c: c_send_on(c, f, g, (OUT,)))
            d_rest(mate)

        @pl.when((k == 1) & outer)
        def _():
            for j in range(sub):
                d_pass(facing, j, across)
            d_rest(mate)

        @pl.when((k == 2) & outer)
        def _():
            for j in range(sub):
                d_pass(beyond, j, across)

        @pl.when(k == 2)
        def _():
            d_rest(facing)

        @pl.when((k >= 2) & (k - 2 < early) & inner)
        def _():
            c_pass(k - 2, mate, (MAIN,))

        @pl.when(k == 3)
        def _():
            d_rest(beyond)

        first_product(
            jnp.where(k == 0, f, jnp.where(k == 1, mate, jnp.where(k == 2, facing, beyond)))
        )
        return carry

    lax.fori_loop(0, n_fs, step, 0)
    norms()

    def swapped(c):
        return c >= n_col - moved

    def serve(c):
        c_rest(c, mate)
        c_rest(c, facing)
        c_rest(c, beyond)
        out_ref[:, col_lanes(c)] = second_product(0, c)

        @pl.when(c >= own)
        def _():
            back[c - own] = second_product(1, c)
            b_copy(c).start()

    def relay(c):
        @pl.when(c >= early)
        def _():
            c_pass(c, mate, (MAIN,))

        @pl.when(swapped(c))
        def _():
            c_send_on(c, mate, g, across)

        @pl.when(c + ahead < n_col)
        def _():
            c_send_on(c + ahead, f, g, (MAIN,))

        for src in (facing, beyond):
            c_pass(c, src, across)

            @pl.when(c < own)
            def _():
                c_send_on(c, src, g, (OUT,))

    def relay_and_serve(c):
        relay(c)
        first = c - (n_col - 4)

        def from_mate(q):
            g_copy(q).wait_recv()
            m_out(1, q)

        @pl.when(c == n_col - 8)
        def _():
            for q in range(pieces):
                m_relay(0, q)

        @pl.when(c == n_col - 5)
        def _():
            for q in range(pieces // 2):
                from_mate(q)
            for q in range(pieces):
                m_rest(0, q)

        @pl.when(c == n_col - 4)
        def _():
            for q in range(pieces // 2, pieces):
                from_mate(q)
            for q in range(pieces // 2):
                m_relay(1, q)

        @pl.when(c == n_col - 3)
        def _():
            for q in range(pieces // 2, pieces):
                m_relay(1, q)
            for q in range(pieces):
                m_rest(1, q)

        low = jnp.where(first < 1, 0, 2 * (first - 1))
        high = jnp.where(first < 1, 0, jnp.where(c == n_col - 1, n_col, 2 * first))
        each_col(low, high, serve)

    @pl.when(inner)
    def _():
        for q in range(pieces):
            m_out(0, q)
        each_col(0, n_col, relay_and_serve)

    @pl.when(outer)
    def _():
        for q in range(pieces):
            g_copy(q).start()
            m_out(0, q)
        for share in others:
            each_col(0, n_col - moved, lambda c: c_send_on(c, f, share, (MAIN,)))

        def pass_own(c):
            for src in (mate, facing, beyond):
                c_pass(c, src, across)

        each_col(0, own, pass_own)
        for q in range(pieces):
            m_relay(0, q)
        for q in range(pieces):
            m_rest(0, q)

        def make_own(c):
            for src in (mate, facing, beyond):
                c_rest(c, src)
            out_ref[:, col_lanes(c)] = second_product(0, c)

        each_col(0, own, make_own)
        each_col(own, n_col, lambda c: b_copy(c).wait_recv())

    for d in range(1, n_tp):
        a_copy(d).wait_send()
        for src in range(n_fs):
            r_copy(src, d).wait_send()
    for q in range(pieces):
        m_drain(0, q)

    def d_sent(src, share, ways):
        for j in range(sub):
            for way in ways:
                d_copy(src, share, j, way).wait_send()

    def c_sent(low, high, src, share, ways):
        def act(c):
            for way in ways:
                c_copy(c, src, share, way).wait_send()

        each_col(low, high, act)

    @pl.when(inner)
    def _():
        d_sent(f, g, (MAIN, OUT))
        d_sent(mate, g, (MAIN,))
        c_sent(0, n_col, f, g, (MAIN,))
        c_sent(0, n_col, mate, g, (MAIN,))
        c_sent(0, own, f, g, (OUT,))
        c_sent(n_col - moved, n_col, mate, g, across)
        for src in (facing, beyond):
            d_sent(src, g, [OUT] + across)
            c_sent(0, n_col, src, g, across)
            c_sent(0, own, src, g, (OUT,))
        for q in range(pieces):
            m_drain(1, q)
        each_col(own, n_col, lambda c: b_copy(c).wait_send())

    @pl.when(outer)
    def _():
        for share in [g] + others:
            d_sent(f, share, (MAIN,))
        c_sent(0, n_col, f, g, (MAIN,))
        for share in others:
            c_sent(0, n_col - moved, f, share, (MAIN,))
        for src in (mate, facing, beyond):
            d_sent(src, g, across)
            c_sent(0, own, src, g, across)
        for q in range(pieces):
            g_copy(q).wait_send()


def paired_call(sizes, arguments):
    n_grp, n_fs, n_tp = sizes
    residual_in, hidden_first, down_weight, _, _, _, gate_weight, _ = arguments
    rows, model = residual_in.shape
    depth, width = gate_weight.shape
    cols = down_weight.shape[1]
    tokens = rows * n_tp
    lanes = 128
    n_col = width // lanes
    sub = 4
    own = max(1, n_col * 4 // 11)
    moved = 1
    pieces = 4
    vmem = pl.BlockSpec(memory_space=pltpu.VMEM)
    anywhere = pl.BlockSpec(memory_space=pl.ANY)
    dma = pltpu.SemaphoreType.DMA
    return pl.pallas_call(
        functools.partial(paired_kernel, (n_grp, n_fs, n_tp, sub, own, moved, pieces)),
        out_shape=(
            jax.ShapeDtypeStruct((rows, model), jnp.bfloat16),
            jax.ShapeDtypeStruct((tokens, width), jnp.bfloat16),
        ),
        in_specs=[vmem, anywhere, anywhere, vmem, vmem, vmem, anywhere, anywhere],
        out_specs=(vmem, vmem),
        scratch_shapes=[
            pltpu.VMEM((n_fs,) + down_weight.shape, jnp.bfloat16),
            pltpu.VMEM((n_col, n_fs, depth, 2 * lanes), jnp.bfloat16),
            pltpu.VMEM((tokens, width), jnp.bfloat16),
            pltpu.VMEM((n_fs, tokens, cols), jnp.bfloat16),
            pltpu.VMEM((n_tp, n_fs, rows, cols), jnp.bfloat16),
            pltpu.VMEM((2, tokens, model), jnp.bfloat16),
            pltpu.VMEM((n_col - own, tokens, lanes), jnp.bfloat16),
            dma((2,)),
            dma((n_col, 2)),
            dma((1 + n_grp, n_fs, n_grp * sub)),
            dma((n_fs, n_grp * sub)),
            dma((1 + n_grp, n_fs, n_col, n_grp)),
            dma((n_fs, n_col, n_grp)),
            dma((n_tp,)),
            dma((n_tp,)),
            dma((n_tp, n_fs)),
            dma((n_tp, n_fs)),
            dma((2, n_tp, n_tp // 2, pieces)),
            dma((2, n_tp, pieces)),
            dma((pieces,)),
            dma((pieces,)),
            dma((n_col - own,)),
            dma((n_col - own,)),
        ],
        compiler_params=pltpu.CompilerParams(
            collective_id=0, has_side_effects=True, vmem_limit_bytes=60 * 1024 * 1024
        ),
        name="paired_half_steps",
    )(*arguments)


def fits_pairs(sizes, residual_in, down_weight, gate_weight):
    n_grp, n_fs, n_tp = sizes
    depth, width = gate_weight.shape
    return (
        n_fs == 4
        and n_tp % 2 == 0
        and width % 128 == 0
        and width // 128 >= 9
        and depth % (n_grp * 32) == 0
        and down_weight.shape[0] % (n_grp * 4 * 16) == 0
        and residual_in.shape[0] % (4 * 16) == 0
    )


def on_device(
    sizes,
    residual_in,
    hidden_first,
    down_weight,
    mixer_out,
    norm_gain,
    norm_shift,
    gate_weight,
    up_weight,
):
    if fits_pairs(sizes, residual_in, down_weight, gate_weight):
        arguments = (
            residual_in,
            hidden_first,
            down_weight,
            mixer_out,
            norm_gain,
            norm_shift,
            gate_weight,
            up_weight,
        )
        return paired_call(sizes, arguments)
    n_grp, n_fs, n_tp = sizes
    rows, model = residual_in.shape
    depth, width = gate_weight.shape
    cols = down_weight.shape[1]
    sub = 1
    if depth % (n_grp * 2 * 32) == 0 and down_weight.shape[0] % (n_grp * 2 * 32) == 0:
        sub = 2
    chunks = n_grp * sub
    each = max(1, width * 3 // (11 * 128)) * 128
    shared = (width - each) // 128 * 128
    each = width - shared
    if width % 128:
        hidden_first = hidden_first.reshape(rows, n_tp, width).transpose(1, 0, 2)
    vmem = pl.BlockSpec(memory_space=pltpu.VMEM)
    anywhere = pl.BlockSpec(memory_space=pl.ANY)
    dma = pltpu.SemaphoreType.DMA
    tokens = rows * n_tp
    return pl.pallas_call(
        functools.partial(kernel, (n_grp, n_fs, n_tp, sub)),
        out_shape=(
            jax.ShapeDtypeStruct((rows, model), jnp.bfloat16),
            jax.ShapeDtypeStruct((tokens, width), jnp.bfloat16),
        ),
        in_specs=[vmem, anywhere, anywhere, vmem, vmem, vmem, anywhere, anywhere],
        out_specs=(vmem, vmem),
        scratch_shapes=[
            pltpu.VMEM((n_fs,) + down_weight.shape, jnp.bfloat16),
            pltpu.VMEM((n_fs, 2, depth, shared), jnp.bfloat16),
            pltpu.VMEM((n_fs, 2, depth, each), jnp.bfloat16),
            pltpu.VMEM((tokens, width), jnp.bfloat16),
            pltpu.VMEM((n_fs, tokens, cols), jnp.bfloat16),
            pltpu.VMEM((n_tp, n_fs, rows, cols), jnp.bfloat16),
            pltpu.VMEM((2, tokens, model), jnp.bfloat16),
            pltpu.VMEM((2, tokens, shared), jnp.float32),
            pltpu.VMEM((2, tokens, each), jnp.float32),
            pltpu.VMEM((tokens, shared), jnp.bfloat16),
            dma((6,)),
            dma((n_fs, 1 + n_grp, chunks)),
            dma((n_fs, chunks)),
            dma((2 * n_fs, 1 + n_grp, chunks)),
            dma((2 * n_fs, chunks)),
            dma((2 * n_fs, 1 + n_grp, chunks)),
            dma((2 * n_fs, chunks)),
            dma((n_tp,)),
            dma((n_tp,)),
            dma((n_tp, n_fs)),
            dma((n_tp, n_fs)),
            dma((2, n_tp, n_tp // 2)),
            dma((2, n_tp)),
            dma((1,)),
            dma((1,)),
            dma((2,)),
            dma((2,)),
        ],
        compiler_params=pltpu.CompilerParams(
            collective_id=0, has_side_effects=True, vmem_limit_bytes=60 * 1024 * 1024
        ),
        name="half_steps",
    )(
        residual_in,
        hidden_first,
        down_weight,
        mixer_out,
        norm_gain,
        norm_shift,
        gate_weight,
        up_weight,
    )


def solution(mesh):
    sizes = tuple(mesh.shape[axis] for axis in ("grp", "fs", "tp"))
    in_specs = (
        P(("grp", "fs", "tp"), None),
        P(("grp", "fs", "tp"), None),
        P("tp", "fs"),
        P(("grp", "fs", "tp"), None),
        P(),
        P(),
        P("fs", "tp"),
        P("fs", "tp"),
    )
    out_specs = (P(("grp", "fs", "tp"), None), P(("grp", "fs"), "tp"))
    return jax.shard_map(
        functools.partial(on_device, sizes),
        mesh=mesh,
        in_specs=in_specs,
        out_specs=out_specs,
        check_vma=False,
    )
```

```python
import functools

import jax
import jax.numpy as jnp
from jax import lax
from jax.experimental import pallas as pl
from jax.experimental.pallas import tpu as pltpu
from jax.sharding import PartitionSpec as P

MESH = pl.DeviceIdType.MESH


def layer_norm(values, gain, shift):
    center = values - jnp.mean(values, axis=-1, keepdims=True)
    variance = jnp.mean(center * center, axis=-1, keepdims=True)
    return center * lax.rsqrt(variance + 1e-05) * gain + shift


def kernel(
    sizes,
    res_ref,
    hid_ref,
    down_ref,
    mix_ref,
    gain_ref,
    shift_ref,
    gate_ref,
    up_ref,
    mixed_ref,
    out_ref,
    down_all,
    host_all,
    each_all,
    spread,
    part,
    red,
    mixed_all,
    host_acc,
    each_acc,
    back,
    load_sem,
    d_send,
    d_recv,
    h_send,
    h_recv,
    e_send,
    e_recv,
    a_send,
    a_recv,
    r_send,
    r_recv,
    m_send,
    m_recv,
    g_send,
    g_recv,
    b_send,
    b_recv,
):
    n_grp, n_fs, n_tp, sub = sizes
    shared = host_all.shape[3]
    g, f, t = lax.axis_index("grp"), lax.axis_index("fs"), lax.axis_index("tp")
    rows = res_ref.shape[0]
    width = gate_ref.shape[1]
    depth = gate_ref.shape[0]
    chunks = n_grp * sub

    def hid_block(peer):
        if len(hid_ref.shape) == 3:
            return hid_ref.at[peer]
        return hid_ref.at[:, pl.ds(pl.multiple_of(peer * width, width), width)]

    def own_rows(peer):
        return pl.ds(pl.multiple_of(peer * rows, rows), rows)

    load_down = pltpu.make_async_copy(down_ref, down_all.at[f], load_sem.at[0])
    loads = []
    for mat, ref in enumerate((gate_ref, up_ref)):
        loads.append(
            pltpu.make_async_copy(
                ref.at[:, pl.ds(0, shared)], host_all.at[f, mat], load_sem.at[1 + mat]
            )
        )
        loads.append(
            pltpu.make_async_copy(
                ref.at[:, pl.ds(shared, width - shared)], each_all.at[f, mat], load_sem.at[4 + mat]
            )
        )
    load_hid = pltpu.make_async_copy(hid_block(t), spread.at[own_rows(t)], load_sem.at[3])
    load_down.start()
    load_hid.start()
    for load in loads:
        load.start()

    lower = 2 * (f // 2)
    half = n_fs // 2
    host = lower + jnp.where(lower + 1 < half, 1, 0)
    is_host = f == host
    other = 2 * lower + 1 - f
    low_host = 1 if half > 1 else 0
    high_host = 2 * ((n_fs - 1) // 2)

    barrier = pltpu.get_barrier_semaphore()

    def greet(device):
        pl.semaphore_signal(barrier, inc=1, device_id=device, device_id_type=MESH)

    for d in range(1, n_grp):
        greet({"grp": lax.rem(g + d, n_grp)})
    for d in range(1, n_tp):
        greet({"tp": lax.rem(t + d, n_tp)})

    @pl.when(f > 0)
    def _():
        greet({"fs": f - 1})

    @pl.when(f < n_fs - 1)
    def _():
        greet({"fs": f + 1})

    inner = jnp.minimum(f, 1) + jnp.minimum(n_fs - 1 - f, 1)
    pl.semaphore_wait(barrier, n_grp - 1 + n_tp - 1 + inner)

    def block_copy(all_refs, send, recv):
        def copy(src, chunk, way, device):
            blocks = all_refs(src)
            size = blocks.shape[0] // chunks
            block = blocks.at[pl.ds(pl.multiple_of(chunk * size, size), size)]
            return pltpu.make_async_remote_copy(
                src_ref=block,
                dst_ref=block,
                send_sem=send(src).at[way, chunk],
                recv_sem=recv(src).at[chunk],
                device_id=device,
                device_id_type=MESH,
            )

        return copy

    def weight(refs, send, recv, mat):
        return block_copy(
            lambda src: refs.at[src, mat],
            lambda src: send.at[2 * src + mat],
            lambda src: recv.at[2 * src + mat],
        )

    def start(copy):
        copy.start()

    def wait_send(copy):
        copy.wait_send()

    class Gather:
        def __init__(self, copies, low, high, whole, needs):
            self.copies, self.low, self.high = copies, low, high
            self.whole, self.needs = whole, needs

        def whole_up(self, plane):
            return (2 * plane < n_fs) & self.whole

        def whole_down(self, plane):
            return (2 * plane >= n_fs) & self.whole

        def reached(self, plane):
            return (plane >= self.low) & (plane <= self.high)

        def along(self, copy, src, chunk, act, mine):
            up = (src <= f) & self.reached(f + 1)
            down = (src >= f) & self.reached(f - 1)
            if not mine:
                up = up & self.whole_up(f + 1)
                down = down & self.whole_down(f - 1)

            @pl.when(up)
            def _():
                act(copy(src, chunk, 0, {"fs": f + 1}))

            @pl.when(down)
            def _():
                act(copy(src, chunk, 1, {"fs": f - 1}))

        def all_along(self, src, act):
            for j in range(sub):
                for copy in self.copies:
                    self.along(copy, src, g * sub + j, act, True)
            if self.whole:
                for d in range(1, n_grp):
                    for j in range(sub):
                        for copy in self.copies:
                            chunk = lax.rem(g + d, n_grp) * sub + j
                            self.along(copy, src, chunk, act, False)

        def across(self, copy, src, chunk, act):
            for d in range(1, n_grp):
                act(copy(src, chunk, 1 + d, {"grp": lax.rem(g + d, n_grp)}))

        def whole_in(self, src):
            return ((src < f) & self.whole_up(f)) | ((src > f) & self.whole_down(f))

        def comes(self, src):
            return (src >= 0) & (src < n_fs) & (src != f) & self.reached(f)

        def swaps(self, src):
            return self.comes(src) & self.needs & jnp.logical_not(self.whole_in(src))

        def take(self, src):
            @pl.when(self.comes(src))
            def _():
                for j in range(sub):
                    for copy in self.copies:
                        chunk = g * sub + j
                        copy(src, chunk, 0, {"fs": other}).wait_recv()
                        self.along(copy, src, chunk, start, True)

                        @pl.when(self.swaps(src))
                        def _():
                            self.across(copy, src, chunk, start)

            if self.whole:

                @pl.when(self.comes(src) & self.whole_in(src))
                def _():
                    for d in range(1, n_grp):
                        for j in range(sub):
                            for copy in self.copies:
                                chunk = lax.rem(g + d, n_grp) * sub + j
                                copy(src, chunk, 0, {"fs": other}).wait_recv()
                                self.along(copy, src, chunk, start, False)

        def take_across(self, src):
            @pl.when(self.swaps(src))
            def _():
                for d in range(1, n_grp):
                    for j in range(sub):
                        for copy in self.copies:
                            chunk = lax.rem(g + d, n_grp) * sub + j
                            copy(src, chunk, 0, {"fs": other}).wait_recv()

        def drain(self, src):
            @pl.when((src == f) | self.comes(src))
            def _():
                if self.whole:
                    @pl.when((src == f) | self.whole_in(src))
                    def _():
                        for d in range(1, n_grp):
                            for j in range(sub):
                                for copy in self.copies:
                                    chunk = lax.rem(g + d, n_grp) * sub + j
                                    self.along(copy, src, chunk, wait_send, False)
                for j in range(sub):
                    for copy in self.copies:
                        self.along(copy, src, g * sub + j, wait_send, True)

            @pl.when(self.swaps(src))
            def _():
                for j in range(sub):
                    for copy in self.copies:
                        self.across(copy, src, g * sub + j, wait_send)

    def source(k):
        return f + (1 - 2 * lax.rem(k, 2)) * ((k + 1) // 2)

    def valid(src):
        return (src >= 0) & (src < n_fs)

    d_copy = block_copy(
        lambda src: down_all.at[src], lambda src: d_send.at[src], lambda src: d_recv.at[src]
    )
    down = Gather([d_copy], 0, n_fs - 1, False, True)
    hosted = Gather(
        [weight(host_all, h_send, h_recv, mat) for mat in range(2)],
        low_host,
        high_host,
        True,
        is_host,
    )
    each = Gather(
        [weight(each_all, e_send, e_recv, mat) for mat in range(2)], 0, n_fs - 1, True, True
    )

    def a_copy(d):
        peer = lax.rem(t + d, n_tp)
        return pltpu.make_async_remote_copy(
            src_ref=hid_block(peer),
            dst_ref=spread.at[own_rows(t)],
            send_sem=a_send.at[d],
            recv_sem=a_recv.at[d],
            device_id={"tp": peer},
            device_id_type=MESH,
        )

    def r_copy(src, d):
        peer = lax.rem(t + d, n_tp)
        return pltpu.make_async_remote_copy(
            src_ref=part.at[src, own_rows(peer)],
            dst_ref=red.at[d, src],
            send_sem=r_send.at[d, src],
            recv_sem=r_recv.at[d, src],
            device_id={"tp": peer},
            device_id_type=MESH,
        )

    core = lax.rem(t, 2)
    sibling = t + 1 - 2 * core

    def m_copy(owner, whose, hop):
        peer = sibling if hop == 0 else lax.rem(t + 2 * hop, n_tp)
        place = mixed_all.at[whose, own_rows(owner)]
        return pltpu.make_async_remote_copy(
            src_ref=place,
            dst_ref=place,
            send_sem=m_send.at[whose, owner, hop],
            recv_sem=m_recv.at[whose, owner],
            device_id={"tp": peer},
            device_id_type=MESH,
        )

    chips = n_tp // 2

    def m_out(whose):
        for hop in list(range(1, chips)) + [0]:
            m_copy(t, whose, hop).start()

    def m_relay(whose):
        for hop in range(1, chips):
            owner = lax.rem(t + 2 * hop, n_tp)
            m_copy(owner, whose, 0).wait_recv()
            m_copy(owner, whose, 0).start()

    def m_rest(whose):
        for hop in range(chips):
            m_copy(lax.rem(sibling + 2 * hop, n_tp), whose, 0).wait_recv()

    def m_drain(whose):
        for hop in range(chips):
            m_copy(t, whose, hop).wait_send()
        for hop in range(1, chips):
            m_copy(lax.rem(t + 2 * hop, n_tp), whose, 0).wait_send()

    def g_copy():
        return pltpu.make_async_remote_copy(
            src_ref=mixed_all.at[0, own_rows(t)],
            dst_ref=mixed_all.at[1, own_rows(t)],
            send_sem=g_send.at[0],
            recv_sem=g_recv.at[0],
            device_id={"fs": other},
            device_id_type=MESH,
        )

    tiles = 2
    tile = n_tp * rows // tiles

    def tile_rows(i):
        return pl.ds(pl.multiple_of(i * tile, tile), tile)

    def b_copy(i):
        return pltpu.make_async_remote_copy(
            src_ref=back.at[tile_rows(i)],
            dst_ref=out_ref.at[tile_rows(i), pl.ds(0, shared)],
            send_sem=b_send.at[i],
            recv_sem=b_recv.at[i],
            device_id={"fs": other},
            device_id_type=MESH,
        )

    load_down.wait()
    down.all_along(f, start)
    for d in range(1, n_tp):
        a_copy(d).start()
    for load in loads:
        load.wait()
    load_hid.wait()

    @pl.when(jnp.logical_not(is_host))
    def _():
        hosted.all_along(f, start)

    def first_half(k, carry):
        src = source(k)

        down.take(src)

        @pl.when((k == 2 * n_fs - 2) & is_host)
        def _():
            hosted.all_along(f, start)

        @pl.when(k == 2)
        def _():
            for d in range(1, n_tp):
                a_copy(d).wait_recv()

        done = source(k - 2)

        @pl.when((k >= 2) & valid(done))
        def _():
            down.take_across(done)
            part[done] = jnp.dot(
                spread[...], down_all[done], preferred_element_type=jnp.float32
            ).astype(jnp.bfloat16)
            for d in range(1, n_tp):
                r_copy(done, d).start()

        return carry

    lax.fori_loop(1, 2 * n_fs + 1, first_half, 0)

    for src in range(n_fs):
        for d in range(1, n_tp):
            r_copy(src, d).wait_recv()
    pieces = []
    for src in range(n_fs):
        total = part[src, own_rows(t)].astype(jnp.float32)
        for d in range(1, n_tp):
            total = total + red[d, src].astype(jnp.float32)
        pieces.append(total)
    branch = jnp.concatenate(pieces, axis=1)
    first = layer_norm(
        jnp.sqrt(2.0) * res_ref[...].astype(jnp.float32) + 0.5 * branch,
        gain_ref[0:1],
        shift_ref[0:1],
    )
    mixed = layer_norm(
        jnp.sqrt(2.0) * first + mix_ref[...].astype(jnp.float32), gain_ref[1:2], shift_ref[1:2]
    ).astype(jnp.bfloat16)
    mixed_all[0, own_rows(t)] = mixed
    mixed_ref[...] = mixed

    @pl.when(jnp.logical_not(is_host))
    def _():
        g_copy().start()

    m_out(0)

    @pl.when(jnp.logical_not(is_host))
    def _():
        each.all_along(f, start)

    def take_hosted(k, carry):
        hosted.take(source(k))
        return carry

    lax.fori_loop(1, 2 * n_fs - 1, take_hosted, 0)

    @pl.when(is_host)
    def _():
        each.all_along(f, start)

    m_relay(0)

    @pl.when(is_host)
    def _():
        g_copy().wait_recv()
        m_out(1)

    def take_each(k, carry):
        each.take(source(k))
        return carry

    lax.fori_loop(1, 3, take_each, 0)
    m_rest(0)

    def products(whose, span, gather, refs, total):
        total[...] = jnp.zeros_like(total)

        def add(k, carry):
            src = source(k)

            @pl.when(valid(src))
            def _():
                if gather is not None:
                    gather.take_across(src)
                here = pl.ds(pl.multiple_of(src * depth, depth), depth)
                for mat in range(2):
                    total[mat] += jnp.dot(
                        mixed_all[whose, span, here],
                        refs[src, mat],
                        preferred_element_type=jnp.float32,
                    )

            return carry

        lax.fori_loop(0, 2 * n_fs - 1, add, 0)
        gate = total[0]
        return (gate / (1.0 + jnp.exp(-gate)) * total[1]).astype(jnp.bfloat16)

    everything = pl.ds(0, n_tp * rows)

    @pl.when(is_host)
    def _():
        m_relay(1)
        out_ref[:, pl.ds(0, shared)] = products(0, everything, hosted, host_all, host_acc)

    lax.fori_loop(3, 2 * n_fs - 1, take_each, 0)

    @pl.when(is_host)
    def _():
        m_rest(1)

        def serve(i, carry):
            back[tile_rows(i)] = products(
                1, tile_rows(i), None, host_all, host_acc.at[:, pl.ds(0, tile)]
            )
            b_copy(i).start()
            return carry

        lax.fori_loop(0, tiles, serve, 0)

    out_ref[:, pl.ds(shared, width - shared)] = products(0, everything, each, each_all, each_acc)

    @pl.when(is_host)
    def _():
        for i in range(tiles):
            b_copy(i).wait_send()
        m_drain(1)

    @pl.when(jnp.logical_not(is_host))
    def _():
        g_copy().wait_send()
        for i in range(tiles):
            b_copy(i).wait_recv()

    m_drain(0)
    for d in range(1, n_tp):
        a_copy(d).wait_send()
        for src in range(n_fs):
            r_copy(src, d).wait_send()

    def drain(src, carry):
        for gather in (down, hosted, each):
            gather.drain(src)
        return carry

    lax.fori_loop(0, n_fs, drain, 0)


def paired_kernel(
    sizes,
    res_ref,
    hid_ref,
    down_ref,
    mix_ref,
    gain_ref,
    shift_ref,
    gate_ref,
    up_ref,
    mixed_ref,
    out_ref,
    down_all,
    cols_all,
    spread,
    part,
    red,
    mixed_all,
    back,
    result,
    load_sem,
    d_send,
    d_recv,
    d_late,
    c_send,
    c_recv,
    c_late,
    a_sem,
    r_sem,
    m_send,
    m_recv,
    m_late,
    g_send,
    g_recv,
    b_send,
    b_recv,
    w_sem,
):
    n_grp, n_fs, n_tp, sub, own, pieces = sizes
    g, f, t = lax.axis_index("grp"), lax.axis_index("fs"), lax.axis_index("tp")
    rows = res_ref.shape[0]
    width = gate_ref.shape[1]
    depth = gate_ref.shape[0]
    n_col = cols_all.shape[0]
    lanes = width // n_col

    lower = 2 * (f // 2)
    mate = 2 * lower + 1 - f
    inner = (f > 0) & (f < n_fs - 1)
    outer = jnp.logical_not(inner)
    facing = n_fs - 1 - jnp.where(inner, f, mate)
    beyond = n_fs - 1 - jnp.where(inner, mate, f)

    def hid_block(peer):
        return hid_ref.at[:, pl.ds(pl.multiple_of(peer * width, width), width)]

    def own_rows(peer):
        return pl.ds(pl.multiple_of(peer * rows, rows), rows)

    load_down = pltpu.make_async_copy(down_ref, down_all.at[f], load_sem.at[0])
    load_hid = pltpu.make_async_copy(hid_block(t), spread.at[own_rows(t)], load_sem.at[1])

    def load_col(c, mat):
        return pltpu.make_async_copy(
            (gate_ref, up_ref)[mat].at[:, pl.ds(pl.multiple_of(c * lanes, lanes), lanes)],
            cols_all.at[c, f, :, pl.ds(mat * lanes, lanes)],
            load_sem.at[2],
        )

    load_down.start()
    load_hid.start()

    def each(low, high, act):
        def body(c, carry):
            act(c)
            return carry

        lax.fori_loop(low, high, body, 0)

    def load_cols(c):
        for mat in range(2):
            load_col(c, mat).start()

    def ended(ref, sem):
        pltpu.make_async_copy(ref, ref, sem).wait()

    each(0, n_col, load_cols)

    barrier = pltpu.get_barrier_semaphore()

    def greet(device):
        pl.semaphore_signal(barrier, inc=1, device_id=device, device_id_type=MESH)

    for d in range(1, n_grp):
        greet({"grp": lax.rem(g + d, n_grp)})
    for d in range(1, n_tp):
        greet({"tp": lax.rem(t + d, n_tp)})
    greet({"fs": mate})

    @pl.when(inner)
    def _():
        greet({"fs": facing})

    with jax.named_scope("barrier"):
        pl.semaphore_wait(barrier, n_grp - 1 + n_tp - 1 + 1 + inner.astype(jnp.int32))

    MAIN, OUT, ACROSS = 0, 1, 2

    def device_of(way):
        if way == MAIN:
            return {"fs": jnp.where(inner, facing, mate)}
        if way == OUT:
            return {"fs": mate}
        return {"grp": lax.rem(g + way - ACROSS + 1, n_grp)}

    def d_place(src, share, j):
        size = down_all.shape[1] // (n_grp * sub)
        return down_all.at[src, pl.ds(pl.multiple_of((share * sub + j) * size, size), size)]

    def d_copy(src, share, j, way, sem):
        block = d_place(src, share, j)
        return pltpu.make_async_remote_copy(
            src_ref=block,
            dst_ref=block,
            send_sem=d_send.at[way],
            recv_sem=sem,
            device_id=device_of(way),
            device_id_type=MESH,
        )

    def c_copy(c, src, share, way, sem):
        size = depth // n_grp
        block = cols_all.at[c, src, pl.ds(pl.multiple_of(share * size, size), size)]
        return pltpu.make_async_remote_copy(
            src_ref=block,
            dst_ref=block,
            send_sem=c_send.at[way],
            recv_sem=sem,
            device_id=device_of(way),
            device_id_type=MESH,
        )

    d_half = down_all.shape[1] // n_grp
    c_half = depth // n_grp

    across = [ACROSS + d - 1 for d in range(1, n_grp)]
    others = [lax.rem(g + d, n_grp) for d in range(1, n_grp)]

    def d_send_on(src, j, ways):
        for way in ways:
            sem = d_recv.at[src, j] if way in (MAIN, OUT) else d_late.at[src]
            d_copy(src, g, j, way, sem).start()

    def d_send_late(src, share, j):
        d_copy(src, share, j, MAIN, d_late.at[src]).start()

    def c_send_on(c, src, ways):
        for way in ways:
            sem = c_recv.at[src, c] if way in (MAIN, OUT) else c_late.at[c]
            c_copy(c, src, g, way, sem).start()

    def c_send_late(c, src, share):
        c_copy(c, src, share, MAIN, c_late.at[c]).start()

    def d_pass(src, j, ways):
        d_copy(src, g, j, MAIN, d_recv.at[src, j]).wait_recv()
        d_send_on(src, j, ways)

    def c_pass(c, src, ways):
        c_copy(c, src, g, MAIN, c_recv.at[src, c]).wait_recv()
        c_send_on(c, src, ways)

    def d_rest(src):
        ended(down_all.at[src, pl.ds(0, (n_grp - 1) * d_half)], d_late.at[src])

    def c_rest(c):
        ended(cols_all.at[c, pl.ds(0, n_fs - 1), pl.ds(0, (n_grp - 1) * c_half)], c_late.at[c])

    def a_copy(d):
        peer = lax.rem(t + d, n_tp)
        return pltpu.make_async_remote_copy(
            src_ref=hid_block(peer),
            dst_ref=spread.at[own_rows(t)],
            send_sem=a_sem.at[0],
            recv_sem=a_sem.at[1],
            device_id={"tp": peer},
            device_id_type=MESH,
        )

    def r_copy(src, d):
        peer = lax.rem(t + d, n_tp)
        return pltpu.make_async_remote_copy(
            src_ref=part.at[src, own_rows(peer)],
            dst_ref=red.at[d, src],
            send_sem=r_sem.at[0],
            recv_sem=r_sem.at[1],
            device_id={"tp": peer},
            device_id_type=MESH,
        )

    core = lax.rem(t, 2)
    sibling = t + 1 - 2 * core
    chips = n_tp // 2
    piece = rows // pieces

    def piece_rows(owner, q):
        return pl.ds(pl.multiple_of(owner * rows + q * piece, piece), piece)

    def m_copy(owner, whose, hop, q):
        peer = sibling if hop == 0 else lax.rem(t + 2 * hop, n_tp)
        place = mixed_all.at[whose, piece_rows(owner, q)]
        return pltpu.make_async_remote_copy(
            src_ref=place,
            dst_ref=place,
            send_sem=m_send.at[whose],
            recv_sem=m_late.at[whose] if hop == 0 else m_recv.at[whose, owner // 2, q],
            device_id={"tp": peer},
            device_id_type=MESH,
        )

    def m_out(whose, q):
        for hop in list(range(1, chips)) + [0]:
            m_copy(t, whose, hop, q).start()

    def m_relay(whose, q):
        for hop in range(1, chips):
            owner = lax.rem(t + 2 * hop, n_tp)
            m_copy(owner, whose, hop, q).wait_recv()
            m_copy(owner, whose, 0, q).start()

    def m_rest(whose):
        ended(mixed_all.at[whose, pl.ds(0, chips * rows)], m_late.at[whose])

    def m_drain(whose):
        ended(mixed_all.at[whose, pl.ds(0, (2 * chips - 1) * rows)], m_send.at[whose])

    def g_copy(q):
        return pltpu.make_async_remote_copy(
            src_ref=mixed_all.at[0, piece_rows(t, q)],
            dst_ref=mixed_all.at[1, piece_rows(t, q)],
            send_sem=g_send.at[0],
            recv_sem=g_recv.at[q],
            device_id={"fs": mate},
            device_id_type=MESH,
        )

    def col_lanes(c):
        return pl.ds(pl.multiple_of(c * lanes, lanes), lanes)

    def b_copy(c):
        return pltpu.make_async_remote_copy(
            src_ref=back.at[c - own],
            dst_ref=result.at[:, col_lanes(c)],
            send_sem=b_send.at[0],
            recv_sem=b_recv.at[c - own],
            device_id={"fs": mate},
            device_id_type=MESH,
        )

    def w_copy(c):
        return pltpu.make_async_copy(
            result.at[:, col_lanes(c)], out_ref.at[:, col_lanes(c)], w_sem.at[0]
        )

    write_mixed = pltpu.make_async_copy(mixed_all.at[0, own_rows(t)], mixed_ref, w_sem.at[1])

    def first_product(src):
        part[src] = jnp.dot(
            spread[...], down_all[src], preferred_element_type=jnp.float32
        ).astype(jnp.bfloat16)
        for d in range(1, n_tp):
            r_copy(src, d).start()

    def take_hidden():
        load_hid.wait()
        ended(spread.at[pl.ds(0, (n_tp - 1) * rows)], a_sem.at[1])

    def norms():
        ended(red.at[pl.ds(1, n_tp - 1)], r_sem.at[1])
        columns = []
        for src in range(n_fs):
            total = part[src, own_rows(t)].astype(jnp.float32)
            for d in range(1, n_tp):
                total = total + red[d, src].astype(jnp.float32)
            columns.append(total)
        branch = jnp.concatenate(columns, axis=1)
        first = layer_norm(
            jnp.sqrt(2.0) * res_ref[...].astype(jnp.float32) + 0.5 * branch,
            gain_ref[0:1],
            shift_ref[0:1],
        )
        mixed = layer_norm(
            jnp.sqrt(2.0) * first + mix_ref[...].astype(jnp.float32),
            gain_ref[1:2],
            shift_ref[1:2],
        ).astype(jnp.bfloat16)
        mixed_all[0, own_rows(t)] = mixed

    def second_product(whose, c):
        weight = cols_all[c].reshape(n_fs * depth, 2 * lanes)
        total = jnp.dot(mixed_all[whose], weight, preferred_element_type=jnp.float32)
        gate = total[:, :lanes]
        return (gate / (1.0 + jnp.exp(-gate)) * total[:, lanes:]).astype(jnp.bfloat16)

    load_down.wait()

    @pl.when(inner)
    def _():
        each(0, sub, lambda j: d_send_on(f, j, (MAIN, OUT)))

    @pl.when(outer)
    def _():
        each(0, sub, lambda j: d_send_on(f, j, (MAIN,)))
        for share in others:
            each(0, sub, lambda j: d_send_late(f, share, j))

    for d in range(1, n_tp):
        a_copy(d).start()
    with jax.named_scope("loaded"):
        ended(cols_all.at[:, f], load_sem.at[2])

    @pl.when(outer)
    def _():
        each(0, n_col, lambda c: c_send_on(c, f, (MAIN,)))

    with jax.named_scope("first_pass"):

        @pl.when(inner)
        def _():
            def both(j):
                d_pass(mate, j, (MAIN,))
                d_pass(facing, j, [OUT] + across)

            each(0, sub, both)
            each(0, own, lambda c: c_send_on(c, f, (MAIN,)))

        @pl.when(outer)
        def _():
            each(0, sub, lambda j: d_pass(mate, j, across))

    with jax.named_scope("hidden"):
        take_hidden()

    def step(k, carry):
        with jax.named_scope("step_wait"):

            @pl.when((k == 1) & inner)
            def _():
                d_rest(facing)

            @pl.when((k == 1) & outer)
            def _():
                d_rest(mate)

            @pl.when((k == 2) & inner)
            def _():
                each(0, sub, lambda j: d_pass(beyond, j, [OUT] + across))
                each(0, own, lambda c: c_send_on(c, f, (OUT,)))
                d_rest(mate)

            @pl.when((k == 2) & outer)
            def _():
                each(0, sub, lambda j: d_pass(facing, j, across))
                d_rest(facing)

            @pl.when((k == 3) & inner)
            def _():
                c_pass(0, mate, (MAIN,))
                d_rest(beyond)

            @pl.when((k == 3) & outer)
            def _():
                each(0, sub, lambda j: d_pass(beyond, j, across))
                d_rest(beyond)

        second = jnp.where(inner, facing, mate)
        third = jnp.where(inner, mate, facing)
        with jax.named_scope("product"):
            first_product(
                jnp.where(k == 0, f, jnp.where(k == 1, second, jnp.where(k == 2, third, beyond)))
            )
        return carry

    lax.fori_loop(0, n_fs, step, 0)
    hosted = n_col - own
    slots = 2 * hosted

    @pl.when(inner)
    def _():
        def begin(c):
            @pl.when(c + 1 < own)
            def _():
                c_pass(c + 1, mate, (MAIN,))

            c_pass(c, facing, [OUT] + across)

        with jax.named_scope("begin"):
            each(0, own, begin)

    with jax.named_scope("norms"):
        norms()

    def serve(i):
        c = jnp.where(
            i < hosted - 1,
            own + i,
            jnp.where(i < hosted + 1, i - hosted + 1, jnp.where(i == hosted + 1, n_col - 1, i - hosted)),
        )
        with jax.named_scope("rest"):
            c_rest(c)

        @pl.when(c >= own)
        def _():
            with jax.named_scope("prod1"):
                back[c - own] = second_product(1, c)
            b_copy(c).start()

        with jax.named_scope("prod0"):
            result[:, col_lanes(c)] = second_product(0, c)
        w_copy(c).start()

    def feed(c):
        @pl.when(c < n_col)
        def _():
            c_send_on(c, f, (MAIN,))
            c_pass(c, mate, (MAIN,))

    def slot(s):
        c = own + s // 2
        src = jnp.where(s % 2 == 0, facing, beyond)

        @pl.when(s % 2 == 0)
        def _():
            feed(c + 2)

        with jax.named_scope("slot"):
            c_pass(c, src, across)

        when = s - (slots - 14)

        @pl.when(when == 1)
        def _():
            with jax.named_scope("m0"):
                for q in range(pieces):
                    m_relay(0, q)

        for q in range(pieces):

            @pl.when(when == 3 + q)
            def _():
                with jax.named_scope("from_mate"):
                    g_copy(q).wait_recv()
                    m_out(1, q)

            @pl.when(when == min(6 + q // 2 + q // 3, 8))
            def _():
                with jax.named_scope("m1"):
                    m_relay(1, q)

        @pl.when(when == 8)
        def _():
            with jax.named_scope("m_rest"):
                m_rest(0)
                m_rest(1)

        done = jnp.maximum(when - 8, 0)
        more = jnp.where(when == 13, n_col, jnp.maximum(when - 7, 0))
        each(done, more, serve)

    @pl.when(inner)
    def _():
        for q in range(pieces):
            m_out(0, q)
        write_mixed.start()
        feed(own)
        feed(own + 1)
        with jax.named_scope("beyond_own"):
            each(0, own, lambda c: c_pass(c, beyond, [OUT] + across))
        each(0, slots, slot)

    @pl.when(outer)
    def _():
        for q in range(pieces):
            g_copy(q).start()
            m_out(0, q)
        write_mixed.start()
        for share in others:
            each(own, n_col, lambda c: c_send_late(c, f, share))
            each(0, own, lambda c: c_send_late(c, f, share))

        def pass_own(c):
            with jax.named_scope("pass_own"):
                c_pass(c, mate, across)

        def pass_far(src):
            def act(c):
                with jax.named_scope("pass_far"):
                    c_pass(c, src, across)

            return act

        each(0, own, pass_own)
        each(0, own, pass_far(facing))
        with jax.named_scope("m0"):
            for q in range(pieces):
                m_relay(0, q)
            m_rest(0)
        each(0, own, pass_far(beyond))

        def make_own(c):
            with jax.named_scope("rest"):
                c_rest(c)
            with jax.named_scope("prod0"):
                result[:, col_lanes(c)] = second_product(0, c)
            w_copy(c).start()

        each(0, own, make_own)
        with jax.named_scope("b_wait"):

            def take_back(c):
                b_copy(c).wait_recv()
                w_copy(c).start()

            each(own, n_col, take_back)

    def d_sent(blocks, ways):
        for way in ways:
            ended(down_all.at[pl.ds(0, blocks), pl.ds(0, d_half)], d_send.at[way])

    def c_sent(columns, blocks, ways):
        for way in ways:
            ended(
                cols_all.at[pl.ds(0, columns), pl.ds(0, blocks), pl.ds(0, c_half)], c_send.at[way]
            )

    with jax.named_scope("drain"):
        ended(spread.at[pl.ds(0, (n_tp - 1) * rows)], a_sem.at[0])
        ended(red.at[pl.ds(1, n_tp - 1)], r_sem.at[0])
        m_drain(0)

        @pl.when(inner)
        def _():
            d_sent(2, (MAIN,))
            d_sent(3, (OUT,))
            d_sent(2, across)
            c_sent(n_col, 2, (MAIN,))
            c_sent(own, 3, (OUT,))
            c_sent(n_col, 2, across)
            m_drain(1)
            ended(back, b_send.at[0])

        @pl.when(outer)
        def _():
            ended(down_all.at[f], d_send.at[MAIN])
            ended(cols_all.at[:, f], c_send.at[MAIN])
            d_sent(3, across)
            c_sent(own, 3, across)
            ended(mixed_all.at[0, own_rows(t)], g_send.at[0])

    with jax.named_scope("written"):
        write_mixed.wait()
        ended(result, w_sem.at[0])


def paired_call(sizes, arguments):
    n_grp, n_fs, n_tp = sizes
    residual_in, hidden_first, down_weight, _, _, _, gate_weight, _ = arguments
    rows, model = residual_in.shape
    depth, width = gate_weight.shape
    cols = down_weight.shape[1]
    tokens = rows * n_tp
    lanes = 128
    n_col = width // lanes
    share = down_weight.shape[0] // (n_grp * 16)
    sub = max(n for n in range(1, 12) if share % n == 0)
    own = n_col * 4 // 11
    pieces = 4
    vmem = pl.BlockSpec(memory_space=pltpu.VMEM)
    anywhere = pl.BlockSpec(memory_space=pl.ANY)
    dma = pltpu.SemaphoreType.DMA
    return pl.pallas_call(
        functools.partial(paired_kernel, (n_grp, n_fs, n_tp, sub, own, pieces)),
        out_shape=(
            jax.ShapeDtypeStruct((rows, model), jnp.bfloat16),
            jax.ShapeDtypeStruct((tokens, width), jnp.bfloat16),
        ),
        in_specs=[vmem, anywhere, anywhere, vmem, vmem, vmem, anywhere, anywhere],
        out_specs=(anywhere, anywhere),
        scratch_shapes=[
            pltpu.VMEM((n_fs,) + down_weight.shape, jnp.bfloat16),
            pltpu.VMEM((n_col, n_fs, depth, 2 * lanes), jnp.bfloat16),
            pltpu.VMEM((tokens, width), jnp.bfloat16),
            pltpu.VMEM((n_fs, tokens, cols), jnp.bfloat16),
            pltpu.VMEM((n_tp, n_fs, rows, cols), jnp.bfloat16),
            pltpu.VMEM((2, tokens, model), jnp.bfloat16),
            pltpu.VMEM((n_col - own, tokens, lanes), jnp.bfloat16),
            pltpu.VMEM((tokens, width), jnp.bfloat16),
            dma((3,)),
            dma((1 + n_grp,)),
            dma((n_fs, sub)),
            dma((n_fs,)),
            dma((1 + n_grp,)),
            dma((n_fs, n_col)),
            dma((n_col,)),
            dma((2,)),
            dma((2,)),
            dma((2,)),
            dma((2, n_tp // 2, pieces)),
            dma((2,)),
            dma((1,)),
            dma((pieces,)),
            dma((1,)),
            dma((n_col - own,)),
            dma((2,)),
        ],
        compiler_params=pltpu.CompilerParams(
            collective_id=0, has_side_effects=True, vmem_limit_bytes=60 * 1024 * 1024
        ),
        name="paired_half_steps",
    )(*arguments)


def fits_pairs(sizes, residual_in, down_weight, gate_weight):
    n_grp, n_fs, n_tp = sizes
    depth, width = gate_weight.shape
    return (
        n_fs == 4
        and n_tp % 2 == 0
        and width % 128 == 0
        and width // 128 >= 10
        and depth % (n_grp * 32) == 0
        and down_weight.shape[0] % (n_grp * 16) == 0
        and residual_in.shape[0] % (4 * 16) == 0
    )


def on_device(
    sizes,
    residual_in,
    hidden_first,
    down_weight,
    mixer_out,
    norm_gain,
    norm_shift,
    gate_weight,
    up_weight,
):
    if fits_pairs(sizes, residual_in, down_weight, gate_weight):
        arguments = (
            residual_in,
            hidden_first,
            down_weight,
            mixer_out,
            norm_gain,
            norm_shift,
            gate_weight,
            up_weight,
        )
        return paired_call(sizes, arguments)
    n_grp, n_fs, n_tp = sizes
    rows, model = residual_in.shape
    depth, width = gate_weight.shape
    cols = down_weight.shape[1]
    sub = 1
    if depth % (n_grp * 2 * 32) == 0 and down_weight.shape[0] % (n_grp * 2 * 32) == 0:
        sub = 2
    chunks = n_grp * sub
    each = max(1, width * 3 // (11 * 128)) * 128
    shared = (width - each) // 128 * 128
    each = width - shared
    if width % 128:
        hidden_first = hidden_first.reshape(rows, n_tp, width).transpose(1, 0, 2)
    vmem = pl.BlockSpec(memory_space=pltpu.VMEM)
    anywhere = pl.BlockSpec(memory_space=pl.ANY)
    dma = pltpu.SemaphoreType.DMA
    tokens = rows * n_tp
    return pl.pallas_call(
        functools.partial(kernel, (n_grp, n_fs, n_tp, sub)),
        out_shape=(
            jax.ShapeDtypeStruct((rows, model), jnp.bfloat16),
            jax.ShapeDtypeStruct((tokens, width), jnp.bfloat16),
        ),
        in_specs=[vmem, anywhere, anywhere, vmem, vmem, vmem, anywhere, anywhere],
        out_specs=(vmem, vmem),
        scratch_shapes=[
            pltpu.VMEM((n_fs,) + down_weight.shape, jnp.bfloat16),
            pltpu.VMEM((n_fs, 2, depth, shared), jnp.bfloat16),
            pltpu.VMEM((n_fs, 2, depth, each), jnp.bfloat16),
            pltpu.VMEM((tokens, width), jnp.bfloat16),
            pltpu.VMEM((n_fs, tokens, cols), jnp.bfloat16),
            pltpu.VMEM((n_tp, n_fs, rows, cols), jnp.bfloat16),
            pltpu.VMEM((2, tokens, model), jnp.bfloat16),
            pltpu.VMEM((2, tokens, shared), jnp.float32),
            pltpu.VMEM((2, tokens, each), jnp.float32),
            pltpu.VMEM((tokens, shared), jnp.bfloat16),
            dma((6,)),
            dma((n_fs, 1 + n_grp, chunks)),
            dma((n_fs, chunks)),
            dma((2 * n_fs, 1 + n_grp, chunks)),
            dma((2 * n_fs, chunks)),
            dma((2 * n_fs, 1 + n_grp, chunks)),
            dma((2 * n_fs, chunks)),
            dma((n_tp,)),
            dma((n_tp,)),
            dma((n_tp, n_fs)),
            dma((n_tp, n_fs)),
            dma((2, n_tp, n_tp // 2)),
            dma((2, n_tp)),
            dma((1,)),
            dma((1,)),
            dma((2,)),
            dma((2,)),
        ],
        compiler_params=pltpu.CompilerParams(
            collective_id=0, has_side_effects=True, vmem_limit_bytes=60 * 1024 * 1024
        ),
        name="half_steps",
    )(
        residual_in,
        hidden_first,
        down_weight,
        mixer_out,
        norm_gain,
        norm_shift,
        gate_weight,
        up_weight,
    )


def solution(mesh):
    sizes = tuple(mesh.shape[axis] for axis in ("grp", "fs", "tp"))
    in_specs = (
        P(("grp", "fs", "tp"), None),
        P(("grp", "fs", "tp"), None),
        P("tp", "fs"),
        P(("grp", "fs", "tp"), None),
        P(),
        P(),
        P("fs", "tp"),
        P("fs", "tp"),
    )
    out_specs = (P(("grp", "fs", "tp"), None), P(("grp", "fs"), "tp"))
    return jax.shard_map(
        functools.partial(on_device, sizes),
        mesh=mesh,
        in_specs=in_specs,
        out_specs=out_specs,
        check_vma=False,
    )
```

```python
import functools

import jax
import jax.numpy as jnp
from jax import lax
from jax.experimental import pallas as pl
from jax.experimental.pallas import tpu as pltpu
from jax.sharding import PartitionSpec as P

MESH = pl.DeviceIdType.MESH


def layer_norm(values, gain, shift):
    center = values - jnp.mean(values, axis=-1, keepdims=True)
    variance = jnp.mean(center * center, axis=-1, keepdims=True)
    return center * lax.rsqrt(variance + 1e-05) * gain + shift


def kernel(
    sizes,
    res_ref,
    hid_ref,
    down_ref,
    mix_ref,
    gain_ref,
    shift_ref,
    gate_ref,
    up_ref,
    mixed_ref,
    out_ref,
    down_all,
    host_all,
    each_all,
    spread,
    part,
    red,
    mixed_all,
    host_acc,
    each_acc,
    back,
    load_sem,
    d_send,
    d_recv,
    h_send,
    h_recv,
    e_send,
    e_recv,
    a_send,
    a_recv,
    r_send,
    r_recv,
    m_send,
    m_recv,
    g_send,
    g_recv,
    b_send,
    b_recv,
):
    n_grp, n_fs, n_tp, sub = sizes
    shared = host_all.shape[3]
    g, f, t = lax.axis_index("grp"), lax.axis_index("fs"), lax.axis_index("tp")
    rows = res_ref.shape[0]
    width = gate_ref.shape[1]
    depth = gate_ref.shape[0]
    chunks = n_grp * sub

    def hid_block(peer):
        if len(hid_ref.shape) == 3:
            return hid_ref.at[peer]
        return hid_ref.at[:, pl.ds(pl.multiple_of(peer * width, width), width)]

    def own_rows(peer):
        return pl.ds(pl.multiple_of(peer * rows, rows), rows)

    load_down = pltpu.make_async_copy(down_ref, down_all.at[f], load_sem.at[0])
    loads = []
    for mat, ref in enumerate((gate_ref, up_ref)):
        loads.append(
            pltpu.make_async_copy(
                ref.at[:, pl.ds(0, shared)], host_all.at[f, mat], load_sem.at[1 + mat]
            )
        )
        loads.append(
            pltpu.make_async_copy(
                ref.at[:, pl.ds(shared, width - shared)], each_all.at[f, mat], load_sem.at[4 + mat]
            )
        )
    load_hid = pltpu.make_async_copy(hid_block(t), spread.at[own_rows(t)], load_sem.at[3])
    load_down.start()
    load_hid.start()
    for load in loads:
        load.start()

    lower = 2 * (f // 2)
    half = n_fs // 2
    host = lower + jnp.where(lower + 1 < half, 1, 0)
    is_host = f == host
    other = 2 * lower + 1 - f
    low_host = 1 if half > 1 else 0
    high_host = 2 * ((n_fs - 1) // 2)

    barrier = pltpu.get_barrier_semaphore()

    def greet(device):
        pl.semaphore_signal(barrier, inc=1, device_id=device, device_id_type=MESH)

    for d in range(1, n_grp):
        greet({"grp": lax.rem(g + d, n_grp)})
    for d in range(1, n_tp):
        greet({"tp": lax.rem(t + d, n_tp)})

    @pl.when(f > 0)
    def _():
        greet({"fs": f - 1})

    @pl.when(f < n_fs - 1)
    def _():
        greet({"fs": f + 1})

    inner = jnp.minimum(f, 1) + jnp.minimum(n_fs - 1 - f, 1)
    pl.semaphore_wait(barrier, n_grp - 1 + n_tp - 1 + inner)

    def block_copy(all_refs, send, recv):
        def copy(src, chunk, way, device):
            blocks = all_refs(src)
            size = blocks.shape[0] // chunks
            block = blocks.at[pl.ds(pl.multiple_of(chunk * size, size), size)]
            return pltpu.make_async_remote_copy(
                src_ref=block,
                dst_ref=block,
                send_sem=send(src).at[way, chunk],
                recv_sem=recv(src).at[chunk],
                device_id=device,
                device_id_type=MESH,
            )

        return copy

    def weight(refs, send, recv, mat):
        return block_copy(
            lambda src: refs.at[src, mat],
            lambda src: send.at[2 * src + mat],
            lambda src: recv.at[2 * src + mat],
        )

    def start(copy):
        copy.start()

    def wait_send(copy):
        copy.wait_send()

    class Gather:
        def __init__(self, copies, low, high, whole, needs):
            self.copies, self.low, self.high = copies, low, high
            self.whole, self.needs = whole, needs

        def whole_up(self, plane):
            return (2 * plane < n_fs) & self.whole

        def whole_down(self, plane):
            return (2 * plane >= n_fs) & self.whole

        def reached(self, plane):
            return (plane >= self.low) & (plane <= self.high)

        def along(self, copy, src, chunk, act, mine):
            up = (src <= f) & self.reached(f + 1)
            down = (src >= f) & self.reached(f - 1)
            if not mine:
                up = up & self.whole_up(f + 1)
                down = down & self.whole_down(f - 1)

            @pl.when(up)
            def _():
                act(copy(src, chunk, 0, {"fs": f + 1}))

            @pl.when(down)
            def _():
                act(copy(src, chunk, 1, {"fs": f - 1}))

        def all_along(self, src, act):
            for j in range(sub):
                for copy in self.copies:
                    self.along(copy, src, g * sub + j, act, True)
            if self.whole:
                for d in range(1, n_grp):
                    for j in range(sub):
                        for copy in self.copies:
                            chunk = lax.rem(g + d, n_grp) * sub + j
                            self.along(copy, src, chunk, act, False)

        def across(self, copy, src, chunk, act):
            for d in range(1, n_grp):
                act(copy(src, chunk, 1 + d, {"grp": lax.rem(g + d, n_grp)}))

        def whole_in(self, src):
            return ((src < f) & self.whole_up(f)) | ((src > f) & self.whole_down(f))

        def comes(self, src):
            return (src >= 0) & (src < n_fs) & (src != f) & self.reached(f)

        def swaps(self, src):
            return self.comes(src) & self.needs & jnp.logical_not(self.whole_in(src))

        def take(self, src):
            @pl.when(self.comes(src))
            def _():
                for j in range(sub):
                    for copy in self.copies:
                        chunk = g * sub + j
                        copy(src, chunk, 0, {"fs": other}).wait_recv()
                        self.along(copy, src, chunk, start, True)

                        @pl.when(self.swaps(src))
                        def _():
                            self.across(copy, src, chunk, start)

            if self.whole:

                @pl.when(self.comes(src) & self.whole_in(src))
                def _():
                    for d in range(1, n_grp):
                        for j in range(sub):
                            for copy in self.copies:
                                chunk = lax.rem(g + d, n_grp) * sub + j
                                copy(src, chunk, 0, {"fs": other}).wait_recv()
                                self.along(copy, src, chunk, start, False)

        def take_across(self, src):
            @pl.when(self.swaps(src))
            def _():
                for d in range(1, n_grp):
                    for j in range(sub):
                        for copy in self.copies:
                            chunk = lax.rem(g + d, n_grp) * sub + j
                            copy(src, chunk, 0, {"fs": other}).wait_recv()

        def drain(self, src):
            @pl.when((src == f) | self.comes(src))
            def _():
                if self.whole:
                    @pl.when((src == f) | self.whole_in(src))
                    def _():
                        for d in range(1, n_grp):
                            for j in range(sub):
                                for copy in self.copies:
                                    chunk = lax.rem(g + d, n_grp) * sub + j
                                    self.along(copy, src, chunk, wait_send, False)
                for j in range(sub):
                    for copy in self.copies:
                        self.along(copy, src, g * sub + j, wait_send, True)

            @pl.when(self.swaps(src))
            def _():
                for j in range(sub):
                    for copy in self.copies:
                        self.across(copy, src, g * sub + j, wait_send)

    def source(k):
        return f + (1 - 2 * lax.rem(k, 2)) * ((k + 1) // 2)

    def valid(src):
        return (src >= 0) & (src < n_fs)

    d_copy = block_copy(
        lambda src: down_all.at[src], lambda src: d_send.at[src], lambda src: d_recv.at[src]
    )
    down = Gather([d_copy], 0, n_fs - 1, False, True)
    hosted = Gather(
        [weight(host_all, h_send, h_recv, mat) for mat in range(2)],
        low_host,
        high_host,
        True,
        is_host,
    )
    each = Gather(
        [weight(each_all, e_send, e_recv, mat) for mat in range(2)], 0, n_fs - 1, True, True
    )

    def a_copy(d):
        peer = lax.rem(t + d, n_tp)
        return pltpu.make_async_remote_copy(
            src_ref=hid_block(peer),
            dst_ref=spread.at[own_rows(t)],
            send_sem=a_send.at[d],
            recv_sem=a_recv.at[d],
            device_id={"tp": peer},
            device_id_type=MESH,
        )

    def r_copy(src, d):
        peer = lax.rem(t + d, n_tp)
        return pltpu.make_async_remote_copy(
            src_ref=part.at[src, own_rows(peer)],
            dst_ref=red.at[d, src],
            send_sem=r_send.at[d, src],
            recv_sem=r_recv.at[d, src],
            device_id={"tp": peer},
            device_id_type=MESH,
        )

    core = lax.rem(t, 2)
    sibling = t + 1 - 2 * core

    def m_copy(owner, whose, hop):
        peer = sibling if hop == 0 else lax.rem(t + 2 * hop, n_tp)
        place = mixed_all.at[whose, own_rows(owner)]
        return pltpu.make_async_remote_copy(
            src_ref=place,
            dst_ref=place,
            send_sem=m_send.at[whose, owner, hop],
            recv_sem=m_recv.at[whose, owner],
            device_id={"tp": peer},
            device_id_type=MESH,
        )

    chips = n_tp // 2

    def m_out(whose):
        for hop in list(range(1, chips)) + [0]:
            m_copy(t, whose, hop).start()

    def m_relay(whose):
        for hop in range(1, chips):
            owner = lax.rem(t + 2 * hop, n_tp)
            m_copy(owner, whose, 0).wait_recv()
            m_copy(owner, whose, 0).start()

    def m_rest(whose):
        for hop in range(chips):
            m_copy(lax.rem(sibling + 2 * hop, n_tp), whose, 0).wait_recv()

    def m_drain(whose):
        for hop in range(chips):
            m_copy(t, whose, hop).wait_send()
        for hop in range(1, chips):
            m_copy(lax.rem(t + 2 * hop, n_tp), whose, 0).wait_send()

    def g_copy():
        return pltpu.make_async_remote_copy(
            src_ref=mixed_all.at[0, own_rows(t)],
            dst_ref=mixed_all.at[1, own_rows(t)],
            send_sem=g_send.at[0],
            recv_sem=g_recv.at[0],
            device_id={"fs": other},
            device_id_type=MESH,
        )

    tiles = 2
    tile = n_tp * rows // tiles

    def tile_rows(i):
        return pl.ds(pl.multiple_of(i * tile, tile), tile)

    def b_copy(i):
        return pltpu.make_async_remote_copy(
            src_ref=back.at[tile_rows(i)],
            dst_ref=out_ref.at[tile_rows(i), pl.ds(0, shared)],
            send_sem=b_send.at[i],
            recv_sem=b_recv.at[i],
            device_id={"fs": other},
            device_id_type=MESH,
        )

    load_down.wait()
    down.all_along(f, start)
    for d in range(1, n_tp):
        a_copy(d).start()
    for load in loads:
        load.wait()
    load_hid.wait()

    @pl.when(jnp.logical_not(is_host))
    def _():
        hosted.all_along(f, start)

    def first_half(k, carry):
        src = source(k)

        down.take(src)

        @pl.when((k == 2 * n_fs - 2) & is_host)
        def _():
            hosted.all_along(f, start)

        @pl.when(k == 2)
        def _():
            for d in range(1, n_tp):
                a_copy(d).wait_recv()

        done = source(k - 2)

        @pl.when((k >= 2) & valid(done))
        def _():
            down.take_across(done)
            part[done] = jnp.dot(
                spread[...], down_all[done], preferred_element_type=jnp.float32
            ).astype(jnp.bfloat16)
            for d in range(1, n_tp):
                r_copy(done, d).start()

        return carry

    lax.fori_loop(1, 2 * n_fs + 1, first_half, 0)

    for src in range(n_fs):
        for d in range(1, n_tp):
            r_copy(src, d).wait_recv()
    pieces = []
    for src in range(n_fs):
        total = part[src, own_rows(t)].astype(jnp.float32)
        for d in range(1, n_tp):
            total = total + red[d, src].astype(jnp.float32)
        pieces.append(total)
    branch = jnp.concatenate(pieces, axis=1)
    first = layer_norm(
        jnp.sqrt(2.0) * res_ref[...].astype(jnp.float32) + 0.5 * branch,
        gain_ref[0:1],
        shift_ref[0:1],
    )
    mixed = layer_norm(
        jnp.sqrt(2.0) * first + mix_ref[...].astype(jnp.float32), gain_ref[1:2], shift_ref[1:2]
    ).astype(jnp.bfloat16)
    mixed_all[0, own_rows(t)] = mixed
    mixed_ref[...] = mixed

    @pl.when(jnp.logical_not(is_host))
    def _():
        g_copy().start()

    m_out(0)

    @pl.when(jnp.logical_not(is_host))
    def _():
        each.all_along(f, start)

    def take_hosted(k, carry):
        hosted.take(source(k))
        return carry

    lax.fori_loop(1, 2 * n_fs - 1, take_hosted, 0)

    @pl.when(is_host)
    def _():
        each.all_along(f, start)

    m_relay(0)

    @pl.when(is_host)
    def _():
        g_copy().wait_recv()
        m_out(1)

    def take_each(k, carry):
        each.take(source(k))
        return carry

    lax.fori_loop(1, 3, take_each, 0)
    m_rest(0)

    def products(whose, span, gather, refs, total):
        total[...] = jnp.zeros_like(total)

        def add(k, carry):
            src = source(k)

            @pl.when(valid(src))
            def _():
                if gather is not None:
                    gather.take_across(src)
                here = pl.ds(pl.multiple_of(src * depth, depth), depth)
                for mat in range(2):
                    total[mat] += jnp.dot(
                        mixed_all[whose, span, here],
                        refs[src, mat],
                        preferred_element_type=jnp.float32,
                    )

            return carry

        lax.fori_loop(0, 2 * n_fs - 1, add, 0)
        gate = total[0]
        return (gate / (1.0 + jnp.exp(-gate)) * total[1]).astype(jnp.bfloat16)

    everything = pl.ds(0, n_tp * rows)

    @pl.when(is_host)
    def _():
        m_relay(1)
        out_ref[:, pl.ds(0, shared)] = products(0, everything, hosted, host_all, host_acc)

    lax.fori_loop(3, 2 * n_fs - 1, take_each, 0)

    @pl.when(is_host)
    def _():
        m_rest(1)

        def serve(i, carry):
            back[tile_rows(i)] = products(
                1, tile_rows(i), None, host_all, host_acc.at[:, pl.ds(0, tile)]
            )
            b_copy(i).start()
            return carry

        lax.fori_loop(0, tiles, serve, 0)

    out_ref[:, pl.ds(shared, width - shared)] = products(0, everything, each, each_all, each_acc)

    @pl.when(is_host)
    def _():
        for i in range(tiles):
            b_copy(i).wait_send()
        m_drain(1)

    @pl.when(jnp.logical_not(is_host))
    def _():
        g_copy().wait_send()
        for i in range(tiles):
            b_copy(i).wait_recv()

    m_drain(0)
    for d in range(1, n_tp):
        a_copy(d).wait_send()
        for src in range(n_fs):
            r_copy(src, d).wait_send()

    def drain(src, carry):
        for gather in (down, hosted, each):
            gather.drain(src)
        return carry

    lax.fori_loop(0, n_fs, drain, 0)


def paired_kernel(
    sizes,
    res_ref,
    hid_ref,
    down_ref,
    mix_ref,
    gain_ref,
    shift_ref,
    gate_ref,
    up_ref,
    mixed_ref,
    out_ref,
    down_all,
    cols_all,
    spread,
    part,
    red,
    mixed_all,
    back,
    res_now,
    mix_now,
    gain_now,
    shift_now,
    load_sem,
    d_send,
    d_recv,
    d_late,
    c_send,
    c_recv,
    c_late,
    a_sem,
    r_sem,
    m_send,
    m_recv,
    m_late,
    g_send,
    g_recv,
    b_send,
    b_recv,
):
    n_grp, n_fs, n_tp, sub, own, pieces, ahead, parts = sizes
    g, f, t = lax.axis_index("grp"), lax.axis_index("fs"), lax.axis_index("tp")
    rows = res_ref.shape[0]
    width = gate_ref.shape[1]
    depth = gate_ref.shape[0]
    n_col = cols_all.shape[0]
    lanes = width // n_col

    lower = 2 * (f // 2)
    mate = 2 * lower + 1 - f
    inner = (f > 0) & (f < n_fs - 1)
    outer = jnp.logical_not(inner)
    facing = n_fs - 1 - jnp.where(inner, f, mate)
    beyond = n_fs - 1 - jnp.where(inner, mate, f)

    def hid_block(peer):
        return hid_ref.at[:, pl.ds(pl.multiple_of(peer * width, width), width)]

    def own_rows(peer):
        return pl.ds(pl.multiple_of(peer * rows, rows), rows)

    load_down = pltpu.make_async_copy(down_ref, down_all.at[f], load_sem.at[0])
    load_hid = pltpu.make_async_copy(hid_block(t), spread.at[own_rows(t)], load_sem.at[1])

    def load_col(c, mat):
        return pltpu.make_async_copy(
            (gate_ref, up_ref)[mat].at[:, pl.ds(pl.multiple_of(c * lanes, lanes), lanes)],
            cols_all.at[c, f, :, pl.ds(mat * lanes, lanes)],
            load_sem.at[2],
        )

    load_down.start()
    load_hid.start()
    row_loads = [
        pltpu.make_async_copy(whole, now, load_sem.at[3 + k])
        for k, (whole, now) in enumerate(
            (
                (res_ref, res_now),
                (mix_ref, mix_now),
                (gain_ref, gain_now),
                (shift_ref, shift_now),
            )
        )
    ]
    for load in row_loads:
        load.start()

    def each(low, high, act):
        def body(c, carry):
            act(c)
            return carry

        lax.fori_loop(low, high, body, 0)

    def load_cols(c):
        for mat in range(2):
            load_col(c, mat).start()

    def ended(ref, sem):
        pltpu.make_async_copy(ref, ref, sem).wait()

    each(0, n_col, load_cols)

    barrier = pltpu.get_barrier_semaphore()

    def greet(device):
        pl.semaphore_signal(barrier, inc=1, device_id=device, device_id_type=MESH)

    for d in range(1, n_grp):
        greet({"grp": lax.rem(g + d, n_grp)})
    for d in range(1, n_tp):
        greet({"tp": lax.rem(t + d, n_tp)})
    greet({"fs": mate})

    @pl.when(inner)
    def _():
        greet({"fs": facing})

    with jax.named_scope("barrier"):
        pl.semaphore_wait(barrier, n_grp - 1 + n_tp - 1 + 1 + inner.astype(jnp.int32))

    MAIN, OUT, ACROSS = 0, 1, 2

    def device_of(way):
        if way == MAIN:
            return {"fs": jnp.where(inner, facing, mate)}
        if way == OUT:
            return {"fs": mate}
        return {"grp": lax.rem(g + way - ACROSS + 1, n_grp)}

    def d_place(src, share, j):
        size = down_all.shape[1] // (n_grp * sub)
        return down_all.at[src, pl.ds(pl.multiple_of((share * sub + j) * size, size), size)]

    def d_copy(src, share, j, way, sem):
        block = d_place(src, share, j)
        return pltpu.make_async_remote_copy(
            src_ref=block,
            dst_ref=block,
            send_sem=d_send.at[way],
            recv_sem=sem,
            device_id=device_of(way),
            device_id_type=MESH,
        )

    def c_copy(c, src, share, part_of, way, sem, count=None):
        whole = depth // n_grp
        size = whole if part_of is None else whole // parts
        start = share * whole + (0 if part_of is None else part_of * size)
        block = cols_all.at[c, src, pl.ds(pl.multiple_of(start, size), size)]
        return pltpu.make_async_remote_copy(
            src_ref=block,
            dst_ref=block,
            send_sem=c_send.at[way if count is None else count],
            recv_sem=sem,
            device_id=device_of(way),
            device_id_type=MESH,
        )

    def place_at(receiver, src):
        return src - (src > receiver).astype(jnp.int32)

    def receiver_of(way):
        return jnp.where(inner, facing, mate) if way == MAIN else mate

    def moved_copy(d):
        block = cols_all.at[own - 1, mate, pl.ds(pl.multiple_of(g * c_half, c_half), c_half)]
        return pltpu.make_async_remote_copy(
            src_ref=block,
            dst_ref=block,
            send_sem=c_send.at[ACROSS + n_grp - 2 + d],
            recv_sem=c_late.at[own - 1],
            device_id={"grp": lax.rem(g + d, n_grp)},
            device_id_type=MESH,
        )

    d_half = down_all.shape[1] // n_grp
    c_half = depth // n_grp

    across = [ACROSS + d - 1 for d in range(1, n_grp)]
    others = [lax.rem(g + d, n_grp) for d in range(1, n_grp)]

    def d_send_on(src, j, ways):
        for way in ways:
            if way in (MAIN, OUT):
                sem = d_recv.at[place_at(receiver_of(way), src), j]
            else:
                sem = d_late.at[src]
            d_copy(src, g, j, way, sem).start()

    def d_send_late(src, share, j):
        d_copy(src, share, j, MAIN, d_late.at[src]).start()

    def c_part_on(c, src, k, ways):
        for way in ways:
            if way in (MAIN, OUT):
                sem = c_recv.at[place_at(receiver_of(way), src), c * parts + k]
            else:
                sem = c_late.at[c]
            c_copy(c, src, g, k, way, sem).start()

    def c_send_on(c, src, ways):
        for k in range(parts):
            c_part_on(c, src, k, ways)

    def c_send_late(c, src, share):
        c_copy(c, src, share, None, MAIN, c_late.at[c], ACROSS + n_grp - 1).start()

    def d_pass(src, j, ways):
        d_copy(src, g, j, MAIN, d_recv.at[place_at(f, src), j]).wait_recv()
        d_send_on(src, j, ways)

    def c_pass(c, src, ways):
        for k in range(parts):
            sem = c_recv.at[place_at(f, src), c * parts + k]
            c_copy(c, src, g, k, MAIN, sem).wait_recv()
            c_part_on(c, src, k, ways)

    def d_rest(src):
        ended(down_all.at[src, pl.ds(0, (n_grp - 1) * d_half)], d_late.at[src])

    def c_rest(c):
        ended(cols_all.at[c, pl.ds(0, n_fs - 1), pl.ds(0, (n_grp - 1) * c_half)], c_late.at[c])

    def a_copy(d):
        peer = lax.rem(t + d, n_tp)
        return pltpu.make_async_remote_copy(
            src_ref=hid_block(peer),
            dst_ref=spread.at[own_rows(t)],
            send_sem=a_sem.at[0],
            recv_sem=a_sem.at[1],
            device_id={"tp": peer},
            device_id_type=MESH,
        )

    def r_copy(src, d):
        peer = lax.rem(t + d, n_tp)
        return pltpu.make_async_remote_copy(
            src_ref=part.at[src, own_rows(peer)],
            dst_ref=red.at[d, src],
            send_sem=r_sem.at[0],
            recv_sem=r_sem.at[1],
            device_id={"tp": peer},
            device_id_type=MESH,
        )

    core = lax.rem(t, 2)
    sibling = t + 1 - 2 * core
    chips = n_tp // 2
    piece = rows // pieces

    def piece_rows(owner, q):
        return pl.ds(pl.multiple_of(owner * rows + q * piece, piece), piece)

    def m_copy(owner, whose, hop, q):
        peer = sibling if hop == 0 else lax.rem(t + 2 * hop, n_tp)
        place = mixed_all.at[whose, piece_rows(owner, q)]
        return pltpu.make_async_remote_copy(
            src_ref=place,
            dst_ref=place,
            send_sem=m_send.at[whose],
            recv_sem=m_late.at[whose] if hop == 0 else m_recv.at[owner // 2, whose * (q + 1)],
            device_id={"tp": peer},
            device_id_type=MESH,
        )

    def m_out(whose, q):
        for hop in list(range(1, chips)) + [0]:
            m_copy(t, whose, hop, q).start()

    def m_relay(whose, q):
        for hop in range(1, chips):
            owner = lax.rem(t + 2 * hop, n_tp)
            m_copy(owner, whose, hop, q).wait_recv()
            m_copy(owner, whose, 0, q).start()

    def m_relay_all():
        for hop in range(1, chips):
            owner = lax.rem(t + 2 * hop, n_tp)
            ended(mixed_all.at[0, own_rows(owner)], m_recv.at[owner // 2, 0])
            for q in range(pieces):
                m_copy(owner, 0, 0, q).start()

    def m_rest(whose):
        ended(mixed_all.at[whose, pl.ds(0, chips * rows)], m_late.at[whose])

    def m_drain(whose):
        ended(mixed_all.at[whose, pl.ds(0, (2 * chips - 1) * rows)], m_send.at[whose])

    def g_copy(q):
        return pltpu.make_async_remote_copy(
            src_ref=mixed_all.at[0, piece_rows(t, q)],
            dst_ref=mixed_all.at[1, piece_rows(t, q)],
            send_sem=g_send.at[0],
            recv_sem=g_recv.at[q],
            device_id={"fs": mate},
            device_id_type=MESH,
        )

    def col_lanes(c):
        return pl.ds(pl.multiple_of(c * lanes, lanes), lanes)

    tile = n_tp * rows // 2

    def tile_rows(h):
        return pl.ds(pl.multiple_of(h * tile, tile), tile)

    def b_copy(c, span=slice(None)):
        return pltpu.make_async_remote_copy(
            src_ref=back.at[c - own, span],
            dst_ref=out_ref.at[span, col_lanes(c)],
            send_sem=b_send.at[0],
            recv_sem=b_recv.at[0],
            device_id={"fs": mate},
            device_id_type=MESH,
        )

    def first_product(src):
        part[src] = jnp.dot(
            spread[...], down_all[src], preferred_element_type=jnp.float32
        ).astype(jnp.bfloat16)
        for d in range(1, n_tp):
            r_copy(src, d).start()

    def take_hidden():
        load_hid.wait()
        ended(spread.at[pl.ds(0, (n_tp - 1) * rows)], a_sem.at[1])

    def sums_in():
        ended(red.at[pl.ds(1, n_tp - 1)], r_sem.at[1])
        for load in row_loads:
            load.wait()

    def norms(q):
        here = pl.ds(pl.multiple_of(q * piece, piece), piece)
        columns = []
        for src in range(n_fs):
            total = part[src, piece_rows(t, q)].astype(jnp.float32)
            for d in range(1, n_tp):
                total = total + red[d, src, here].astype(jnp.float32)
            columns.append(total)
        branch = jnp.concatenate(columns, axis=1)
        first = layer_norm(
            jnp.sqrt(2.0) * res_now[here].astype(jnp.float32) + 0.5 * branch,
            gain_now[0:1],
            shift_now[0:1],
        )
        mixed = layer_norm(
            jnp.sqrt(2.0) * first + mix_now[here].astype(jnp.float32),
            gain_now[1:2],
            shift_now[1:2],
        ).astype(jnp.bfloat16)
        mixed_all[0, piece_rows(t, q)] = mixed
        mixed_ref[here] = mixed

    def second_product(whose, c, span=slice(None)):
        weight = cols_all[c].reshape(n_fs * depth, 2 * lanes)
        total = jnp.dot(mixed_all[whose, span], weight, preferred_element_type=jnp.float32)
        gate = total[:, :lanes]
        return (gate / (1.0 + jnp.exp(-gate)) * total[:, lanes:]).astype(jnp.bfloat16)

    load_down.wait()

    @pl.when(inner)
    def _():
        each(0, sub, lambda j: d_send_on(f, j, (MAIN, OUT)))

    @pl.when(outer)
    def _():
        each(0, sub, lambda j: d_send_on(f, j, (MAIN,)))
        for share in others:
            each(0, sub, lambda j: d_send_late(f, share, j))

    for d in range(1, n_tp):
        a_copy(d).start()
    with jax.named_scope("loaded"):
        ended(cols_all.at[:, f], load_sem.at[2])

    @pl.when(outer)
    def _():
        each(0, ahead, lambda c: c_send_on(c, f, (MAIN,)))

    with jax.named_scope("first_pass"):

        @pl.when(inner)
        def _():
            def both(j):
                d_pass(mate, j, (MAIN,))
                d_pass(facing, j, [OUT] + across)

            each(0, sub, both)
            each(0, own, lambda c: c_send_on(c, f, (MAIN,)))

        @pl.when(outer)
        def _():
            each(0, sub, lambda j: d_pass(mate, j, across))

    with jax.named_scope("hidden"):
        take_hidden()

    part_way = min(4, sub)

    def step(k, carry):
        with jax.named_scope("step_wait"):

            @pl.when((k == 1) & inner)
            def _():
                each(0, part_way, lambda j: d_pass(beyond, j, [OUT] + across))
                d_rest(facing)

            @pl.when((k == 1) & outer)
            def _():
                each(0, part_way, lambda j: d_pass(facing, j, across))
                d_rest(mate)

            @pl.when((k == 2) & inner)
            def _():
                each(part_way, sub, lambda j: d_pass(beyond, j, [OUT] + across))
                each(0, own, lambda c: c_send_on(c, f, (OUT,)))
                d_rest(mate)

            @pl.when((k == 2) & outer)
            def _():
                each(part_way, sub, lambda j: d_pass(facing, j, across))
                each(0, part_way, lambda j: d_pass(beyond, j, across))
                d_rest(facing)

            @pl.when((k == 3) & inner)
            def _():
                c_pass(0, facing, [OUT] + across)
                c_pass(0, mate, (MAIN,))
                c_pass(1, facing, [OUT] + across)
                d_rest(beyond)

            @pl.when((k == 3) & outer)
            def _():
                each(part_way, sub, lambda j: d_pass(beyond, j, across))
                d_rest(beyond)

        second = jnp.where(inner, facing, mate)
        third = jnp.where(inner, mate, facing)
        with jax.named_scope("product"):
            first_product(
                jnp.where(k == 0, f, jnp.where(k == 1, second, jnp.where(k == 2, third, beyond)))
            )
        return carry

    lax.fori_loop(0, n_fs, step, 0)
    hosted = n_col - own
    slots = 2 * hosted

    @pl.when(inner)
    def _():
        def begin(c):
            @pl.when(c > 0)
            def _():
                c_pass(c, mate, (MAIN,))

            @pl.when(c > 1)
            def _():
                c_pass(c, facing, [OUT] + across)

        with jax.named_scope("begin"):
            each(0, own, begin)

    with jax.named_scope("sums_in"):
        sums_in()

    def norms_out(q):
        with jax.named_scope("norms"):
            norms(q)

        @pl.when(outer)
        def _():
            g_copy(q).start()

        m_out(0, q)

        @pl.when(inner & (q == pieces // 2 - 1))
        def _():
            c_pass(0, beyond, [OUT] + across)
            feed(own)

    def feed(c):
        @pl.when(c < n_col)
        def _():
            c_send_on(c, f, (MAIN,))
            c_pass(c, mate, (MAIN,))

    each(0, pieces, norms_out)

    def serve(i):
        c = jnp.where(
            i < hosted - 1,
            own + i,
            jnp.where(i == hosted - 1, 0, jnp.where(i == hosted, n_col - 1, i - hosted)),
        )
        with jax.named_scope("rest"):
            c_rest(c)

        @pl.when((c >= own) & (c < n_col - 1))
        def _():
            with jax.named_scope("prod1"):
                back[c - own] = second_product(1, c)
            b_copy(c).start()

        @pl.when(c == n_col - 1)
        def _():
            def half(h):
                span = tile_rows(h)
                back[c - own, span] = second_product(1, c, span)
                b_copy(c, span).start()

            each(0, 2, half)

        with jax.named_scope("prod0"):
            out_ref[:, col_lanes(c)] = second_product(0, c)

    def slot(s):
        c = own + s // 2
        src = jnp.where(s % 2 == 0, facing, beyond)

        @pl.when(s % 2 == 0)
        def _():
            feed(c + 2)

        with jax.named_scope("slot"):
            c_pass(c, src, across)

        when = s - (slots - 14)

        @pl.when(when == 1)
        def _():
            with jax.named_scope("m0"):
                m_relay_all()

        for q in range(pieces):

            @pl.when(when == 2 + q)
            def _():
                with jax.named_scope("from_mate"):
                    g_copy(q).wait_recv()
                    m_out(1, q)

            @pl.when(when == min(5 + q // 2 + q // 3, 7))
            def _():
                with jax.named_scope("m1"):
                    m_relay(1, q)

        @pl.when(when == 7)
        def _():
            with jax.named_scope("m_rest"):
                m_rest(0)
                m_rest(1)

        @pl.when(s == slots - 1)
        def _():
            for d in range(1, n_grp):
                moved_copy(d).start()

        done = jnp.clip(when - 7, 0, hosted - 2)
        more = jnp.where(when == 13, n_col, jnp.clip(when - 6, 0, hosted - 2))
        each(done, more, serve)

    @pl.when(inner)
    def _():
        with jax.named_scope("beyond_own"):
            c_pass(1, beyond, [OUT] + across)
            feed(own + 1)
            each(2, own, lambda c: c_pass(c, beyond, [OUT] + across))
        each(0, slots, slot)

    @pl.when(outer)
    def _():
        each(ahead, n_col, lambda c: c_send_on(c, f, (MAIN,)))
        for share in others:
            each(own, n_col, lambda c: c_send_late(c, f, share))
            each(0, own - 1, lambda c: c_send_late(c, f, share))

        def pass_own(c):
            with jax.named_scope("pass_own"):
                c_pass(c, mate, across)

        def pass_far(src):
            def act(c):
                with jax.named_scope("pass_far"):
                    c_pass(c, src, across)

            return act

        each(0, own, pass_own)
        each(0, own, pass_far(facing))
        with jax.named_scope("m0"):
            m_relay_all()
            m_rest(0)
        each(0, own, pass_far(beyond))

        def make_own(c):
            with jax.named_scope("rest"):
                c_rest(c)
            with jax.named_scope("prod0"):
                out_ref[:, col_lanes(c)] = second_product(0, c)

        each(0, own, make_own)
        with jax.named_scope("b_wait"):
            ended(back, b_recv.at[0])

    def d_sent(blocks, ways):
        for way in ways:
            ended(down_all.at[pl.ds(0, blocks), pl.ds(0, d_half)], d_send.at[way])

    def c_sent(columns, blocks, ways):
        for way in ways:
            ended(
                cols_all.at[pl.ds(0, columns), pl.ds(0, blocks), pl.ds(0, c_half)], c_send.at[way]
            )

    with jax.named_scope("drain"):
        ended(spread.at[pl.ds(0, (n_tp - 1) * rows)], a_sem.at[0])
        ended(red.at[pl.ds(1, n_tp - 1)], r_sem.at[0])
        m_drain(0)

        @pl.when(inner)
        def _():
            d_sent(2, (MAIN,))
            d_sent(3, (OUT,))
            d_sent(2, across)
            c_sent(n_col, 2, (MAIN,))
            c_sent(own, 3, (OUT,))
            c_sent(n_col, 2, across)
            for d in range(1, n_grp):
                moved_copy(d).wait_send()
            m_drain(1)
            ended(back, b_send.at[0])

        @pl.when(outer)
        def _():
            ended(down_all.at[f], d_send.at[MAIN])
            c_sent(n_col, 1, (MAIN,))
            late = n_col - 1
            ended(
                cols_all.at[pl.ds(0, late), 0, pl.ds(0, (n_grp - 1) * c_half)],
                c_send.at[ACROSS + n_grp - 1],
            )
            d_sent(3, across)
            c_sent(own, 3, across)
            ended(mixed_all.at[0, own_rows(t)], g_send.at[0])


def paired_call(sizes, arguments):
    n_grp, n_fs, n_tp = sizes
    residual_in, hidden_first, down_weight, _, _, _, gate_weight, _ = arguments
    rows, model = residual_in.shape
    depth, width = gate_weight.shape
    cols = down_weight.shape[1]
    tokens = rows * n_tp
    lanes = 128
    n_col = width // lanes
    share = down_weight.shape[0] // (n_grp * 16)
    sub = max(n for n in range(1, 12) if share % n == 0)
    own = n_col * 4 // 11
    pieces = 4
    ahead = n_col - 1
    parts = 2
    vmem = pl.BlockSpec(memory_space=pltpu.VMEM)
    hbm = pl.BlockSpec(memory_space=pltpu.HBM)
    dma = pltpu.SemaphoreType.DMA
    return pl.pallas_call(
        functools.partial(paired_kernel, (n_grp, n_fs, n_tp, sub, own, pieces, ahead, parts)),
        out_shape=(
            jax.ShapeDtypeStruct((rows, model), jnp.bfloat16),
            jax.ShapeDtypeStruct((tokens, width), jnp.bfloat16),
        ),
        in_specs=[hbm] * 8,
        out_specs=(vmem, vmem),
        scratch_shapes=[
            pltpu.VMEM((n_fs,) + down_weight.shape, jnp.bfloat16),
            pltpu.VMEM((n_col, n_fs, depth, 2 * lanes), jnp.bfloat16),
            pltpu.VMEM((tokens, width), jnp.bfloat16),
            pltpu.VMEM((n_fs, tokens, cols), jnp.bfloat16),
            pltpu.VMEM((n_tp, n_fs, rows, cols), jnp.bfloat16),
            pltpu.VMEM((2, tokens, model), jnp.bfloat16),
            pltpu.VMEM((n_col - own, tokens, lanes), jnp.bfloat16),
            pltpu.VMEM((rows, model), jnp.bfloat16),
            pltpu.VMEM((rows, model), jnp.bfloat16),
            pltpu.VMEM((2, model), jnp.float32),
            pltpu.VMEM((2, model), jnp.float32),
            dma((7,)),
            dma((1 + n_grp,)),
            dma((n_fs - 1, sub)),
            dma((n_fs,)),
            dma((2 * n_grp,)),
            dma((n_fs - 1, n_col * parts)),
            dma((n_col,)),
            dma((2,)),
            dma((2,)),
            dma((2,)),
            dma((n_tp // 2, 1 + pieces)),
            dma((2,)),
            dma((1,)),
            dma((pieces,)),
            dma((1,)),
            dma((1,)),
        ],
        compiler_params=pltpu.CompilerParams(
            collective_id=0, has_side_effects=True, vmem_limit_bytes=48 * 1024 * 1024
        ),
        name="paired_half_steps",
    )(*(pltpu.with_memory_space_constraint(a, pltpu.HBM) for a in arguments))


def fits_pairs(sizes, residual_in, down_weight, gate_weight):
    n_grp, n_fs, n_tp = sizes
    depth, width = gate_weight.shape
    return (
        n_fs == 4
        and n_tp % 2 == 0
        and width % 128 == 0
        and width // 128 >= 10
        and depth % (n_grp * 2 * 16) == 0
        and down_weight.shape[0] % (n_grp * 16) == 0
        and residual_in.shape[0] % (4 * 16) == 0
    )


def on_device(
    sizes,
    residual_in,
    hidden_first,
    down_weight,
    mixer_out,
    norm_gain,
    norm_shift,
    gate_weight,
    up_weight,
):
    if fits_pairs(sizes, residual_in, down_weight, gate_weight):
        arguments = (
            residual_in,
            hidden_first,
            down_weight,
            mixer_out,
            norm_gain,
            norm_shift,
            gate_weight,
            up_weight,
        )
        return paired_call(sizes, arguments)
    n_grp, n_fs, n_tp = sizes
    rows, model = residual_in.shape
    depth, width = gate_weight.shape
    cols = down_weight.shape[1]
    sub = 1
    if depth % (n_grp * 2 * 32) == 0 and down_weight.shape[0] % (n_grp * 2 * 32) == 0:
        sub = 2
    chunks = n_grp * sub
    each = max(1, width * 3 // (11 * 128)) * 128
    shared = (width - each) // 128 * 128
    each = width - shared
    if width % 128:
        hidden_first = hidden_first.reshape(rows, n_tp, width).transpose(1, 0, 2)
    vmem = pl.BlockSpec(memory_space=pltpu.VMEM)
    anywhere = pl.BlockSpec(memory_space=pl.ANY)
    dma = pltpu.SemaphoreType.DMA
    tokens = rows * n_tp
    return pl.pallas_call(
        functools.partial(kernel, (n_grp, n_fs, n_tp, sub)),
        out_shape=(
            jax.ShapeDtypeStruct((rows, model), jnp.bfloat16),
            jax.ShapeDtypeStruct((tokens, width), jnp.bfloat16),
        ),
        in_specs=[vmem, anywhere, anywhere, vmem, vmem, vmem, anywhere, anywhere],
        out_specs=(vmem, vmem),
        scratch_shapes=[
            pltpu.VMEM((n_fs,) + down_weight.shape, jnp.bfloat16),
            pltpu.VMEM((n_fs, 2, depth, shared), jnp.bfloat16),
            pltpu.VMEM((n_fs, 2, depth, each), jnp.bfloat16),
            pltpu.VMEM((tokens, width), jnp.bfloat16),
            pltpu.VMEM((n_fs, tokens, cols), jnp.bfloat16),
            pltpu.VMEM((n_tp, n_fs, rows, cols), jnp.bfloat16),
            pltpu.VMEM((2, tokens, model), jnp.bfloat16),
            pltpu.VMEM((2, tokens, shared), jnp.float32),
            pltpu.VMEM((2, tokens, each), jnp.float32),
            pltpu.VMEM((tokens, shared), jnp.bfloat16),
            dma((6,)),
            dma((n_fs, 1 + n_grp, chunks)),
            dma((n_fs, chunks)),
            dma((2 * n_fs, 1 + n_grp, chunks)),
            dma((2 * n_fs, chunks)),
            dma((2 * n_fs, 1 + n_grp, chunks)),
            dma((2 * n_fs, chunks)),
            dma((n_tp,)),
            dma((n_tp,)),
            dma((n_tp, n_fs)),
            dma((n_tp, n_fs)),
            dma((2, n_tp, n_tp // 2)),
            dma((2, n_tp)),
            dma((1,)),
            dma((1,)),
            dma((2,)),
            dma((2,)),
        ],
        compiler_params=pltpu.CompilerParams(
            collective_id=0, has_side_effects=True, vmem_limit_bytes=60 * 1024 * 1024
        ),
        name="half_steps",
    )(
        residual_in,
        hidden_first,
        down_weight,
        mixer_out,
        norm_gain,
        norm_shift,
        gate_weight,
        up_weight,
    )


def solution(mesh):
    sizes = tuple(mesh.shape[axis] for axis in ("grp", "fs", "tp"))
    in_specs = (
        P(("grp", "fs", "tp"), None),
        P(("grp", "fs", "tp"), None),
        P("tp", "fs"),
        P(("grp", "fs", "tp"), None),
        P(),
        P(),
        P("fs", "tp"),
        P("fs", "tp"),
    )
    out_specs = (P(("grp", "fs", "tp"), None), P(("grp", "fs"), "tp"))
    return jax.shard_map(
        functools.partial(on_device, sizes),
        mesh=mesh,
        in_specs=in_specs,
        out_specs=out_specs,
        check_vma=False,
    )
```

```python
import functools

import jax
import jax.numpy as jnp
from jax import lax
from jax.experimental import pallas as pl
from jax.experimental.pallas import tpu as pltpu
from jax.sharding import PartitionSpec as P

MESH = pl.DeviceIdType.MESH


def layer_norm(values, gain, shift):
    center = values - jnp.mean(values, axis=-1, keepdims=True)
    variance = jnp.mean(center * center, axis=-1, keepdims=True)
    return center * lax.rsqrt(variance + 1e-05) * gain + shift


def kernel(
    sizes,
    res_ref,
    hid_ref,
    down_ref,
    mix_ref,
    gain_ref,
    shift_ref,
    gate_ref,
    up_ref,
    mixed_ref,
    out_ref,
    down_all,
    host_all,
    each_all,
    spread,
    part,
    red,
    mixed_all,
    host_acc,
    each_acc,
    back,
    load_sem,
    d_send,
    d_recv,
    h_send,
    h_recv,
    e_send,
    e_recv,
    a_send,
    a_recv,
    r_send,
    r_recv,
    m_send,
    m_recv,
    g_send,
    g_recv,
    b_send,
    b_recv,
):
    n_grp, n_fs, n_tp, sub = sizes
    shared = host_all.shape[3]
    g, f, t = lax.axis_index("grp"), lax.axis_index("fs"), lax.axis_index("tp")
    rows = res_ref.shape[0]
    width = gate_ref.shape[1]
    depth = gate_ref.shape[0]
    chunks = n_grp * sub

    def hid_block(peer):
        if len(hid_ref.shape) == 3:
            return hid_ref.at[peer]
        return hid_ref.at[:, pl.ds(pl.multiple_of(peer * width, width), width)]

    def own_rows(peer):
        return pl.ds(pl.multiple_of(peer * rows, rows), rows)

    load_down = pltpu.make_async_copy(down_ref, down_all.at[f], load_sem.at[0])
    loads = []
    for mat, ref in enumerate((gate_ref, up_ref)):
        loads.append(
            pltpu.make_async_copy(
                ref.at[:, pl.ds(0, shared)], host_all.at[f, mat], load_sem.at[1 + mat]
            )
        )
        loads.append(
            pltpu.make_async_copy(
                ref.at[:, pl.ds(shared, width - shared)], each_all.at[f, mat], load_sem.at[4 + mat]
            )
        )
    load_hid = pltpu.make_async_copy(hid_block(t), spread.at[own_rows(t)], load_sem.at[3])
    load_down.start()
    load_hid.start()
    for load in loads:
        load.start()

    lower = 2 * (f // 2)
    half = n_fs // 2
    host = lower + jnp.where(lower + 1 < half, 1, 0)
    is_host = f == host
    other = 2 * lower + 1 - f
    low_host = 1 if half > 1 else 0
    high_host = 2 * ((n_fs - 1) // 2)

    barrier = pltpu.get_barrier_semaphore()

    def greet(device):
        pl.semaphore_signal(barrier, inc=1, device_id=device, device_id_type=MESH)

    for d in range(1, n_grp):
        greet({"grp": lax.rem(g + d, n_grp)})
    for d in range(1, n_tp):
        greet({"tp": lax.rem(t + d, n_tp)})

    @pl.when(f > 0)
    def _():
        greet({"fs": f - 1})

    @pl.when(f < n_fs - 1)
    def _():
        greet({"fs": f + 1})

    inner = jnp.minimum(f, 1) + jnp.minimum(n_fs - 1 - f, 1)
    pl.semaphore_wait(barrier, n_grp - 1 + n_tp - 1 + inner)

    def block_copy(all_refs, send, recv):
        def copy(src, chunk, way, device):
            blocks = all_refs(src)
            size = blocks.shape[0] // chunks
            block = blocks.at[pl.ds(pl.multiple_of(chunk * size, size), size)]
            return pltpu.make_async_remote_copy(
                src_ref=block,
                dst_ref=block,
                send_sem=send(src).at[way, chunk],
                recv_sem=recv(src).at[chunk],
                device_id=device,
                device_id_type=MESH,
            )

        return copy

    def weight(refs, send, recv, mat):
        return block_copy(
            lambda src: refs.at[src, mat],
            lambda src: send.at[2 * src + mat],
            lambda src: recv.at[2 * src + mat],
        )

    def start(copy):
        copy.start()

    def wait_send(copy):
        copy.wait_send()

    class Gather:
        def __init__(self, copies, low, high, whole, needs):
            self.copies, self.low, self.high = copies, low, high
            self.whole, self.needs = whole, needs

        def whole_up(self, plane):
            return (2 * plane < n_fs) & self.whole

        def whole_down(self, plane):
            return (2 * plane >= n_fs) & self.whole

        def reached(self, plane):
            return (plane >= self.low) & (plane <= self.high)

        def along(self, copy, src, chunk, act, mine):
            up = (src <= f) & self.reached(f + 1)
            down = (src >= f) & self.reached(f - 1)
            if not mine:
                up = up & self.whole_up(f + 1)
                down = down & self.whole_down(f - 1)

            @pl.when(up)
            def _():
                act(copy(src, chunk, 0, {"fs": f + 1}))

            @pl.when(down)
            def _():
                act(copy(src, chunk, 1, {"fs": f - 1}))

        def all_along(self, src, act):
            for j in range(sub):
                for copy in self.copies:
                    self.along(copy, src, g * sub + j, act, True)
            if self.whole:
                for d in range(1, n_grp):
                    for j in range(sub):
                        for copy in self.copies:
                            chunk = lax.rem(g + d, n_grp) * sub + j
                            self.along(copy, src, chunk, act, False)

        def across(self, copy, src, chunk, act):
            for d in range(1, n_grp):
                act(copy(src, chunk, 1 + d, {"grp": lax.rem(g + d, n_grp)}))

        def whole_in(self, src):
            return ((src < f) & self.whole_up(f)) | ((src > f) & self.whole_down(f))

        def comes(self, src):
            return (src >= 0) & (src < n_fs) & (src != f) & self.reached(f)

        def swaps(self, src):
            return self.comes(src) & self.needs & jnp.logical_not(self.whole_in(src))

        def take(self, src):
            @pl.when(self.comes(src))
            def _():
                for j in range(sub):
                    for copy in self.copies:
                        chunk = g * sub + j
                        copy(src, chunk, 0, {"fs": other}).wait_recv()
                        self.along(copy, src, chunk, start, True)

                        @pl.when(self.swaps(src))
                        def _():
                            self.across(copy, src, chunk, start)

            if self.whole:

                @pl.when(self.comes(src) & self.whole_in(src))
                def _():
                    for d in range(1, n_grp):
                        for j in range(sub):
                            for copy in self.copies:
                                chunk = lax.rem(g + d, n_grp) * sub + j
                                copy(src, chunk, 0, {"fs": other}).wait_recv()
                                self.along(copy, src, chunk, start, False)

        def take_across(self, src):
            @pl.when(self.swaps(src))
            def _():
                for d in range(1, n_grp):
                    for j in range(sub):
                        for copy in self.copies:
                            chunk = lax.rem(g + d, n_grp) * sub + j
                            copy(src, chunk, 0, {"fs": other}).wait_recv()

        def drain(self, src):
            @pl.when((src == f) | self.comes(src))
            def _():
                if self.whole:
                    @pl.when((src == f) | self.whole_in(src))
                    def _():
                        for d in range(1, n_grp):
                            for j in range(sub):
                                for copy in self.copies:
                                    chunk = lax.rem(g + d, n_grp) * sub + j
                                    self.along(copy, src, chunk, wait_send, False)
                for j in range(sub):
                    for copy in self.copies:
                        self.along(copy, src, g * sub + j, wait_send, True)

            @pl.when(self.swaps(src))
            def _():
                for j in range(sub):
                    for copy in self.copies:
                        self.across(copy, src, g * sub + j, wait_send)

    def source(k):
        return f + (1 - 2 * lax.rem(k, 2)) * ((k + 1) // 2)

    def valid(src):
        return (src >= 0) & (src < n_fs)

    d_copy = block_copy(
        lambda src: down_all.at[src], lambda src: d_send.at[src], lambda src: d_recv.at[src]
    )
    down = Gather([d_copy], 0, n_fs - 1, False, True)
    hosted = Gather(
        [weight(host_all, h_send, h_recv, mat) for mat in range(2)],
        low_host,
        high_host,
        True,
        is_host,
    )
    each = Gather(
        [weight(each_all, e_send, e_recv, mat) for mat in range(2)], 0, n_fs - 1, True, True
    )

    def a_copy(d):
        peer = lax.rem(t + d, n_tp)
        return pltpu.make_async_remote_copy(
            src_ref=hid_block(peer),
            dst_ref=spread.at[own_rows(t)],
            send_sem=a_send.at[d],
            recv_sem=a_recv.at[d],
            device_id={"tp": peer},
            device_id_type=MESH,
        )

    def r_copy(src, d):
        peer = lax.rem(t + d, n_tp)
        return pltpu.make_async_remote_copy(
            src_ref=part.at[src, own_rows(peer)],
            dst_ref=red.at[d, src],
            send_sem=r_send.at[d, src],
            recv_sem=r_recv.at[d, src],
            device_id={"tp": peer},
            device_id_type=MESH,
        )

    core = lax.rem(t, 2)
    sibling = t + 1 - 2 * core

    def m_copy(owner, whose, hop):
        peer = sibling if hop == 0 else lax.rem(t + 2 * hop, n_tp)
        place = mixed_all.at[whose, own_rows(owner)]
        return pltpu.make_async_remote_copy(
            src_ref=place,
            dst_ref=place,
            send_sem=m_send.at[whose, owner, hop],
            recv_sem=m_recv.at[whose, owner],
            device_id={"tp": peer},
            device_id_type=MESH,
        )

    chips = n_tp // 2

    def m_out(whose):
        for hop in list(range(1, chips)) + [0]:
            m_copy(t, whose, hop).start()

    def m_relay(whose):
        for hop in range(1, chips):
            owner = lax.rem(t + 2 * hop, n_tp)
            m_copy(owner, whose, 0).wait_recv()
            m_copy(owner, whose, 0).start()

    def m_rest(whose):
        for hop in range(chips):
            m_copy(lax.rem(sibling + 2 * hop, n_tp), whose, 0).wait_recv()

    def m_drain(whose):
        for hop in range(chips):
            m_copy(t, whose, hop).wait_send()
        for hop in range(1, chips):
            m_copy(lax.rem(t + 2 * hop, n_tp), whose, 0).wait_send()

    def g_copy():
        return pltpu.make_async_remote_copy(
            src_ref=mixed_all.at[0, own_rows(t)],
            dst_ref=mixed_all.at[1, own_rows(t)],
            send_sem=g_send.at[0],
            recv_sem=g_recv.at[0],
            device_id={"fs": other},
            device_id_type=MESH,
        )

    tiles = 2
    tile = n_tp * rows // tiles

    def tile_rows(i):
        return pl.ds(pl.multiple_of(i * tile, tile), tile)

    def b_copy(i):
        return pltpu.make_async_remote_copy(
            src_ref=back.at[tile_rows(i)],
            dst_ref=out_ref.at[tile_rows(i), pl.ds(0, shared)],
            send_sem=b_send.at[i],
            recv_sem=b_recv.at[i],
            device_id={"fs": other},
            device_id_type=MESH,
        )

    load_down.wait()
    down.all_along(f, start)
    for d in range(1, n_tp):
        a_copy(d).start()
    for load in loads:
        load.wait()
    load_hid.wait()

    @pl.when(jnp.logical_not(is_host))
    def _():
        hosted.all_along(f, start)

    def first_half(k, carry):
        src = source(k)

        down.take(src)

        @pl.when((k == 2 * n_fs - 2) & is_host)
        def _():
            hosted.all_along(f, start)

        @pl.when(k == 2)
        def _():
            for d in range(1, n_tp):
                a_copy(d).wait_recv()

        done = source(k - 2)

        @pl.when((k >= 2) & valid(done))
        def _():
            down.take_across(done)
            part[done] = jnp.dot(
                spread[...], down_all[done], preferred_element_type=jnp.float32
            ).astype(jnp.bfloat16)
            for d in range(1, n_tp):
                r_copy(done, d).start()

        return carry

    lax.fori_loop(1, 2 * n_fs + 1, first_half, 0)

    for src in range(n_fs):
        for d in range(1, n_tp):
            r_copy(src, d).wait_recv()
    pieces = []
    for src in range(n_fs):
        total = part[src, own_rows(t)].astype(jnp.float32)
        for d in range(1, n_tp):
            total = total + red[d, src].astype(jnp.float32)
        pieces.append(total)
    branch = jnp.concatenate(pieces, axis=1)
    first = layer_norm(
        jnp.sqrt(2.0) * res_ref[...].astype(jnp.float32) + 0.5 * branch,
        gain_ref[0:1],
        shift_ref[0:1],
    )
    mixed = layer_norm(
        jnp.sqrt(2.0) * first + mix_ref[...].astype(jnp.float32), gain_ref[1:2], shift_ref[1:2]
    ).astype(jnp.bfloat16)
    mixed_all[0, own_rows(t)] = mixed
    mixed_ref[...] = mixed

    @pl.when(jnp.logical_not(is_host))
    def _():
        g_copy().start()

    m_out(0)

    @pl.when(jnp.logical_not(is_host))
    def _():
        each.all_along(f, start)

    def take_hosted(k, carry):
        hosted.take(source(k))
        return carry

    lax.fori_loop(1, 2 * n_fs - 1, take_hosted, 0)

    @pl.when(is_host)
    def _():
        each.all_along(f, start)

    m_relay(0)

    @pl.when(is_host)
    def _():
        g_copy().wait_recv()
        m_out(1)

    def take_each(k, carry):
        each.take(source(k))
        return carry

    lax.fori_loop(1, 3, take_each, 0)
    m_rest(0)

    def products(whose, span, gather, refs, total):
        total[...] = jnp.zeros_like(total)

        def add(k, carry):
            src = source(k)

            @pl.when(valid(src))
            def _():
                if gather is not None:
                    gather.take_across(src)
                here = pl.ds(pl.multiple_of(src * depth, depth), depth)
                for mat in range(2):
                    total[mat] += jnp.dot(
                        mixed_all[whose, span, here],
                        refs[src, mat],
                        preferred_element_type=jnp.float32,
                    )

            return carry

        lax.fori_loop(0, 2 * n_fs - 1, add, 0)
        gate = total[0]
        return (gate / (1.0 + jnp.exp(-gate)) * total[1]).astype(jnp.bfloat16)

    everything = pl.ds(0, n_tp * rows)

    @pl.when(is_host)
    def _():
        m_relay(1)
        out_ref[:, pl.ds(0, shared)] = products(0, everything, hosted, host_all, host_acc)

    lax.fori_loop(3, 2 * n_fs - 1, take_each, 0)

    @pl.when(is_host)
    def _():
        m_rest(1)

        def serve(i, carry):
            back[tile_rows(i)] = products(
                1, tile_rows(i), None, host_all, host_acc.at[:, pl.ds(0, tile)]
            )
            b_copy(i).start()
            return carry

        lax.fori_loop(0, tiles, serve, 0)

    out_ref[:, pl.ds(shared, width - shared)] = products(0, everything, each, each_all, each_acc)

    @pl.when(is_host)
    def _():
        for i in range(tiles):
            b_copy(i).wait_send()
        m_drain(1)

    @pl.when(jnp.logical_not(is_host))
    def _():
        g_copy().wait_send()
        for i in range(tiles):
            b_copy(i).wait_recv()

    m_drain(0)
    for d in range(1, n_tp):
        a_copy(d).wait_send()
        for src in range(n_fs):
            r_copy(src, d).wait_send()

    def drain(src, carry):
        for gather in (down, hosted, each):
            gather.drain(src)
        return carry

    lax.fori_loop(0, n_fs, drain, 0)


def paired_kernel(
    sizes,
    res_ref,
    hid_ref,
    down_ref,
    mix_ref,
    gain_ref,
    shift_ref,
    gate_ref,
    up_ref,
    mixed_ref,
    out_ref,
    down_all,
    cols_all,
    spread,
    part,
    red,
    mixed_all,
    back,
    res_now,
    mix_now,
    gain_now,
    shift_now,
    load_sem,
    d_send,
    d_recv,
    d_late,
    c_send,
    c_recv,
    c_late,
    a_sem,
    r_sem,
    m_send,
    m_recv,
    m_late,
    g_send,
    g_recv,
    b_send,
    b_recv,
):
    n_grp, n_fs, n_tp, sub, own, pieces, ahead, moved = sizes
    g, f, t = lax.axis_index("grp"), lax.axis_index("fs"), lax.axis_index("tp")
    rows = res_ref.shape[0]
    width = gate_ref.shape[1]
    depth = gate_ref.shape[0]
    n_col = cols_all.shape[0]
    lanes = width // n_col

    lower = 2 * (f // 2)
    mate = 2 * lower + 1 - f
    inner = (f > 0) & (f < n_fs - 1)
    outer = jnp.logical_not(inner)
    facing = n_fs - 1 - jnp.where(inner, f, mate)
    beyond = n_fs - 1 - jnp.where(inner, mate, f)

    def hid_block(peer):
        return hid_ref.at[:, pl.ds(pl.multiple_of(peer * width, width), width)]

    def own_rows(peer):
        return pl.ds(pl.multiple_of(peer * rows, rows), rows)

    load_down = pltpu.make_async_copy(down_ref, down_all.at[f], load_sem.at[0])
    load_hid = pltpu.make_async_copy(hid_block(t), spread.at[own_rows(t)], load_sem.at[1])

    def load_col(c, mat):
        return pltpu.make_async_copy(
            (gate_ref, up_ref)[mat].at[:, pl.ds(pl.multiple_of(c * lanes, lanes), lanes)],
            cols_all.at[c, f, :, pl.ds(mat * lanes, lanes)],
            load_sem.at[2],
        )

    load_down.start()
    load_hid.start()
    row_loads = [
        pltpu.make_async_copy(whole, now, load_sem.at[3 + k])
        for k, (whole, now) in enumerate(
            (
                (res_ref, res_now),
                (mix_ref, mix_now),
                (gain_ref, gain_now),
                (shift_ref, shift_now),
            )
        )
    ]
    for load in row_loads:
        load.start()

    def each(low, high, act):
        def body(c, carry):
            act(c)
            return carry

        lax.fori_loop(low, high, body, 0)

    def load_cols(c):
        for mat in range(2):
            load_col(c, mat).start()

    def ended(ref, sem):
        pltpu.make_async_copy(ref, ref, sem).wait()

    each(0, n_col, load_cols)

    barrier = pltpu.get_barrier_semaphore()

    def greet(device):
        pl.semaphore_signal(barrier, inc=1, device_id=device, device_id_type=MESH)

    for d in range(1, n_grp):
        greet({"grp": lax.rem(g + d, n_grp)})
    for d in range(1, n_tp):
        greet({"tp": lax.rem(t + d, n_tp)})
    greet({"fs": mate})

    @pl.when(inner)
    def _():
        greet({"fs": facing})

    with jax.named_scope("barrier"):
        pl.semaphore_wait(barrier, n_grp - 1 + n_tp - 1 + 1 + inner.astype(jnp.int32))

    MAIN, OUT, ACROSS = 0, 1, 2
    TAIL, LATE, LAST = n_grp, 2 * n_grp, 2 * n_grp + 1

    def device_of(way):
        if way == MAIN:
            return {"fs": jnp.where(inner, facing, mate)}
        if way == OUT:
            return {"fs": mate}
        return {"grp": lax.rem(g + way - ACROSS + 1, n_grp)}

    def d_place(src, share, j):
        size = down_all.shape[1] // (n_grp * sub)
        return down_all.at[src, pl.ds(pl.multiple_of((share * sub + j) * size, size), size)]

    def d_copy(src, share, j, way, sem):
        block = d_place(src, share, j)
        return pltpu.make_async_remote_copy(
            src_ref=block,
            dst_ref=block,
            send_sem=d_send.at[way],
            recv_sem=sem,
            device_id=device_of(way),
            device_id_type=MESH,
        )

    def c_copy(c, src, share, part_of, way, sem, count=None, parts=1):
        whole = depth // n_grp
        size = whole // parts
        block = cols_all.at[
            c, src, pl.ds(pl.multiple_of(share * whole + part_of * size, size), size)
        ]
        return pltpu.make_async_remote_copy(
            src_ref=block,
            dst_ref=block,
            send_sem=c_send.at[way if count is None else count],
            recv_sem=sem,
            device_id=device_of(way),
            device_id_type=MESH,
        )

    def place_at(receiver, src):
        return src - (src > receiver).astype(jnp.int32)

    def receiver_of(way):
        return jnp.where(inner, facing, mate) if way == MAIN else mate

    def tail(c, src):
        for d in range(1, n_grp):
            c_copy(c, src, g, 0, ACROSS + d - 1, c_late.at[c], TAIL + d).start()

    def straight_copies():
        last = n_col - 1
        copies = []
        for share in others:
            copies.append(c_copy(last, f, share, 0, MAIN, c_late.at[last], LATE))
            copies.append(c_copy(own - 1, f, share, 0, MAIN, c_late.at[own - 1], LAST))
        return copies

    d_half = down_all.shape[1] // n_grp
    c_half = depth // n_grp

    across = [ACROSS + d - 1 for d in range(1, n_grp)]
    others = [lax.rem(g + d, n_grp) for d in range(1, n_grp)]

    def d_send_on(src, j, ways):
        for way in ways:
            if way in (MAIN, OUT):
                sem = d_recv.at[place_at(receiver_of(way), src), j]
            else:
                sem = d_late.at[src]
            d_copy(src, g, j, way, sem).start()

    def d_send_late(src, share, j):
        d_copy(src, share, j, MAIN, d_late.at[src]).start()

    def c_part_on(c, src, k, ways, parts):
        for way in ways:
            if way in (MAIN, OUT):
                sem = c_recv.at[place_at(receiver_of(way), src), c + k]
            else:
                sem = c_late.at[c]
            c_copy(c, src, g, k, way, sem, parts=parts).start()

    def c_send_on(c, src, ways, parts=1):
        for k in range(parts):
            c_part_on(c, src, k, ways, parts)

    def c_send_late(c, src, share):
        c_copy(c, src, share, 0, MAIN, c_late.at[c], LATE).start()

    def d_pass(src, j, ways):
        d_copy(src, g, j, MAIN, d_recv.at[place_at(f, src), j]).wait_recv()
        d_send_on(src, j, ways)

    def c_pass(c, src, ways, parts=1):
        for k in range(parts):
            sem = c_recv.at[place_at(f, src), c + k]
            c_copy(c, src, g, k, MAIN, sem, parts=parts).wait_recv()
            c_part_on(c, src, k, ways, parts)

    def c_pass_part(c, src, k):
        sem = c_recv.at[place_at(f, src), c + k]
        c_copy(c, src, g, k, MAIN, sem, parts=2).wait_recv()

    def d_rest(src):
        ended(down_all.at[src, pl.ds(0, (n_grp - 1) * d_half)], d_late.at[src])

    def c_rest(c):
        ended(cols_all.at[c, pl.ds(0, n_fs - 1), pl.ds(0, (n_grp - 1) * c_half)], c_late.at[c])

    def a_copy(d):
        peer = lax.rem(t + d, n_tp)
        return pltpu.make_async_remote_copy(
            src_ref=hid_block(peer),
            dst_ref=spread.at[own_rows(t)],
            send_sem=a_sem.at[0],
            recv_sem=a_sem.at[1],
            device_id={"tp": peer},
            device_id_type=MESH,
        )

    def r_copy(src, d):
        peer = lax.rem(t + d, n_tp)
        return pltpu.make_async_remote_copy(
            src_ref=part.at[src, own_rows(peer)],
            dst_ref=red.at[d, src],
            send_sem=r_sem.at[0],
            recv_sem=r_sem.at[1],
            device_id={"tp": peer},
            device_id_type=MESH,
        )

    core = lax.rem(t, 2)
    sibling = t + 1 - 2 * core
    chips = n_tp // 2
    piece = rows // pieces

    def piece_rows(owner, q):
        return pl.ds(pl.multiple_of(owner * rows + q * piece, piece), piece)

    def m_copy(owner, whose, hop, q):
        peer = sibling if hop == 0 else lax.rem(t + 2 * hop, n_tp)
        place = mixed_all.at[whose, piece_rows(owner, q)]
        return pltpu.make_async_remote_copy(
            src_ref=place,
            dst_ref=place,
            send_sem=m_send.at[whose],
            recv_sem=m_late.at[whose] if hop == 0 else m_recv.at[owner // 2, whose * (q + 1)],
            device_id={"tp": peer},
            device_id_type=MESH,
        )

    def m_out(whose, q):
        for hop in list(range(1, chips)) + [0]:
            m_copy(t, whose, hop, q).start()

    def m_relay(whose, q):
        for hop in range(1, chips):
            owner = lax.rem(t + 2 * hop, n_tp)
            m_copy(owner, whose, hop, q).wait_recv()
            m_copy(owner, whose, 0, q).start()

    def m_relay_all():
        for hop in range(1, chips):
            owner = lax.rem(t + 2 * hop, n_tp)
            ended(mixed_all.at[0, own_rows(owner)], m_recv.at[owner // 2, 0])
            for q in range(pieces):
                m_copy(owner, 0, 0, q).start()

    def m_rest(whose):
        ended(mixed_all.at[whose, pl.ds(0, chips * rows)], m_late.at[whose])

    def m_drain(whose):
        ended(mixed_all.at[whose, pl.ds(0, (2 * chips - 1) * rows)], m_send.at[whose])

    def g_copy(q):
        return pltpu.make_async_remote_copy(
            src_ref=mixed_all.at[0, piece_rows(t, q)],
            dst_ref=mixed_all.at[1, piece_rows(t, q)],
            send_sem=g_send.at[0],
            recv_sem=g_recv.at[q],
            device_id={"fs": mate},
            device_id_type=MESH,
        )

    def col_lanes(c):
        return pl.ds(pl.multiple_of(c * lanes, lanes), lanes)

    tile = n_tp * rows // 2

    def tile_rows(h):
        return pl.ds(pl.multiple_of(h * tile, tile), tile)

    def b_copy(c, span=slice(None)):
        return pltpu.make_async_remote_copy(
            src_ref=back.at[c - own, span],
            dst_ref=out_ref.at[span, col_lanes(c)],
            send_sem=b_send.at[0],
            recv_sem=b_recv.at[0],
            device_id={"fs": mate},
            device_id_type=MESH,
        )

    def first_product(src):
        part[src] = jnp.dot(
            spread[...], down_all[src], preferred_element_type=jnp.float32
        ).astype(jnp.bfloat16)
        for d in range(1, n_tp):
            r_copy(src, d).start()

    def take_hidden():
        load_hid.wait()
        ended(spread.at[pl.ds(0, (n_tp - 1) * rows)], a_sem.at[1])

    def sums_in():
        ended(red.at[pl.ds(1, n_tp - 1)], r_sem.at[1])
        for load in row_loads:
            load.wait()

    def norms(q):
        here = pl.ds(pl.multiple_of(q * piece, piece), piece)
        columns = []
        for src in range(n_fs):
            total = part[src, piece_rows(t, q)].astype(jnp.float32)
            for d in range(1, n_tp):
                total = total + red[d, src, here].astype(jnp.float32)
            columns.append(total)
        branch = jnp.concatenate(columns, axis=1)
        first = layer_norm(
            jnp.sqrt(2.0) * res_now[here].astype(jnp.float32) + 0.5 * branch,
            gain_now[0:1],
            shift_now[0:1],
        )
        mixed = layer_norm(
            jnp.sqrt(2.0) * first + mix_now[here].astype(jnp.float32),
            gain_now[1:2],
            shift_now[1:2],
        ).astype(jnp.bfloat16)
        mixed_all[0, piece_rows(t, q)] = mixed
        mixed_ref[here] = mixed

    def second_product(whose, c, span=slice(None)):
        weight = cols_all[c].reshape(n_fs * depth, 2 * lanes)
        total = jnp.dot(mixed_all[whose, span], weight, preferred_element_type=jnp.float32)
        gate = total[:, :lanes]
        return (gate / (1.0 + jnp.exp(-gate)) * total[:, lanes:]).astype(jnp.bfloat16)

    load_down.wait()

    @pl.when(inner)
    def _():
        each(0, sub, lambda j: d_send_on(f, j, (MAIN, OUT)))

    @pl.when(outer)
    def _():
        each(0, sub, lambda j: d_send_on(f, j, (MAIN,)))
        for share in others:
            each(0, sub, lambda j: d_send_late(f, share, j))

    for d in range(1, n_tp):
        a_copy(d).start()
    with jax.named_scope("loaded"):
        ended(cols_all.at[:, f], load_sem.at[2])

    @pl.when(outer)
    def _():
        each(0, ahead, lambda c: c_send_on(c, f, (MAIN,)))

    with jax.named_scope("first_pass"):

        @pl.when(inner)
        def _():
            def both(j):
                d_pass(mate, j, (MAIN,))
                d_pass(facing, j, [OUT] + across)

            each(0, sub, both)
            each(0, own, lambda c: c_send_on(c, f, (MAIN,)))

        @pl.when(outer)
        def _():
            each(0, sub, lambda j: d_pass(mate, j, across))

    with jax.named_scope("hidden"):
        take_hidden()

    part_way = min(4, sub)

    def step(k, carry):
        with jax.named_scope("step_wait"):

            @pl.when((k == 1) & inner)
            def _():
                each(0, part_way, lambda j: d_pass(beyond, j, [OUT] + across))
                d_rest(facing)

            @pl.when((k == 1) & outer)
            def _():
                each(0, part_way, lambda j: d_pass(facing, j, across))
                d_rest(mate)

            @pl.when((k == 2) & inner)
            def _():
                each(part_way, sub, lambda j: d_pass(beyond, j, [OUT] + across))
                each(0, own, lambda c: c_send_on(c, f, (OUT,)))
                d_rest(mate)

            @pl.when((k == 2) & outer)
            def _():
                each(part_way, sub, lambda j: d_pass(facing, j, across))
                each(0, part_way, lambda j: d_pass(beyond, j, across))
                d_rest(facing)

            @pl.when((k == 3) & inner)
            def _():
                c_pass(0, facing, [OUT] + across)
                c_pass(0, mate, (MAIN,))
                c_pass(1, facing, [OUT] + across)
                d_rest(beyond)

            @pl.when((k == 3) & outer)
            def _():
                each(part_way, sub, lambda j: d_pass(beyond, j, across))
                d_rest(beyond)

        second = jnp.where(inner, facing, mate)
        third = jnp.where(inner, mate, facing)
        with jax.named_scope("product"):
            first_product(
                jnp.where(k == 0, f, jnp.where(k == 1, second, jnp.where(k == 2, third, beyond)))
            )
        return carry

    lax.fori_loop(0, n_fs, step, 0)
    hosted = n_col - own
    slots = 2 * hosted

    @pl.when(inner)
    def _():
        def begin(c):
            @pl.when(c > 0)
            def _():
                c_pass(c, mate, (MAIN,))

            @pl.when((c > 1) & (c < own - 1))
            def _():
                c_pass(c, facing, [OUT] + across)

            @pl.when(c == own - 1)
            def _():
                c_pass(c, facing, (OUT,))

        with jax.named_scope("begin"):
            each(0, own, begin)

    with jax.named_scope("sums_in"):
        sums_in()

    def norms_out(q):
        with jax.named_scope("norms"):
            norms(q)

        @pl.when(outer)
        def _():
            g_copy(q).start()

        m_out(0, q)

        @pl.when(inner & (q == pieces // 2 - 1))
        def _():
            c_pass(0, beyond, [OUT] + across)
            feed(own)

    def feed(c):
        @pl.when(c < n_col - 1)
        def _():
            c_send_on(c, f, (MAIN,))
            c_pass(c, mate, (MAIN,))

        @pl.when(c == n_col - 1)
        def _():
            c_pass(c, mate, (MAIN,), 2)
            c_send_on(c, f, (MAIN,), 2)
            for copy in straight_copies():
                copy.start()

    each(0, pieces, norms_out)

    def serve(i):
        c = jnp.where(
            i < hosted - 1,
            own + i,
            jnp.where(i == hosted - 1, n_col - 1, i - hosted),
        )
        with jax.named_scope("rest"):
            c_rest(c)

        @pl.when((c >= own) & (c < n_col - 1))
        def _():
            with jax.named_scope("prod1"):
                back[c - own] = second_product(1, c)
            b_copy(c).start()

        @pl.when(c == n_col - 1)
        def _():
            def half(h):
                span = tile_rows(h)
                back[c - own, span] = second_product(1, c, span)
                b_copy(c, span).start()

            each(0, 2, half)

        with jax.named_scope("prod0"):
            out_ref[:, col_lanes(c)] = second_product(0, c)

    def slot(s):
        c = own + s // 2
        last = c == n_col - 1
        src = jnp.where((s % 2 == 0) ^ last, facing, beyond)

        @pl.when(s % 2 == 0)
        def _():
            feed(c + 2)

        with jax.named_scope("slot"):

            @pl.when(jnp.logical_not(last))
            def _():
                c_pass(c, src, across)

            @pl.when(s == slots - 2)
            def _():
                c_pass(c, beyond, across, 2)
                each(own - moved, own, lambda m: tail(m, mate))

            @pl.when(s == slots - 1)
            def _():
                for k in range(2):
                    c_pass_part(c, facing, k)

        when = s - (slots - 14)

        @pl.when(when == 1)
        def _():
            with jax.named_scope("m0"):
                m_relay_all()

        for q in range(pieces):

            @pl.when(when == 2 + q)
            def _():
                with jax.named_scope("from_mate"):
                    g_copy(q).wait_recv()
                    m_out(1, q)

            @pl.when(when == min(5 + q // 2 + q // 3, 7))
            def _():
                with jax.named_scope("m1"):
                    m_relay(1, q)

        @pl.when(when == 7)
        def _():
            with jax.named_scope("m_rest"):
                m_rest(0)
                m_rest(1)

        done = jnp.clip(when - 8, 0, hosted - 2)
        more = jnp.where(when == 13, n_col, jnp.clip(when - 7, 0, hosted - 2))
        each(done, more, serve)

    @pl.when(inner)
    def _():
        with jax.named_scope("beyond_own"):
            c_pass(1, beyond, [OUT] + across)
            feed(own + 1)
            each(2, own, lambda c: c_pass(c, beyond, [OUT] + across))
        each(0, slots, slot)

    @pl.when(outer)
    def _():
        each(ahead, n_col - 1, lambda c: c_send_on(c, f, (MAIN,)))
        c_send_on(n_col - 1, f, (MAIN,), 2)
        for share in others:
            each(own, n_col, lambda c: c_send_late(c, f, share))
            each(0, own - moved, lambda c: c_send_late(c, f, share))

        def pass_own(c):
            with jax.named_scope("pass_own"):
                c_pass(c, mate, across)

        def pass_far(src):
            def act(c):
                with jax.named_scope("pass_far"):
                    c_pass(c, src, across)

            return act

        each(0, own, pass_own)
        each(0, own, pass_far(facing))
        with jax.named_scope("m0"):
            m_relay_all()
            m_rest(0)
        each(0, own, pass_far(beyond))

        def make_own(c):
            with jax.named_scope("rest"):
                c_rest(c)
            with jax.named_scope("prod0"):
                out_ref[:, col_lanes(c)] = second_product(0, c)

        each(0, own, make_own)
        with jax.named_scope("b_wait"):
            ended(back, b_recv.at[0])

    def d_sent(blocks, ways):
        for way in ways:
            ended(down_all.at[pl.ds(0, blocks), pl.ds(0, d_half)], d_send.at[way])

    def c_sent(columns, blocks, ways):
        for way in ways:
            ended(
                cols_all.at[pl.ds(0, columns), pl.ds(0, blocks), pl.ds(0, c_half)], c_send.at[way]
            )

    with jax.named_scope("drain"):
        ended(spread.at[pl.ds(0, (n_tp - 1) * rows)], a_sem.at[0])
        ended(red.at[pl.ds(1, n_tp - 1)], r_sem.at[0])
        m_drain(0)

        @pl.when(inner)
        def _():
            d_sent(2, (MAIN,))
            d_sent(3, (OUT,))
            d_sent(2, across)
            c_sent(n_col, 2, (MAIN,))
            c_sent(own, 3, (OUT,))
            c_sent(n_col - 1, 2, across)
            c_sent(moved, 1, [TAIL + d for d in range(1, n_grp)])
            for copy in straight_copies():
                copy.wait_send()
            m_drain(1)
            ended(back, b_send.at[0])

        @pl.when(outer)
        def _():
            ended(down_all.at[f], d_send.at[MAIN])
            c_sent(n_col, 1, (MAIN,))
            late = n_col - moved
            ended(
                cols_all.at[pl.ds(0, late), 0, pl.ds(0, (n_grp - 1) * c_half)],
                c_send.at[LATE],
            )
            d_sent(3, across)
            c_sent(own, 3, across)
            ended(mixed_all.at[0, own_rows(t)], g_send.at[0])


def paired_call(sizes, arguments):
    n_grp, n_fs, n_tp = sizes
    residual_in, hidden_first, down_weight, _, _, _, gate_weight, _ = arguments
    rows, model = residual_in.shape
    depth, width = gate_weight.shape
    cols = down_weight.shape[1]
    tokens = rows * n_tp
    lanes = 128
    n_col = width // lanes
    share = down_weight.shape[0] // (n_grp * 16)
    sub = max(n for n in range(1, 12) if share % n == 0)
    own = n_col * 4 // 11
    pieces = 4
    ahead = n_col - 1
    moved = 2
    vmem = pl.BlockSpec(memory_space=pltpu.VMEM)
    hbm = pl.BlockSpec(memory_space=pltpu.HBM)
    dma = pltpu.SemaphoreType.DMA
    return pl.pallas_call(
        functools.partial(paired_kernel, (n_grp, n_fs, n_tp, sub, own, pieces, ahead, moved)),
        out_shape=(
            jax.ShapeDtypeStruct((rows, model), jnp.bfloat16),
            jax.ShapeDtypeStruct((tokens, width), jnp.bfloat16),
        ),
        in_specs=[hbm] * 8,
        out_specs=(vmem, vmem),
        scratch_shapes=[
            pltpu.VMEM((n_fs,) + down_weight.shape, jnp.bfloat16),
            pltpu.VMEM((n_col, n_fs, depth, 2 * lanes), jnp.bfloat16),
            pltpu.VMEM((tokens, width), jnp.bfloat16),
            pltpu.VMEM((n_fs, tokens, cols), jnp.bfloat16),
            pltpu.VMEM((n_tp, n_fs, rows, cols), jnp.bfloat16),
            pltpu.VMEM((2, tokens, model), jnp.bfloat16),
            pltpu.VMEM((n_col - own, tokens, lanes), jnp.bfloat16),
            pltpu.VMEM((rows, model), jnp.bfloat16),
            pltpu.VMEM((rows, model), jnp.bfloat16),
            pltpu.VMEM((2, model), jnp.float32),
            pltpu.VMEM((2, model), jnp.float32),
            dma((7,)),
            dma((1 + n_grp,)),
            dma((n_fs - 1, sub)),
            dma((n_fs,)),
            dma((2 * n_grp + 2,)),
            dma((n_fs - 1, n_col + 1)),
            dma((n_col,)),
            dma((2,)),
            dma((2,)),
            dma((2,)),
            dma((n_tp // 2, 1 + pieces)),
            dma((2,)),
            dma((1,)),
            dma((pieces,)),
            dma((1,)),
            dma((1,)),
        ],
        compiler_params=pltpu.CompilerParams(
            collective_id=0, has_side_effects=True, vmem_limit_bytes=48 * 1024 * 1024
        ),
        name="paired_half_steps",
    )(*(pltpu.with_memory_space_constraint(a, pltpu.HBM) for a in arguments))


def write_kernel(mixed_ref, hidden_ref, mixed_out, hidden_out, sems):
    copies = [
        pltpu.make_async_copy(hidden_ref, hidden_out, sems.at[0]),
        pltpu.make_async_copy(mixed_ref, mixed_out, sems.at[1]),
    ]
    for copy in copies:
        copy.start()
    for copy in copies:
        copy.wait()


def written(mixed, hidden):
    return pl.pallas_call(
        write_kernel,
        out_shape=(
            jax.ShapeDtypeStruct(mixed.shape, mixed.dtype),
            jax.ShapeDtypeStruct(hidden.shape, hidden.dtype),
        ),
        in_specs=[pl.BlockSpec(memory_space=pltpu.VMEM)] * 2,
        out_specs=(pl.BlockSpec(memory_space=pl.ANY),) * 2,
        scratch_shapes=[pltpu.SemaphoreType.DMA((2,))],
        compiler_params=pltpu.CompilerParams(vmem_limit_bytes=8 * 1024 * 1024),
        name="write_out",
    )(mixed, hidden)


def fits_pairs(sizes, residual_in, down_weight, gate_weight):
    n_grp, n_fs, n_tp = sizes
    depth, width = gate_weight.shape
    return (
        n_grp == 2
        and n_fs == 4
        and n_tp % 2 == 0
        and width % 128 == 0
        and width // 128 >= 10
        and depth % (n_grp * 2 * 16) == 0
        and down_weight.shape[0] % (n_grp * 16) == 0
        and residual_in.shape[0] % (4 * 16) == 0
    )


def on_device(
    sizes,
    residual_in,
    hidden_first,
    down_weight,
    mixer_out,
    norm_gain,
    norm_shift,
    gate_weight,
    up_weight,
):
    if fits_pairs(sizes, residual_in, down_weight, gate_weight):
        arguments = (
            residual_in,
            hidden_first,
            down_weight,
            mixer_out,
            norm_gain,
            norm_shift,
            gate_weight,
            up_weight,
        )
        return written(*paired_call(sizes, arguments))
    n_grp, n_fs, n_tp = sizes
    rows, model = residual_in.shape
    depth, width = gate_weight.shape
    cols = down_weight.shape[1]
    sub = 1
    if depth % (n_grp * 2 * 32) == 0 and down_weight.shape[0] % (n_grp * 2 * 32) == 0:
        sub = 2
    chunks = n_grp * sub
    each = max(1, width * 3 // (11 * 128)) * 128
    shared = (width - each) // 128 * 128
    each = width - shared
    if width % 128:
        hidden_first = hidden_first.reshape(rows, n_tp, width).transpose(1, 0, 2)
    vmem = pl.BlockSpec(memory_space=pltpu.VMEM)
    anywhere = pl.BlockSpec(memory_space=pl.ANY)
    dma = pltpu.SemaphoreType.DMA
    tokens = rows * n_tp
    return pl.pallas_call(
        functools.partial(kernel, (n_grp, n_fs, n_tp, sub)),
        out_shape=(
            jax.ShapeDtypeStruct((rows, model), jnp.bfloat16),
            jax.ShapeDtypeStruct((tokens, width), jnp.bfloat16),
        ),
        in_specs=[vmem, anywhere, anywhere, vmem, vmem, vmem, anywhere, anywhere],
        out_specs=(vmem, vmem),
        scratch_shapes=[
            pltpu.VMEM((n_fs,) + down_weight.shape, jnp.bfloat16),
            pltpu.VMEM((n_fs, 2, depth, shared), jnp.bfloat16),
            pltpu.VMEM((n_fs, 2, depth, each), jnp.bfloat16),
            pltpu.VMEM((tokens, width), jnp.bfloat16),
            pltpu.VMEM((n_fs, tokens, cols), jnp.bfloat16),
            pltpu.VMEM((n_tp, n_fs, rows, cols), jnp.bfloat16),
            pltpu.VMEM((2, tokens, model), jnp.bfloat16),
            pltpu.VMEM((2, tokens, shared), jnp.float32),
            pltpu.VMEM((2, tokens, each), jnp.float32),
            pltpu.VMEM((tokens, shared), jnp.bfloat16),
            dma((6,)),
            dma((n_fs, 1 + n_grp, chunks)),
            dma((n_fs, chunks)),
            dma((2 * n_fs, 1 + n_grp, chunks)),
            dma((2 * n_fs, chunks)),
            dma((2 * n_fs, 1 + n_grp, chunks)),
            dma((2 * n_fs, chunks)),
            dma((n_tp,)),
            dma((n_tp,)),
            dma((n_tp, n_fs)),
            dma((n_tp, n_fs)),
            dma((2, n_tp, n_tp // 2)),
            dma((2, n_tp)),
            dma((1,)),
            dma((1,)),
            dma((2,)),
            dma((2,)),
        ],
        compiler_params=pltpu.CompilerParams(
            collective_id=0, has_side_effects=True, vmem_limit_bytes=60 * 1024 * 1024
        ),
        name="half_steps",
    )(
        residual_in,
        hidden_first,
        down_weight,
        mixer_out,
        norm_gain,
        norm_shift,
        gate_weight,
        up_weight,
    )


def solution(mesh):
    sizes = tuple(mesh.shape[axis] for axis in ("grp", "fs", "tp"))
    in_specs = (
        P(("grp", "fs", "tp"), None),
        P(("grp", "fs", "tp"), None),
        P("tp", "fs"),
        P(("grp", "fs", "tp"), None),
        P(),
        P(),
        P("fs", "tp"),
        P("fs", "tp"),
    )
    out_specs = (P(("grp", "fs", "tp"), None), P(("grp", "fs"), "tp"))
    return jax.shard_map(
        functools.partial(on_device, sizes),
        mesh=mesh,
        in_specs=in_specs,
        out_specs=out_specs,
        check_vma=False,
    )
```

```python
import functools

import jax
import jax.numpy as jnp
from jax import lax
from jax.experimental import pallas as pl
from jax.experimental.pallas import tpu as pltpu
from jax.sharding import PartitionSpec as P

MESH = pl.DeviceIdType.MESH


def layer_norm(values, gain, shift):
    center = values - jnp.mean(values, axis=-1, keepdims=True)
    variance = jnp.mean(center * center, axis=-1, keepdims=True)
    return center * lax.rsqrt(variance + 1e-05) * gain + shift


def kernel(
    sizes,
    res_ref,
    hid_ref,
    down_ref,
    mix_ref,
    gain_ref,
    shift_ref,
    gate_ref,
    up_ref,
    mixed_ref,
    out_ref,
    down_all,
    host_all,
    each_all,
    spread,
    part,
    red,
    mixed_all,
    host_acc,
    each_acc,
    back,
    load_sem,
    d_send,
    d_recv,
    h_send,
    h_recv,
    e_send,
    e_recv,
    a_send,
    a_recv,
    r_send,
    r_recv,
    m_send,
    m_recv,
    g_send,
    g_recv,
    b_send,
    b_recv,
):
    n_grp, n_fs, n_tp, sub = sizes
    shared = host_all.shape[3]
    g, f, t = lax.axis_index("grp"), lax.axis_index("fs"), lax.axis_index("tp")
    rows = res_ref.shape[0]
    width = gate_ref.shape[1]
    depth = gate_ref.shape[0]
    chunks = n_grp * sub

    def hid_block(peer):
        if len(hid_ref.shape) == 3:
            return hid_ref.at[peer]
        return hid_ref.at[:, pl.ds(pl.multiple_of(peer * width, width), width)]

    def own_rows(peer):
        return pl.ds(pl.multiple_of(peer * rows, rows), rows)

    load_down = pltpu.make_async_copy(down_ref, down_all.at[f], load_sem.at[0])
    loads = []
    for mat, ref in enumerate((gate_ref, up_ref)):
        loads.append(
            pltpu.make_async_copy(
                ref.at[:, pl.ds(0, shared)], host_all.at[f, mat], load_sem.at[1 + mat]
            )
        )
        loads.append(
            pltpu.make_async_copy(
                ref.at[:, pl.ds(shared, width - shared)], each_all.at[f, mat], load_sem.at[4 + mat]
            )
        )
    load_hid = pltpu.make_async_copy(hid_block(t), spread.at[own_rows(t)], load_sem.at[3])
    load_down.start()
    load_hid.start()
    for load in loads:
        load.start()

    lower = 2 * (f // 2)
    half = n_fs // 2
    host = lower + jnp.where(lower + 1 < half, 1, 0)
    is_host = f == host
    other = 2 * lower + 1 - f
    low_host = 1 if half > 1 else 0
    high_host = 2 * ((n_fs - 1) // 2)

    barrier = pltpu.get_barrier_semaphore()

    def greet(device):
        pl.semaphore_signal(barrier, inc=1, device_id=device, device_id_type=MESH)

    for d in range(1, n_grp):
        greet({"grp": lax.rem(g + d, n_grp)})
    for d in range(1, n_tp):
        greet({"tp": lax.rem(t + d, n_tp)})

    @pl.when(f > 0)
    def _():
        greet({"fs": f - 1})

    @pl.when(f < n_fs - 1)
    def _():
        greet({"fs": f + 1})

    inner = jnp.minimum(f, 1) + jnp.minimum(n_fs - 1 - f, 1)
    pl.semaphore_wait(barrier, n_grp - 1 + n_tp - 1 + inner)

    def block_copy(all_refs, send, recv):
        def copy(src, chunk, way, device):
            blocks = all_refs(src)
            size = blocks.shape[0] // chunks
            block = blocks.at[pl.ds(pl.multiple_of(chunk * size, size), size)]
            return pltpu.make_async_remote_copy(
                src_ref=block,
                dst_ref=block,
                send_sem=send(src).at[way, chunk],
                recv_sem=recv(src).at[chunk],
                device_id=device,
                device_id_type=MESH,
            )

        return copy

    def weight(refs, send, recv, mat):
        return block_copy(
            lambda src: refs.at[src, mat],
            lambda src: send.at[2 * src + mat],
            lambda src: recv.at[2 * src + mat],
        )

    def start(copy):
        copy.start()

    def wait_send(copy):
        copy.wait_send()

    class Gather:
        def __init__(self, copies, low, high, whole, needs):
            self.copies, self.low, self.high = copies, low, high
            self.whole, self.needs = whole, needs

        def whole_up(self, plane):
            return (2 * plane < n_fs) & self.whole

        def whole_down(self, plane):
            return (2 * plane >= n_fs) & self.whole

        def reached(self, plane):
            return (plane >= self.low) & (plane <= self.high)

        def along(self, copy, src, chunk, act, mine):
            up = (src <= f) & self.reached(f + 1)
            down = (src >= f) & self.reached(f - 1)
            if not mine:
                up = up & self.whole_up(f + 1)
                down = down & self.whole_down(f - 1)

            @pl.when(up)
            def _():
                act(copy(src, chunk, 0, {"fs": f + 1}))

            @pl.when(down)
            def _():
                act(copy(src, chunk, 1, {"fs": f - 1}))

        def all_along(self, src, act):
            for j in range(sub):
                for copy in self.copies:
                    self.along(copy, src, g * sub + j, act, True)
            if self.whole:
                for d in range(1, n_grp):
                    for j in range(sub):
                        for copy in self.copies:
                            chunk = lax.rem(g + d, n_grp) * sub + j
                            self.along(copy, src, chunk, act, False)

        def across(self, copy, src, chunk, act):
            for d in range(1, n_grp):
                act(copy(src, chunk, 1 + d, {"grp": lax.rem(g + d, n_grp)}))

        def whole_in(self, src):
            return ((src < f) & self.whole_up(f)) | ((src > f) & self.whole_down(f))

        def comes(self, src):
            return (src >= 0) & (src < n_fs) & (src != f) & self.reached(f)

        def swaps(self, src):
            return self.comes(src) & self.needs & jnp.logical_not(self.whole_in(src))

        def take(self, src):
            @pl.when(self.comes(src))
            def _():
                for j in range(sub):
                    for copy in self.copies:
                        chunk = g * sub + j
                        copy(src, chunk, 0, {"fs": other}).wait_recv()
                        self.along(copy, src, chunk, start, True)

                        @pl.when(self.swaps(src))
                        def _():
                            self.across(copy, src, chunk, start)

            if self.whole:

                @pl.when(self.comes(src) & self.whole_in(src))
                def _():
                    for d in range(1, n_grp):
                        for j in range(sub):
                            for copy in self.copies:
                                chunk = lax.rem(g + d, n_grp) * sub + j
                                copy(src, chunk, 0, {"fs": other}).wait_recv()
                                self.along(copy, src, chunk, start, False)

        def take_across(self, src):
            @pl.when(self.swaps(src))
            def _():
                for d in range(1, n_grp):
                    for j in range(sub):
                        for copy in self.copies:
                            chunk = lax.rem(g + d, n_grp) * sub + j
                            copy(src, chunk, 0, {"fs": other}).wait_recv()

        def drain(self, src):
            @pl.when((src == f) | self.comes(src))
            def _():
                if self.whole:
                    @pl.when((src == f) | self.whole_in(src))
                    def _():
                        for d in range(1, n_grp):
                            for j in range(sub):
                                for copy in self.copies:
                                    chunk = lax.rem(g + d, n_grp) * sub + j
                                    self.along(copy, src, chunk, wait_send, False)
                for j in range(sub):
                    for copy in self.copies:
                        self.along(copy, src, g * sub + j, wait_send, True)

            @pl.when(self.swaps(src))
            def _():
                for j in range(sub):
                    for copy in self.copies:
                        self.across(copy, src, g * sub + j, wait_send)

    def source(k):
        return f + (1 - 2 * lax.rem(k, 2)) * ((k + 1) // 2)

    def valid(src):
        return (src >= 0) & (src < n_fs)

    d_copy = block_copy(
        lambda src: down_all.at[src], lambda src: d_send.at[src], lambda src: d_recv.at[src]
    )
    down = Gather([d_copy], 0, n_fs - 1, False, True)
    hosted = Gather(
        [weight(host_all, h_send, h_recv, mat) for mat in range(2)],
        low_host,
        high_host,
        True,
        is_host,
    )
    each = Gather(
        [weight(each_all, e_send, e_recv, mat) for mat in range(2)], 0, n_fs - 1, True, True
    )

    def a_copy(d):
        peer = lax.rem(t + d, n_tp)
        return pltpu.make_async_remote_copy(
            src_ref=hid_block(peer),
            dst_ref=spread.at[own_rows(t)],
            send_sem=a_send.at[d],
            recv_sem=a_recv.at[d],
            device_id={"tp": peer},
            device_id_type=MESH,
        )

    def r_copy(src, d):
        peer = lax.rem(t + d, n_tp)
        return pltpu.make_async_remote_copy(
            src_ref=part.at[src, own_rows(peer)],
            dst_ref=red.at[d, src],
            send_sem=r_send.at[d, src],
            recv_sem=r_recv.at[d, src],
            device_id={"tp": peer},
            device_id_type=MESH,
        )

    core = lax.rem(t, 2)
    sibling = t + 1 - 2 * core

    def m_copy(owner, whose, hop):
        peer = sibling if hop == 0 else lax.rem(t + 2 * hop, n_tp)
        place = mixed_all.at[whose, own_rows(owner)]
        return pltpu.make_async_remote_copy(
            src_ref=place,
            dst_ref=place,
            send_sem=m_send.at[whose, owner, hop],
            recv_sem=m_recv.at[whose, owner],
            device_id={"tp": peer},
            device_id_type=MESH,
        )

    chips = n_tp // 2

    def m_out(whose):
        for hop in list(range(1, chips)) + [0]:
            m_copy(t, whose, hop).start()

    def m_relay(whose):
        for hop in range(1, chips):
            owner = lax.rem(t + 2 * hop, n_tp)
            m_copy(owner, whose, 0).wait_recv()
            m_copy(owner, whose, 0).start()

    def m_rest(whose):
        for hop in range(chips):
            m_copy(lax.rem(sibling + 2 * hop, n_tp), whose, 0).wait_recv()

    def m_drain(whose):
        for hop in range(chips):
            m_copy(t, whose, hop).wait_send()
        for hop in range(1, chips):
            m_copy(lax.rem(t + 2 * hop, n_tp), whose, 0).wait_send()

    def g_copy():
        return pltpu.make_async_remote_copy(
            src_ref=mixed_all.at[0, own_rows(t)],
            dst_ref=mixed_all.at[1, own_rows(t)],
            send_sem=g_send.at[0],
            recv_sem=g_recv.at[0],
            device_id={"fs": other},
            device_id_type=MESH,
        )

    tiles = 2
    tile = n_tp * rows // tiles

    def tile_rows(i):
        return pl.ds(pl.multiple_of(i * tile, tile), tile)

    def b_copy(i):
        return pltpu.make_async_remote_copy(
            src_ref=back.at[tile_rows(i)],
            dst_ref=out_ref.at[tile_rows(i), pl.ds(0, shared)],
            send_sem=b_send.at[i],
            recv_sem=b_recv.at[i],
            device_id={"fs": other},
            device_id_type=MESH,
        )

    load_down.wait()
    down.all_along(f, start)
    for d in range(1, n_tp):
        a_copy(d).start()
    for load in loads:
        load.wait()
    load_hid.wait()

    @pl.when(jnp.logical_not(is_host))
    def _():
        hosted.all_along(f, start)

    def first_half(k, carry):
        src = source(k)

        down.take(src)

        @pl.when((k == 2 * n_fs - 2) & is_host)
        def _():
            hosted.all_along(f, start)

        @pl.when(k == 2)
        def _():
            for d in range(1, n_tp):
                a_copy(d).wait_recv()

        done = source(k - 2)

        @pl.when((k >= 2) & valid(done))
        def _():
            down.take_across(done)
            part[done] = jnp.dot(
                spread[...], down_all[done], preferred_element_type=jnp.float32
            ).astype(jnp.bfloat16)
            for d in range(1, n_tp):
                r_copy(done, d).start()

        return carry

    lax.fori_loop(1, 2 * n_fs + 1, first_half, 0)

    for src in range(n_fs):
        for d in range(1, n_tp):
            r_copy(src, d).wait_recv()
    pieces = []
    for src in range(n_fs):
        total = part[src, own_rows(t)].astype(jnp.float32)
        for d in range(1, n_tp):
            total = total + red[d, src].astype(jnp.float32)
        pieces.append(total)
    branch = jnp.concatenate(pieces, axis=1)
    first = layer_norm(
        jnp.sqrt(2.0) * res_ref[...].astype(jnp.float32) + 0.5 * branch,
        gain_ref[0:1],
        shift_ref[0:1],
    )
    mixed = layer_norm(
        jnp.sqrt(2.0) * first + mix_ref[...].astype(jnp.float32), gain_ref[1:2], shift_ref[1:2]
    ).astype(jnp.bfloat16)
    mixed_all[0, own_rows(t)] = mixed
    mixed_ref[...] = mixed

    @pl.when(jnp.logical_not(is_host))
    def _():
        g_copy().start()

    m_out(0)

    @pl.when(jnp.logical_not(is_host))
    def _():
        each.all_along(f, start)

    def take_hosted(k, carry):
        hosted.take(source(k))
        return carry

    lax.fori_loop(1, 2 * n_fs - 1, take_hosted, 0)

    @pl.when(is_host)
    def _():
        each.all_along(f, start)

    m_relay(0)

    @pl.when(is_host)
    def _():
        g_copy().wait_recv()
        m_out(1)

    def take_each(k, carry):
        each.take(source(k))
        return carry

    lax.fori_loop(1, 3, take_each, 0)
    m_rest(0)

    def products(whose, span, gather, refs, total):
        total[...] = jnp.zeros_like(total)

        def add(k, carry):
            src = source(k)

            @pl.when(valid(src))
            def _():
                if gather is not None:
                    gather.take_across(src)
                here = pl.ds(pl.multiple_of(src * depth, depth), depth)
                for mat in range(2):
                    total[mat] += jnp.dot(
                        mixed_all[whose, span, here],
                        refs[src, mat],
                        preferred_element_type=jnp.float32,
                    )

            return carry

        lax.fori_loop(0, 2 * n_fs - 1, add, 0)
        gate = total[0]
        return (gate / (1.0 + jnp.exp(-gate)) * total[1]).astype(jnp.bfloat16)

    everything = pl.ds(0, n_tp * rows)

    @pl.when(is_host)
    def _():
        m_relay(1)
        out_ref[:, pl.ds(0, shared)] = products(0, everything, hosted, host_all, host_acc)

    lax.fori_loop(3, 2 * n_fs - 1, take_each, 0)

    @pl.when(is_host)
    def _():
        m_rest(1)

        def serve(i, carry):
            back[tile_rows(i)] = products(
                1, tile_rows(i), None, host_all, host_acc.at[:, pl.ds(0, tile)]
            )
            b_copy(i).start()
            return carry

        lax.fori_loop(0, tiles, serve, 0)

    out_ref[:, pl.ds(shared, width - shared)] = products(0, everything, each, each_all, each_acc)

    @pl.when(is_host)
    def _():
        for i in range(tiles):
            b_copy(i).wait_send()
        m_drain(1)

    @pl.when(jnp.logical_not(is_host))
    def _():
        g_copy().wait_send()
        for i in range(tiles):
            b_copy(i).wait_recv()

    m_drain(0)
    for d in range(1, n_tp):
        a_copy(d).wait_send()
        for src in range(n_fs):
            r_copy(src, d).wait_send()

    def drain(src, carry):
        for gather in (down, hosted, each):
            gather.drain(src)
        return carry

    lax.fori_loop(0, n_fs, drain, 0)


def paired_kernel(
    sizes,
    res_ref,
    hid_ref,
    down_ref,
    mix_ref,
    gain_ref,
    shift_ref,
    gate_ref,
    up_ref,
    mixed_ref,
    out_ref,
    down_all,
    cols_all,
    spread,
    part,
    red,
    mixed_all,
    back,
    res_now,
    mix_now,
    gain_now,
    shift_now,
    early,
    load_sem,
    d_send,
    d_recv,
    d_late,
    c_send,
    c_recv,
    c_late,
    a_sem,
    r_sem,
    m_send,
    m_recv,
    m_late,
    g_send,
    g_recv,
    b_send,
    b_recv,
):
    n_grp, n_fs, n_tp, sub, own, pieces, ahead, moved = sizes
    g, f, t = lax.axis_index("grp"), lax.axis_index("fs"), lax.axis_index("tp")
    rows = res_ref.shape[0]
    width = gate_ref.shape[1]
    depth = gate_ref.shape[0]
    n_col = cols_all.shape[0]
    lanes = width // n_col

    lower = 2 * (f // 2)
    mate = 2 * lower + 1 - f
    inner = (f > 0) & (f < n_fs - 1)
    outer = jnp.logical_not(inner)
    facing = n_fs - 1 - jnp.where(inner, f, mate)
    beyond = n_fs - 1 - jnp.where(inner, mate, f)

    def hid_block(peer):
        return hid_ref.at[:, pl.ds(pl.multiple_of(peer * width, width), width)]

    def own_rows(peer):
        return pl.ds(pl.multiple_of(peer * rows, rows), rows)

    barrier = pltpu.get_barrier_semaphore()

    def greet(device):
        pl.semaphore_signal(barrier, inc=1, device_id=device, device_id_type=MESH)

    for d in range(1, n_grp):
        greet({"grp": lax.rem(g + d, n_grp)})
    for d in range(1, n_tp):
        greet({"tp": lax.rem(t + d, n_tp)})
    greet({"fs": mate})

    @pl.when(inner)
    def _():
        greet({"fs": facing})

    load_down = pltpu.make_async_copy(down_ref, down_all.at[f], load_sem.at[0])
    load_hid = pltpu.make_async_copy(hid_block(t), spread.at[own_rows(t)], load_sem.at[1])

    def load_col(c, mat):
        return pltpu.make_async_copy(
            (gate_ref, up_ref)[mat].at[:, pl.ds(pl.multiple_of(c * lanes, lanes), lanes)],
            cols_all.at[c, f, :, pl.ds(mat * lanes, lanes)],
            load_sem.at[2],
        )

    load_down.start()
    load_hid.start()
    row_loads = [
        pltpu.make_async_copy(whole, now, load_sem.at[3 + k])
        for k, (whole, now) in enumerate(
            (
                (res_ref, res_now),
                (mix_ref, mix_now),
                (gain_ref, gain_now),
                (shift_ref, shift_now),
            )
        )
    ]
    for load in row_loads:
        load.start()

    def each(low, high, act):
        def body(c, carry):
            act(c)
            return carry

        lax.fori_loop(low, high, body, 0)

    def load_cols(c):
        for mat in range(2):
            load_col(c, mat).start()

    def ended(ref, sem):
        pltpu.make_async_copy(ref, ref, sem).wait()

    each(0, n_col, load_cols)

    with jax.named_scope("barrier"):
        pl.semaphore_wait(barrier, n_grp - 1 + n_tp - 1 + 1 + inner.astype(jnp.int32))

    MAIN, OUT, ACROSS = 0, 1, 2
    TAIL, LATE, LAST = n_grp, 2 * n_grp, 2 * n_grp + 1

    def device_of(way):
        if way == MAIN:
            return {"fs": jnp.where(inner, facing, mate)}
        if way == OUT:
            return {"fs": mate}
        return {"grp": lax.rem(g + way - ACROSS + 1, n_grp)}

    def d_place(src, share, j):
        size = down_all.shape[1] // (n_grp * sub)
        return down_all.at[src, pl.ds(pl.multiple_of((share * sub + j) * size, size), size)]

    def d_copy(src, share, j, way, sem):
        block = d_place(src, share, j)
        return pltpu.make_async_remote_copy(
            src_ref=block,
            dst_ref=block,
            send_sem=d_send.at[way],
            recv_sem=sem,
            device_id=device_of(way),
            device_id_type=MESH,
        )

    def c_copy(c, src, share, part_of, way, sem, count=None, parts=1):
        whole = depth // n_grp
        size = whole // parts
        block = cols_all.at[
            c, src, pl.ds(pl.multiple_of(share * whole + part_of * size, size), size)
        ]
        return pltpu.make_async_remote_copy(
            src_ref=block,
            dst_ref=block,
            send_sem=c_send.at[way if count is None else count],
            recv_sem=sem,
            device_id=device_of(way),
            device_id_type=MESH,
        )

    def place_at(receiver, src):
        return src - (src > receiver).astype(jnp.int32)

    def receiver_of(way):
        return jnp.where(inner, facing, mate) if way == MAIN else mate

    def tail(c, src):
        for d in range(1, n_grp):
            c_copy(c, src, g, 0, ACROSS + d - 1, c_late.at[c], TAIL + d).start()

    def straight_copies():
        last = n_col - 1
        copies = []
        for share in others:
            copies.append(c_copy(last, f, share, 0, MAIN, c_late.at[n_col], LATE))
            copies.append(c_copy(own - 1, f, share, 0, MAIN, c_late.at[own - 1], LAST))
        return copies

    d_half = down_all.shape[1] // n_grp
    c_half = depth // n_grp

    across = [ACROSS + d - 1 for d in range(1, n_grp)]
    others = [lax.rem(g + d, n_grp) for d in range(1, n_grp)]

    def d_send_on(src, j, ways):
        for way in ways:
            if way in (MAIN, OUT):
                sem = d_recv.at[place_at(receiver_of(way), src), j]
            else:
                sem = d_late.at[src]
            d_copy(src, g, j, way, sem).start()

    def d_send_late(src, share, j):
        d_copy(src, share, j, MAIN, d_late.at[src]).start()

    def arrival(c, k, parts):
        return c if parts == 1 else own + 2 * (c - own) + k

    def c_part_on(c, src, k, ways, parts):
        for way in ways:
            if way in (MAIN, OUT):
                sem = c_recv.at[place_at(receiver_of(way), src), arrival(c, k, parts)]
            else:
                sem = c_late.at[c]
            c_copy(c, src, g, k, way, sem, parts=parts).start()

    def c_send_on(c, src, ways, parts=1):
        for k in range(parts):
            c_part_on(c, src, k, ways, parts)

    def c_send_late(c, src, share):
        c_copy(c, src, share, 0, MAIN, c_late.at[c], LATE).start()

    def d_pass(src, j, ways):
        d_copy(src, g, j, MAIN, d_recv.at[place_at(f, src), j]).wait_recv()
        d_send_on(src, j, ways)

    def c_pass(c, src, ways, parts=1):
        for k in range(parts):
            sem = c_recv.at[place_at(f, src), arrival(c, k, parts)]
            c_copy(c, src, g, k, MAIN, sem, parts=parts).wait_recv()
            c_part_on(c, src, k, ways, parts)

    def c_pass_part(c, src, k):
        sem = c_recv.at[place_at(f, src), arrival(c, k, 2)]
        c_copy(c, src, g, k, MAIN, sem, parts=2).wait_recv()

    def d_rest(src):
        ended(down_all.at[src, pl.ds(0, (n_grp - 1) * d_half)], d_late.at[src])

    def c_rest(c):
        ended(cols_all.at[c, pl.ds(0, n_fs - 1), pl.ds(0, (n_grp - 1) * c_half)], c_late.at[c])

    def a_copy(d):
        peer = lax.rem(t + d, n_tp)
        return pltpu.make_async_remote_copy(
            src_ref=hid_block(peer),
            dst_ref=spread.at[own_rows(t)],
            send_sem=a_sem.at[0],
            recv_sem=a_sem.at[1],
            device_id={"tp": peer},
            device_id_type=MESH,
        )

    def r_copy(src, d):
        peer = lax.rem(t + d, n_tp)
        return pltpu.make_async_remote_copy(
            src_ref=part.at[src, own_rows(peer)],
            dst_ref=red.at[d, src],
            send_sem=r_sem.at[0],
            recv_sem=r_sem.at[1],
            device_id={"tp": peer},
            device_id_type=MESH,
        )

    core = lax.rem(t, 2)
    sibling = t + 1 - 2 * core
    chips = n_tp // 2
    piece = rows // pieces

    def piece_rows(owner, q):
        return pl.ds(pl.multiple_of(owner * rows + q * piece, piece), piece)

    def m_copy(owner, whose, hop, q):
        peer = sibling if hop == 0 else lax.rem(t + 2 * hop, n_tp)
        place = mixed_all.at[whose, piece_rows(owner, q)]
        return pltpu.make_async_remote_copy(
            src_ref=place,
            dst_ref=place,
            send_sem=m_send.at[whose],
            recv_sem=m_late.at[whose] if hop == 0 else m_recv.at[owner // 2, whose * (q + 1)],
            device_id={"tp": peer},
            device_id_type=MESH,
        )

    def m_out(whose, q):
        for hop in list(range(1, chips)) + [0]:
            m_copy(t, whose, hop, q).start()

    def m_relay(whose, q):
        for hop in range(1, chips):
            owner = lax.rem(t + 2 * hop, n_tp)
            m_copy(owner, whose, hop, q).wait_recv()
            m_copy(owner, whose, 0, q).start()

    def m_relay_all():
        for hop in range(1, chips):
            owner = lax.rem(t + 2 * hop, n_tp)
            ended(mixed_all.at[0, own_rows(owner)], m_recv.at[owner // 2, 0])
            for q in range(pieces):
                m_copy(owner, 0, 0, q).start()

    def m_rest(whose):
        ended(mixed_all.at[whose, pl.ds(0, chips * rows)], m_late.at[whose])

    def m_drain(whose):
        ended(mixed_all.at[whose, pl.ds(0, (2 * chips - 1) * rows)], m_send.at[whose])

    def g_copy(q):
        return pltpu.make_async_remote_copy(
            src_ref=mixed_all.at[0, piece_rows(t, q)],
            dst_ref=mixed_all.at[1, piece_rows(t, q)],
            send_sem=g_send.at[0],
            recv_sem=g_recv.at[q],
            device_id={"fs": mate},
            device_id_type=MESH,
        )

    def col_lanes(c):
        return pl.ds(pl.multiple_of(c * lanes, lanes), lanes)

    tile = n_tp * rows // 2

    def tile_rows(h):
        return pl.ds(pl.multiple_of(h * tile, tile), tile)

    def b_copy(c, span=slice(None)):
        return pltpu.make_async_remote_copy(
            src_ref=back.at[c - own, span],
            dst_ref=out_ref.at[span, col_lanes(c)],
            send_sem=b_send.at[0],
            recv_sem=b_recv.at[0],
            device_id={"fs": mate},
            device_id_type=MESH,
        )

    def first_product(src):
        part[src] = jnp.dot(
            spread[...], down_all[src], preferred_element_type=jnp.float32
        ).astype(jnp.bfloat16)
        for d in range(1, n_tp):
            r_copy(src, d).start()

    def take_hidden():
        load_hid.wait()
        ended(spread.at[pl.ds(0, (n_tp - 1) * rows)], a_sem.at[1])

    def sums_in():
        ended(red.at[pl.ds(1, n_tp - 1)], r_sem.at[1])
        for load in row_loads:
            load.wait()

    def norms(q):
        here = pl.ds(pl.multiple_of(q * piece, piece), piece)
        columns = []
        for src in range(n_fs):
            total = part[src, piece_rows(t, q)].astype(jnp.float32)
            for d in range(1, n_tp):
                total = total + red[d, src, here].astype(jnp.float32)
            columns.append(total)
        branch = jnp.concatenate(columns, axis=1)
        first = layer_norm(
            jnp.sqrt(2.0) * res_now[here].astype(jnp.float32) + 0.5 * branch,
            gain_now[0:1],
            shift_now[0:1],
        )
        mixed = layer_norm(
            jnp.sqrt(2.0) * first + mix_now[here].astype(jnp.float32),
            gain_now[1:2],
            shift_now[1:2],
        ).astype(jnp.bfloat16)
        mixed_all[0, piece_rows(t, q)] = mixed
        mixed_ref[here] = mixed

    def second_product(whose, c, span=slice(None)):
        weight = cols_all[c].reshape(n_fs * depth, 2 * lanes)
        total = jnp.dot(mixed_all[whose, span], weight, preferred_element_type=jnp.float32)
        gate = total[:, :lanes]
        return (gate / (1.0 + jnp.exp(-gate)) * total[:, lanes:]).astype(jnp.bfloat16)

    load_down.wait()

    @pl.when(inner)
    def _():
        each(0, sub, lambda j: d_send_on(f, j, (MAIN, OUT)))

    @pl.when(outer)
    def _():
        each(0, sub, lambda j: d_send_on(f, j, (MAIN,)))
        for share in others:
            each(0, sub, lambda j: d_send_late(f, share, j))

    for d in range(1, n_tp):
        a_copy(d).start()
    with jax.named_scope("loaded"):
        ended(cols_all.at[:, f], load_sem.at[2])

    @pl.when(outer)
    def _():
        each(0, own, lambda c: c_send_on(c, f, (MAIN,)))
        each(own, ahead, lambda c: c_send_on(c, f, (MAIN,), 2))

    with jax.named_scope("first_pass"):

        @pl.when(inner)
        def _():
            def both(j):
                d_pass(mate, j, (MAIN,))
                d_pass(facing, j, [OUT] + across)

            each(0, sub, both)
            each(0, own, lambda c: c_send_on(c, f, (MAIN,)))

        @pl.when(outer)
        def _():
            each(0, sub, lambda j: d_pass(mate, j, across))

    with jax.named_scope("hidden"):
        take_hidden()

    part_way = min(4, sub)

    def step(k, carry):
        with jax.named_scope("step_wait"):

            @pl.when((k == 1) & inner)
            def _():
                each(0, part_way, lambda j: d_pass(beyond, j, [OUT] + across))
                d_rest(facing)

            @pl.when((k == 1) & outer)
            def _():
                each(0, part_way, lambda j: d_pass(facing, j, across))
                d_rest(mate)

            @pl.when((k == 2) & inner)
            def _():
                each(part_way, sub, lambda j: d_pass(beyond, j, [OUT] + across))
                each(0, own, lambda c: c_send_on(c, f, (OUT,)))
                d_rest(mate)

            @pl.when((k == 2) & outer)
            def _():
                each(part_way, sub, lambda j: d_pass(facing, j, across))
                each(0, part_way, lambda j: d_pass(beyond, j, across))
                d_rest(facing)

            @pl.when((k == 3) & inner)
            def _():
                c_pass(0, facing, [OUT] + across)
                c_pass(0, mate, (MAIN,))
                c_pass(1, facing, [OUT] + across)
                d_rest(beyond)

            @pl.when((k == 3) & outer)
            def _():
                each(part_way, sub, lambda j: d_pass(beyond, j, across))
                d_rest(beyond)

        second = jnp.where(inner, facing, mate)
        third = jnp.where(inner, mate, facing)
        with jax.named_scope("product"):
            first_product(
                jnp.where(k == 0, f, jnp.where(k == 1, second, jnp.where(k == 2, third, beyond)))
            )
        return carry

    lax.fori_loop(0, n_fs, step, 0)
    hosted = n_col - own
    slots = 2 * hosted

    @pl.when(inner)
    def _():
        def begin(c):
            @pl.when(c > 0)
            def _():
                c_pass(c, mate, (MAIN,))

            @pl.when((c > 1) & (c < own - 1))
            def _():
                c_pass(c, facing, [OUT] + across)

            @pl.when(c == own - 1)
            def _():
                c_pass(c, facing, (OUT,))

        with jax.named_scope("begin"):
            each(0, own, begin)

    with jax.named_scope("sums_in"):
        sums_in()

    def norms_out(q):
        with jax.named_scope("norms"):
            norms(q)

        @pl.when(outer)
        def _():
            g_copy(q).start()

        m_out(0, q)

        @pl.when(inner & (q == pieces // 2 - 1))
        def _():
            c_pass(0, beyond, [OUT] + across)
            feed(own)

    def feed(c):
        @pl.when(c < n_col - 1)
        def _():
            c_send_on(c, f, (MAIN,), 2)
            c_pass(c, mate, (MAIN,), 2)

        @pl.when(c == n_col - 1)
        def _():
            c_pass(c, mate, (MAIN,), 2)
            c_send_on(c, f, (MAIN,), 2)
            for copy in straight_copies():
                copy.start()

    each(0, pieces, norms_out)

    def serve(i):
        c = jnp.where(
            i < hosted - 1,
            own + i,
            jnp.where(i == hosted - 1, n_col - 1, i - hosted),
        )
        last = n_col - 1

        @pl.when(c < last)
        def _():
            with jax.named_scope("rest"):
                c_rest(c)

        @pl.when((c >= own) & (c < last))
        def _():
            with jax.named_scope("prod1"):
                back[c - own] = second_product(1, c)
            b_copy(c).start()

        @pl.when(c == last)
        def _():
            def term(span, src):
                here = pl.ds(pl.multiple_of(src * depth, depth), depth)
                return jnp.dot(
                    mixed_all[1, span, here],
                    cols_all[last, src],
                    preferred_element_type=jnp.float32,
                )

            def add(k):
                src = jnp.where(k == 0, f, jnp.where(k == 1, mate, beyond))
                early[...] += term(slice(None), src)

            def half(h):
                span = tile_rows(h)
                total = early[span] + term(span, facing)
                gate = total[:, :lanes]
                back[last - own, span] = (
                    gate / (1.0 + jnp.exp(-gate)) * total[:, lanes:]
                ).astype(jnp.bfloat16)
                b_copy(last, span).start()

            early[...] = jnp.zeros_like(early)
            add(0)
            with jax.named_scope("rest"):
                ended(cols_all.at[last, pl.ds(0, 2), pl.ds(0, c_half)], c_late.at[last])
            each(1, 3, add)
            with jax.named_scope("rest_last"):
                ended(cols_all.at[last, 0, pl.ds(0, c_half)], c_late.at[n_col])
            each(0, 2, half)

        with jax.named_scope("prod0"):
            out_ref[:, col_lanes(c)] = second_product(0, c)

    def slot(s):
        c = own + s // 2
        last = c == n_col - 1
        src = jnp.where((s % 2 == 0) ^ last, facing, beyond)

        @pl.when(s % 2 == 0)
        def _():
            feed(c + 2)

        with jax.named_scope("slot"):

            @pl.when(jnp.logical_not(last))
            def _():
                c_pass(c, src, across, 2)

            @pl.when(s == slots - 2)
            def _():
                c_pass(c, beyond, across, 2)

            @pl.when(s == slots - 1)
            def _():
                for k in range(2):
                    c_pass_part(c, facing, k)
                each(own - moved, own, lambda m: tail(m, mate))

        when = s - (slots - 14)

        @pl.when(when == 1)
        def _():
            with jax.named_scope("m0"):
                m_relay_all()

        for q in range(pieces):

            @pl.when(when == 2 + q)
            def _():
                with jax.named_scope("from_mate"):
                    g_copy(q).wait_recv()
                    m_out(1, q)

            @pl.when(when == min(5 + q // 2 + q // 3, 7))
            def _():
                with jax.named_scope("m1"):
                    m_relay(1, q)

        @pl.when(when == 7)
        def _():
            with jax.named_scope("m_rest"):
                m_rest(0)
                m_rest(1)

        done = jnp.clip(when - 8, 0, hosted - 2)
        more = jnp.where(when == 13, n_col, jnp.clip(when - 7, 0, hosted - 2))
        each(done, more, serve)

    @pl.when(inner)
    def _():
        with jax.named_scope("beyond_own"):
            c_pass(1, beyond, [OUT] + across)
            feed(own + 1)
            each(2, own, lambda c: c_pass(c, beyond, [OUT] + across))
        each(0, slots, slot)

    @pl.when(outer)
    def _():
        each(ahead, n_col - 1, lambda c: c_send_on(c, f, (MAIN,), 2))
        c_send_on(n_col - 1, f, (MAIN,), 2)
        for share in others:
            each(own, n_col, lambda c: c_send_late(c, f, share))
            each(0, own - moved, lambda c: c_send_late(c, f, share))

        def pass_own(c):
            with jax.named_scope("pass_own"):
                c_pass(c, mate, across)

        def pass_far(src):
            def act(c):
                with jax.named_scope("pass_far"):
                    c_pass(c, src, across)

            return act

        each(0, own, pass_own)
        each(0, own, pass_far(facing))
        with jax.named_scope("m0"):
            m_relay_all()
            m_rest(0)
        each(0, own, pass_far(beyond))

        def make_own(c):
            with jax.named_scope("rest"):
                c_rest(c)
            with jax.named_scope("prod0"):
                out_ref[:, col_lanes(c)] = second_product(0, c)

        each(0, own, make_own)
        with jax.named_scope("b_wait"):
            ended(back, b_recv.at[0])

    def d_sent(blocks, ways):
        for way in ways:
            ended(down_all.at[pl.ds(0, blocks), pl.ds(0, d_half)], d_send.at[way])

    def c_sent(columns, blocks, ways):
        for way in ways:
            ended(
                cols_all.at[pl.ds(0, columns), pl.ds(0, blocks), pl.ds(0, c_half)], c_send.at[way]
            )

    with jax.named_scope("drain"):
        ended(spread.at[pl.ds(0, (n_tp - 1) * rows)], a_sem.at[0])
        ended(red.at[pl.ds(1, n_tp - 1)], r_sem.at[0])
        m_drain(0)

        @pl.when(inner)
        def _():
            d_sent(2, (MAIN,))
            d_sent(3, (OUT,))
            d_sent(2, across)
            c_sent(n_col, 2, (MAIN,))
            c_sent(own, 3, (OUT,))
            c_sent(n_col - 1, 2, across)
            c_sent(moved, 1, [TAIL + d for d in range(1, n_grp)])
            for copy in straight_copies():
                copy.wait_send()
            m_drain(1)
            ended(back, b_send.at[0])

        @pl.when(outer)
        def _():
            ended(down_all.at[f], d_send.at[MAIN])
            c_sent(n_col, 1, (MAIN,))
            late = n_col - moved
            ended(
                cols_all.at[pl.ds(0, late), 0, pl.ds(0, (n_grp - 1) * c_half)],
                c_send.at[LATE],
            )
            d_sent(3, across)
            c_sent(own, 3, across)
            ended(mixed_all.at[0, own_rows(t)], g_send.at[0])


def paired_call(sizes, arguments):
    n_grp, n_fs, n_tp = sizes
    residual_in, hidden_first, down_weight, _, _, _, gate_weight, _ = arguments
    rows, model = residual_in.shape
    depth, width = gate_weight.shape
    cols = down_weight.shape[1]
    tokens = rows * n_tp
    lanes = 128
    n_col = width // lanes
    share = down_weight.shape[0] // (n_grp * 16)
    sub = max(n for n in range(1, 12) if share % n == 0)
    own = n_col * 4 // 11
    pieces = 4
    ahead = n_col - 1
    moved = 2
    vmem = pl.BlockSpec(memory_space=pltpu.VMEM)
    hbm = pl.BlockSpec(memory_space=pltpu.HBM)
    dma = pltpu.SemaphoreType.DMA
    return pl.pallas_call(
        functools.partial(paired_kernel, (n_grp, n_fs, n_tp, sub, own, pieces, ahead, moved)),
        out_shape=(
            jax.ShapeDtypeStruct((rows, model), jnp.bfloat16),
            jax.ShapeDtypeStruct((tokens, width), jnp.bfloat16),
        ),
        in_specs=[hbm] * 8,
        out_specs=(vmem, vmem),
        scratch_shapes=[
            pltpu.VMEM((n_fs,) + down_weight.shape, jnp.bfloat16),
            pltpu.VMEM((n_col, n_fs, depth, 2 * lanes), jnp.bfloat16),
            pltpu.VMEM((tokens, width), jnp.bfloat16),
            pltpu.VMEM((n_fs, tokens, cols), jnp.bfloat16),
            pltpu.VMEM((n_tp, n_fs, rows, cols), jnp.bfloat16),
            pltpu.VMEM((2, tokens, model), jnp.bfloat16),
            pltpu.VMEM((n_col - own, tokens, lanes), jnp.bfloat16),
            pltpu.VMEM((rows, model), jnp.bfloat16),
            pltpu.VMEM((rows, model), jnp.bfloat16),
            pltpu.VMEM((2, model), jnp.float32),
            pltpu.VMEM((2, model), jnp.float32),
            pltpu.VMEM((tokens, 2 * lanes), jnp.float32),
            dma((7,)),
            dma((1 + n_grp,)),
            dma((n_fs - 1, sub)),
            dma((n_fs,)),
            dma((2 * n_grp + 2,)),
            dma((n_fs - 1, 2 * n_col - own)),
            dma((n_col + 1,)),
            dma((2,)),
            dma((2,)),
            dma((2,)),
            dma((n_tp // 2, 1 + pieces)),
            dma((2,)),
            dma((1,)),
            dma((pieces,)),
            dma((1,)),
            dma((1,)),
        ],
        compiler_params=pltpu.CompilerParams(
            collective_id=0, has_side_effects=True, vmem_limit_bytes=48 * 1024 * 1024
        ),
        name="paired_half_steps",
    )(*(pltpu.with_memory_space_constraint(a, pltpu.HBM) for a in arguments))


def write_kernel(mixed_ref, hidden_ref, mixed_out, hidden_out, sems):
    copies = [
        pltpu.make_async_copy(hidden_ref, hidden_out, sems.at[0]),
        pltpu.make_async_copy(mixed_ref, mixed_out, sems.at[1]),
    ]
    for copy in copies:
        copy.start()
    for copy in copies:
        copy.wait()


def written(mixed, hidden):
    return pl.pallas_call(
        write_kernel,
        out_shape=(
            jax.ShapeDtypeStruct(mixed.shape, mixed.dtype),
            jax.ShapeDtypeStruct(hidden.shape, hidden.dtype),
        ),
        in_specs=[pl.BlockSpec(memory_space=pltpu.VMEM)] * 2,
        out_specs=(pl.BlockSpec(memory_space=pl.ANY),) * 2,
        scratch_shapes=[pltpu.SemaphoreType.DMA((2,))],
        compiler_params=pltpu.CompilerParams(vmem_limit_bytes=8 * 1024 * 1024),
        name="write_out",
    )(mixed, hidden)


def fits_pairs(sizes, residual_in, down_weight, gate_weight):
    n_grp, n_fs, n_tp = sizes
    depth, width = gate_weight.shape
    return (
        n_grp == 2
        and n_fs == 4
        and n_tp % 2 == 0
        and width % 128 == 0
        and width // 128 >= 10
        and depth % (n_grp * 2 * 16) == 0
        and down_weight.shape[0] % (n_grp * 16) == 0
        and residual_in.shape[0] % (4 * 16) == 0
    )


def on_device(
    sizes,
    residual_in,
    hidden_first,
    down_weight,
    mixer_out,
    norm_gain,
    norm_shift,
    gate_weight,
    up_weight,
):
    if fits_pairs(sizes, residual_in, down_weight, gate_weight):
        arguments = (
            residual_in,
            hidden_first,
            down_weight,
            mixer_out,
            norm_gain,
            norm_shift,
            gate_weight,
            up_weight,
        )
        return written(*paired_call(sizes, arguments))
    n_grp, n_fs, n_tp = sizes
    rows, model = residual_in.shape
    depth, width = gate_weight.shape
    cols = down_weight.shape[1]
    sub = 1
    if depth % (n_grp * 2 * 32) == 0 and down_weight.shape[0] % (n_grp * 2 * 32) == 0:
        sub = 2
    chunks = n_grp * sub
    each = max(1, width * 3 // (11 * 128)) * 128
    shared = (width - each) // 128 * 128
    each = width - shared
    if width % 128:
        hidden_first = hidden_first.reshape(rows, n_tp, width).transpose(1, 0, 2)
    vmem = pl.BlockSpec(memory_space=pltpu.VMEM)
    anywhere = pl.BlockSpec(memory_space=pl.ANY)
    dma = pltpu.SemaphoreType.DMA
    tokens = rows * n_tp
    return pl.pallas_call(
        functools.partial(kernel, (n_grp, n_fs, n_tp, sub)),
        out_shape=(
            jax.ShapeDtypeStruct((rows, model), jnp.bfloat16),
            jax.ShapeDtypeStruct((tokens, width), jnp.bfloat16),
        ),
        in_specs=[vmem, anywhere, anywhere, vmem, vmem, vmem, anywhere, anywhere],
        out_specs=(vmem, vmem),
        scratch_shapes=[
            pltpu.VMEM((n_fs,) + down_weight.shape, jnp.bfloat16),
            pltpu.VMEM((n_fs, 2, depth, shared), jnp.bfloat16),
            pltpu.VMEM((n_fs, 2, depth, each), jnp.bfloat16),
            pltpu.VMEM((tokens, width), jnp.bfloat16),
            pltpu.VMEM((n_fs, tokens, cols), jnp.bfloat16),
            pltpu.VMEM((n_tp, n_fs, rows, cols), jnp.bfloat16),
            pltpu.VMEM((2, tokens, model), jnp.bfloat16),
            pltpu.VMEM((2, tokens, shared), jnp.float32),
            pltpu.VMEM((2, tokens, each), jnp.float32),
            pltpu.VMEM((tokens, shared), jnp.bfloat16),
            dma((6,)),
            dma((n_fs, 1 + n_grp, chunks)),
            dma((n_fs, chunks)),
            dma((2 * n_fs, 1 + n_grp, chunks)),
            dma((2 * n_fs, chunks)),
            dma((2 * n_fs, 1 + n_grp, chunks)),
            dma((2 * n_fs, chunks)),
            dma((n_tp,)),
            dma((n_tp,)),
            dma((n_tp, n_fs)),
            dma((n_tp, n_fs)),
            dma((2, n_tp, n_tp // 2)),
            dma((2, n_tp)),
            dma((1,)),
            dma((1,)),
            dma((2,)),
            dma((2,)),
        ],
        compiler_params=pltpu.CompilerParams(
            collective_id=0, has_side_effects=True, vmem_limit_bytes=60 * 1024 * 1024
        ),
        name="half_steps",
    )(
        residual_in,
        hidden_first,
        down_weight,
        mixer_out,
        norm_gain,
        norm_shift,
        gate_weight,
        up_weight,
    )


def solution(mesh):
    sizes = tuple(mesh.shape[axis] for axis in ("grp", "fs", "tp"))
    in_specs = (
        P(("grp", "fs", "tp"), None),
        P(("grp", "fs", "tp"), None),
        P("tp", "fs"),
        P(("grp", "fs", "tp"), None),
        P(),
        P(),
        P("fs", "tp"),
        P("fs", "tp"),
    )
    out_specs = (P(("grp", "fs", "tp"), None), P(("grp", "fs"), "tp"))
    return jax.shard_map(
        functools.partial(on_device, sizes),
        mesh=mesh,
        in_specs=in_specs,
        out_specs=out_specs,
        check_vma=False,
    )
```
